32 devices in a mesh: sp: 8 (over z, y), tp: 4 (over x, core).
Axes of the slice: x: 2, y: 2, z: 4, core: 2. Of those that a mesh axis runs over, the one named last changes fastest.
Arguments:
- latents: bfloat16 [2048, 4096], P('sp'), may hold values from -0.4375 to 0.4375
- query_heads: bfloat16 [2048, 16, 128], P('sp', 'tp'), may hold values from -8 to 8
- key_heads: bfloat16 [2048, 16, 128], P('sp', 'tp'), may hold values from -8 to 8
- value_heads: bfloat16 [2048, 16, 128], P('sp', 'tp'), may hold values from -6 to 6
- map_outputs: bfloat16 [2048, 2, 16, 128], P('sp', None, 'tp'), may hold values from -6 to 6
- log_sums: float32 [2048, 16, 2], P('sp', 'tp'), may hold values from -600 to 600, as said below
- out_grad: bfloat16 [2048, 16, 128], P('sp', 'tp'), may hold values from -6 to 6
- mix_lambda: float32 [16], P('tp'), may hold values from 0.3 to 0.8
- norm_gain: float32 [128], replicated, may hold values from 0.1 to 1.9
Outputs:
- query_grad: bfloat16 [2048, 16, 128], P('sp', 'tp')
- key_grad: bfloat16 [2048, 16, 128], P('sp', 'tp')
- value_grad: bfloat16 [2048, 16, 128], P('sp', 'tp')
- weight_grad: float32 [4096, 2048], P('sp', 'tp')
The draws below stay inside these ranges and needn't reach their ends.
Inputs may be any that keep to these rules, and one draw needn't show every extreme that they name: query_heads, key_heads and value_heads together with map_outputs and log_sums are one consistent causal forward pass: log_sums is the row's log-sum of exp(score_m) over keys at or before the row, and map_outputs[:, m] is prob_m times value_heads rounded to bfloat16.
All inputs are finite; a program needn't handle non-finite values.
Results may differ from the reference program's by a relative error of at most 0.019.
Values may be sent and summed in bfloat16 or wider, within the bound.
A program may use at most 64 MiB of HBM per device.

```python
import math
import jax
import jax.numpy as jnp
from jax import lax

D = 4096
HEADS = 16
DH = 64
TOKENS = 2048


def attention_forward(key):
    shape = (TOKENS, HEADS, 2 * DH)
    query_f = jnp.clip(1.3 * jax.random.normal(jax.random.fold_in(key, 101), shape, jnp.float32), -8.0, 8.0)
    key_f = jnp.clip(1.3 * jax.random.normal(jax.random.fold_in(key, 102), shape, jnp.float32), -8.0, 8.0)
    value_f = jnp.clip(jax.random.normal(jax.random.fold_in(key, 103), shape, jnp.float32), -6.0, 6.0)
    query_low = query_f.astype(jnp.bfloat16)
    key_low = key_f.astype(jnp.bfloat16)
    value_low = value_f.astype(jnp.bfloat16)
    length = TOKENS
    span = math.gcd(length, 512)
    score_scale = DH ** (-0.5)

    def per_head(inputs):
        query_one, key_one, value_one = inputs
        query_split = query_one.astype(jnp.float32).reshape(length, 2, DH)
        key_split = key_one.astype(jnp.float32).reshape(length, 2, DH)
        value_wide = value_one.astype(jnp.float32)
        key_pos = jnp.arange(length, dtype=jnp.int32)

        def visit(block_index):
            anchor = (block_index * span).astype(jnp.int32)
            query_blk = lax.dynamic_slice_in_dim(query_split, anchor, span, 0)
            scores = jnp.einsum('qmd,kmd->mqk', query_blk, key_split) * score_scale
            query_pos = anchor + jnp.arange(span, dtype=jnp.int32)
            causal = key_pos[None, :] <= query_pos[:, None]
            masked = jnp.where(causal[None], scores, -jnp.inf)
            highest = jnp.max(masked, axis=-1, keepdims=True)
            log_total = highest + jnp.log(jnp.sum(jnp.exp(masked - highest), axis=-1, keepdims=True))
            probs = jnp.exp(masked - log_total)
            outputs = jnp.einsum('mqk,ke->mqe', probs, value_wide)
            return (log_total[..., 0].T, outputs)
        lse_blocks, out_blocks = lax.map(visit, jnp.arange(length // span, dtype=jnp.int32))
        lse_head = lse_blocks.reshape(length, 2)
        out_head = jnp.transpose(out_blocks, (1, 0, 2, 3)).reshape(2, length, 2 * DH)
        return (lse_head, out_head)
    lse_all, out_all = lax.map(per_head, (jnp.transpose(query_low, (1, 0, 2)), jnp.transpose(key_low, (1, 0, 2)), jnp.transpose(value_low, (1, 0, 2))))
    log_table = jnp.transpose(lse_all, (1, 0, 2))
    out_table = jnp.transpose(out_all, (2, 1, 0, 3)).astype(jnp.bfloat16)
    return (query_low, key_low, value_low, out_table, log_table)


def draw_query_heads(key, part):
    return attention_forward(key)[0]


def draw_key_heads(key, part):
    return attention_forward(key)[1]


def draw_value_heads(key, part):
    return attention_forward(key)[2]


def draw_map_outputs(key, part):
    return attention_forward(key)[3]


def draw_log_sums(key, part):
    return attention_forward(key)[4]


def raised(values, stream_key, source, target, parts, factor):
    def block_of(position):
        return (jnp.arange(values.shape[position]) // (values.shape[position] // parts)).reshape((-1,) + (1,) * (values.ndim - 1 - position))

    near = jax.random.permutation(stream_key, parts)[block_of(target)]
    far = (block_of(target) + parts // 2) % parts
    return jnp.where((block_of(source) == near) | (block_of(source) == far), factor * values, values)


def level_of(key, extent, split, least, top_value):
    factor_of, own = 1.0, jax.random.fold_in(key, 6)
    for position, shards_of in split:
        steps = jnp.exp(jax.random.uniform(jax.random.fold_in(own, position), (shards_of,), jnp.float32, least / len(split), top_value / len(split)))
        factor_of = factor_of * jnp.repeat(steps, extent[position] // shards_of).reshape([-1 if axis == position else 1 for axis in range(len(extent))])
    return factor_of


def noise(key, dims, scale, most, pieces=(), kind=jnp.bfloat16):
    level = level_of(key, dims, pieces, -0.22, 0.18) if pieces else 1.0
    values = jax.random.normal(key, dims, jnp.float32) * scale * level
    return jnp.minimum(jnp.maximum(values, -most), most).astype(kind)


def gaussian_with(stream_key, shape, deviation, reach, shards, heavy, kind=jnp.bfloat16):
    entries = deviation * jax.random.normal(stream_key, shape, jnp.float32)
    if shards:
        entries = entries * level_of(stream_key, shape, shards, -0.22, 0.18)
    return jnp.clip(raised(entries, jax.random.fold_in(stream_key, 3), *heavy), -reach, reach).astype(kind)


def setup_inputs(seed: int = 0) -> dict:
    seeds = jax.random.split(jax.random.key(seed), 10)
    return {
        "latents": gaussian_with(seeds[0], (TOKENS, D), 0.02, 0.4375, ((0, 8),), (0, 1, 8, 2.0)),
        "query_heads": draw_query_heads(jax.random.fold_in(seeds[9], 71), 0),
        "key_heads": draw_key_heads(jax.random.fold_in(seeds[9], 71), 0),
        "value_heads": draw_value_heads(jax.random.fold_in(seeds[9], 71), 0),
        "map_outputs": draw_map_outputs(jax.random.fold_in(seeds[9], 71), 0),
        "log_sums": draw_log_sums(jax.random.fold_in(seeds[9], 71), 0),
        "out_grad": noise(seeds[6], (TOKENS, HEADS, 2 * DH), 1.0, 6.0, ((0, 8), (1, 4))),
        "mix_lambda": jnp.clip(0.3 + 0.5 * jax.random.uniform(seeds[7], (HEADS,), jnp.float32) ** level_of(seeds[7], (HEADS,), ((0, 4),), -0.2, 0.2), 0.3, 0.8),
        "norm_gain": jnp.clip(1.0 + 0.18 * jax.random.normal(seeds[8], (2 * DH,), jnp.float32), 0.1, 1.9),
    }


EPSILON = 1e-05

def reference(latents, query_heads, key_heads, value_heads, map_outputs, log_sums, out_grad, mix_lambda, norm_gain):
    highest = lax.Precision.HIGHEST
    score_scale = DH ** (-0.5)
    first_map = map_outputs[:, 0].astype(jnp.float32)
    second_map = map_outputs[:, 1].astype(jnp.float32)
    lambda_col = mix_lambda[None, :, None]
    combined = first_map - lambda_col * second_map
    inverse = lax.rsqrt(lax.optimization_barrier(jnp.mean(combined * combined, axis=-1, keepdims=True)) + EPSILON)
    weighted = norm_gain[None, None, :] * out_grad.astype(jnp.float32)
    grad_out = (inverse * weighted - inverse ** 3 * combined * lax.optimization_barrier(jnp.mean(combined * weighted, axis=-1, keepdims=True))).astype(jnp.bfloat16)
    grad_wide = lax.optimization_barrier(grad_out).astype(jnp.float32)
    row_terms = jnp.stack([lax.optimization_barrier(jnp.sum(grad_wide * first_map, axis=-1)), lax.optimization_barrier(jnp.sum(grad_wide * second_map, axis=-1))], axis=-1)
    length = query_heads.shape[0]
    span = math.gcd(length, 512)

    def per_head(inputs):
        query_one, key_one, value_one, grad_one, lse_one, term_one, lam = inputs
        query_split = query_one.astype(jnp.float32).reshape(length, 2, DH)
        key_split = key_one.astype(jnp.float32).reshape(length, 2, DH)
        value_wide = value_one.astype(jnp.float32)
        grad_full = grad_one.astype(jnp.float32)
        key_pos = jnp.arange(length, dtype=jnp.int32)
        map_signs = jnp.stack([jnp.ones((), jnp.float32), -lam])

        def visit(running, block_index):
            key_acc, value_acc = running
            anchor = (block_index * span).astype(jnp.int32)
            query_blk = lax.dynamic_slice_in_dim(query_split, anchor, span, 0)
            grad_blk = lax.dynamic_slice_in_dim(grad_full, anchor, span, 0)
            lse_blk = lax.dynamic_slice_in_dim(lse_one, anchor, span, 0)
            term_blk = lax.dynamic_slice_in_dim(term_one, anchor, span, 0)
            scores = jnp.einsum('qmd,kmd->mqk', query_blk, key_split, precision=highest) * score_scale
            query_pos = anchor + jnp.arange(span, dtype=jnp.int32)
            causal = key_pos[None, :] <= query_pos[:, None]
            softmax_maps = jnp.exp(jnp.where(causal[None], scores - lse_blk.T[:, :, None], -jnp.inf))
            mixed_grad = jnp.dot(grad_blk, value_wide.T, precision=highest)
            score_grad = map_signs[:, None, None] * softmax_maps * (mixed_grad[None] - term_blk.T[:, :, None])
            score_low = lax.optimization_barrier(score_grad.astype(jnp.bfloat16)).astype(jnp.float32)
            diff_weights = lax.optimization_barrier((softmax_maps[0] - lam * softmax_maps[1]).astype(jnp.bfloat16)).astype(jnp.float32)
            value_acc = value_acc + jnp.dot(diff_weights.T, grad_blk, precision=highest)
            query_part = score_scale * jnp.einsum('mqk,kmd->qmd', score_low, key_split, precision=highest)
            key_acc = key_acc + score_scale * jnp.einsum('mqk,qmd->kmd', score_low, query_blk, precision=highest)
            return ((key_acc, value_acc), query_part)
        start_state = (jnp.zeros((length, 2, DH), jnp.float32), jnp.zeros((length, 2 * DH), jnp.float32))
        (key_acc, value_acc), query_parts = lax.scan(visit, start_state, jnp.arange(length // span, dtype=jnp.int32))
        return (query_parts.reshape(length, 2 * DH), key_acc.reshape(length, 2 * DH), value_acc)

    def head_major(array):
        return jnp.transpose(array, (1, 0, 2))
    query_all, key_all, value_all = lax.map(per_head, (head_major(query_heads), head_major(key_heads), head_major(value_heads), head_major(grad_out), head_major(log_sums), head_major(row_terms), mix_lambda))
    query_grad = head_major(query_all).astype(jnp.bfloat16)
    key_grad = head_major(key_all).astype(jnp.bfloat16)
    value_grad = head_major(value_all).astype(jnp.bfloat16)
    weight_grad = jnp.dot(latents.T, query_grad.reshape(length, -1), preferred_element_type=jnp.float32)
    return (query_grad, key_grad, value_grad, weight_grad)
```

```python
import functools
import math

import jax
import jax.numpy as jnp
from jax import lax
from jax.experimental import pallas as pl
from jax.experimental.pallas import tpu as pltpu
from jax.sharding import PartitionSpec as P

EPSILON = 1e-05
LOG2E = math.log2(math.e)
F32 = jnp.float32
BF16 = jnp.bfloat16
MESH = pl.DeviceIdType.MESH


def dot_nn(a, b):
    return lax.dot_general(a, b, (((1,), (0,)), ((), ())), preferred_element_type=F32)


def dot_nt(a, b):
    return lax.dot_general(a, b, (((1,), (1,)), ((), ())), preferred_element_type=F32)


def dot_tn(a, b):
    return lax.dot_general(a, b, (((0,), (0,)), ((), ())), preferred_element_type=F32)


def norm_backward(heads, width, lam_ref, gain_ref, mo_ref, og_ref, lse_ref, grad_ref, col_ref, row_ref):
    for h in range(heads):
        first = mo_ref[:, 0, h, :].astype(F32)
        second = mo_ref[:, 1, h, :].astype(F32)
        lam = lam_ref[h]
        combined = first - lam * second
        inverse = lax.rsqrt(jnp.mean(combined * combined, axis=-1, keepdims=True) + EPSILON)
        weighted = gain_ref[...] * og_ref[:, h, :].astype(F32)
        grad = (
            inverse * weighted
            - inverse**3 * combined * jnp.mean(combined * weighted, axis=-1, keepdims=True)
        ).astype(BF16)
        grad_ref[:, h * width : (h + 1) * width] = grad
        wide = grad.astype(F32)
        lse = lse_ref[h] * LOG2E
        log_lam = jnp.log(jnp.full((1, 1), lam, F32)) * LOG2E
        lane = lax.broadcasted_iota(jnp.int32, wide.shape, 1)
        stats = jnp.where(lane == 0, lse[:, 0:1], lse[:, 1:2] - log_lam)
        stats = jnp.where(lane == 2, jnp.sum(wide * first, axis=-1, keepdims=True), stats)
        stats = jnp.where(lane == 3, jnp.sum(wide * second, axis=-1, keepdims=True), stats)
        col_ref[h] = stats
        row_ref[h] = jnp.transpose(stats)[0:4]


def main_kernel(nsp, ntp, heads, width, lam, gain, lat, own_k, own_v, own_q, mo, og, lse,
                dq_out, dk_out, dv_out, wg_out,
                own_g, col, row, own_dq, kvb, qgb, stb, dqb, latb, dq_acc, dk_acc, dv_acc,
                kv_s, qg_s, st_s, dq_s, kv_r, qg_r, st_r, dq_r,
                la_s, la_r, lb_s, lb_r, own_sem):
    nz = nsp // 2
    s = lax.axis_index("sp")
    t = lax.axis_index("tp")
    z, y = s // 2, lax.rem(s, 2)
    rows = own_k.shape[0]
    part = rows // ntp
    slab = lat.shape[1] // nsp
    score_scale = (width // 2) ** (-0.5)
    exp_scale = score_scale * LOG2E

    barrier = pltpu.get_barrier_semaphore()
    for d in range(1, nsp):
        pl.semaphore_signal(barrier, inc=1, device_id={"sp": lax.rem(s + d, nsp)}, device_id_type=MESH)
    for d in range(1, ntp):
        pl.semaphore_signal(barrier, inc=1, device_id={"tp": lax.rem(t + d, ntp)}, device_id_type=MESH)
    pl.semaphore_wait(barrier, nsp - 1 + ntp - 1)

    def copy(src, dst, send, recv, to):
        return pltpu.make_async_remote_copy(
            src_ref=src, dst_ref=dst, send_sem=send, recv_sem=recv,
            device_id={"sp": to}, device_id_type=MESH)

    side = 2 * z + (1 - y)

    def kv_copy(block, lane, k, p, src=None):
        to = jnp.minimum(s + 2, nsp - 1) if lane == 0 else side
        return copy(kvb.at[block, p] if src is None else src, kvb.at[block, p],
                    kv_s.at[lane, p, k], kv_r.at[p, block], to)

    def qg_copy(block, lane, k, p, src=None):
        to = jnp.maximum(s - 2, 0) if lane == 0 else side
        return copy(qgb.at[block, p] if src is None else src, qgb.at[block, p],
                    qg_s.at[lane, p, k], qg_r.at[p, block], to)

    def st_copy(block, lane, k, src=None):
        to = jnp.maximum(s - 2, 0) if lane == 0 else side
        return copy(stb.at[block] if src is None else src, stb.at[block],
                    st_s.at[lane, k], st_r.at[block], to)

    for p, src in ((0, own_k), (1, own_v)):
        @pl.when(z < nz - 1)
        def _():
            kv_copy(s, 0, 0, p, src).start()

        @pl.when(y == 0)
        def _():
            kv_copy(s, 1, 0, p, src).start()

    @pl.when(z > 0)
    def _():
        qg_copy(s, 0, 0, 0, own_q).start()

    @pl.when(y == 1)
    def _():
        qg_copy(s, 1, 0, 0, own_q).start()

    norm_backward(heads, width, lam, gain, mo, og, lse, own_g, col, row)

    @pl.when(z > 0)
    def _():
        st_copy(s, 0, 0, row).start()
        qg_copy(s, 0, 0, 1, own_g).start()

    @pl.when(y == 1)
    def _():
        st_copy(s, 1, 0, row).start()
        qg_copy(s, 1, 0, 1, own_g).start()

    lane_id = lax.broadcasted_iota(jnp.int32, (1, width), 1)
    low = jnp.where(lane_id < width // 2, 1.0, 0.0).astype(BF16)
    high = jnp.where(lane_id < width // 2, 0.0, 1.0).astype(BF16)

    def split(x):
        return jnp.concatenate([x * low, x * high], axis=0)

    def query_side(k_at, v_at, diagonal):
        def one(h, carry):
            at = pl.ds(pl.multiple_of(h * width, width), width)
            keys = split(k_at[:, at])
            scores = dot_nt(own_q[:, at], keys)
            mixed = dot_nt(own_g[:, at], v_at[:, at])
            stats = col[h]
            x1 = scores[:, :rows] * exp_scale - stats[:, 0:1]
            x2 = scores[:, rows:] * exp_scale - stats[:, 1:2]
            if diagonal:
                seen = (lax.broadcasted_iota(jnp.int32, (rows, rows), 1)
                        <= lax.broadcasted_iota(jnp.int32, (rows, rows), 0))
                x1 = jnp.where(seen, x1, -jnp.inf)
                x2 = jnp.where(seen, x2, -jnp.inf)
            g1 = (jnp.exp2(x1) * (mixed - stats[:, 2:3])).astype(BF16)
            g2 = (jnp.exp2(x2) * (stats[:, 3:4] - mixed)).astype(BF16)
            part_dq = dot_nn(jnp.concatenate([g1, g2], axis=1), keys)
            if diagonal:
                dq_acc[:, at] = part_dq
            else:
                dq_acc[:, at] += part_dq
            return carry
        lax.fori_loop(0, heads, one, 0)

    def key_side(q_at, g_at, row_at, diagonal):
        def one(h, carry):
            at = pl.ds(pl.multiple_of(h * width, width), width)
            queries = split(q_at[:, at])
            grads = g_at[:, at]
            scores = dot_nt(own_k[:, at], queries)
            mixed = dot_nt(own_v[:, at], grads)
            stats = row_at[h]
            x1 = scores[:, :rows] * exp_scale - stats[0:1]
            x2 = scores[:, rows:] * exp_scale - stats[1:2]
            if diagonal:
                seen = (lax.broadcasted_iota(jnp.int32, (rows, rows), 0)
                        <= lax.broadcasted_iota(jnp.int32, (rows, rows), 1))
                x1 = jnp.where(seen, x1, -jnp.inf)
                x2 = jnp.where(seen, x2, -jnp.inf)
            p1 = jnp.exp2(x1)
            p2 = jnp.exp2(x2)
            g1 = (p1 * (mixed - stats[2:3])).astype(BF16)
            g2 = (p2 * (stats[3:4] - mixed)).astype(BF16)
            part_dv = dot_nn((p1 - p2).astype(BF16), grads)
            part_dk = dot_nn(jnp.concatenate([g1, g2], axis=1), queries)
            if diagonal:
                dv_acc[:, at] = part_dv
                dk_acc[:, at] = part_dk
            else:
                dv_acc[:, at] += part_dv
                dk_acc[:, at] += part_dk
            return carry
        lax.fori_loop(0, heads, one, 0)

    def lat_copy(d):
        to = lax.rem(s + d, nsp)
        mine = pl.ds(pl.multiple_of(t * part, part), part)
        return copy(lat.at[mine, pl.ds(pl.multiple_of(to * slab, slab), slab)],
                    latb.at[s, mine, :], la_s.at[d], la_r.at[d], to)

    def own_lat():
        return pltpu.make_async_copy(
            lat.at[pl.ds(pl.multiple_of(t * part, part), part), pl.ds(pl.multiple_of(s * slab, slab), slab)],
            latb.at[s, pl.ds(pl.multiple_of(t * part, part), part), :], own_sem)

    def share_copy(d):
        mine = pl.ds(pl.multiple_of(t * part, part), part)
        return pltpu.make_async_remote_copy(
            src_ref=latb.at[:, mine, :], dst_ref=latb.at[:, mine, :],
            send_sem=lb_s.at[d], recv_sem=lb_r.at[d],
            device_id={"tp": lax.rem(t + d, ntp)}, device_id_type=MESH)

    own_lat().start()
    query_side(own_k, own_v, True)
    key_side(own_q, own_g, row, True)
    for d in range(1, nsp):
        lat_copy(d).start()

    def step(k, carry):
        below, above = z - k, z + k
        has_below, has_above = below >= 0, above < nz
        kb = jnp.maximum(below, 0) * 2 + y
        qb = jnp.minimum(above, nz - 1) * 2 + y

        for p in range(2):
            @pl.when(has_below)
            def _():
                kv_copy(kb, 0, 0, p).wait_recv()
                kv_copy(kb, 1, k, p).start()

            @pl.when(has_below & (z < nz - 1))
            def _():
                kv_copy(kb, 0, k, p).start()

            @pl.when(has_above)
            def _():
                qg_copy(qb, 0, 0, p).wait_recv()
                qg_copy(qb, 1, k, p).start()
                if p == 0:
                    st_copy(qb, 0, 0).wait_recv()
                    st_copy(qb, 1, k).start()

            @pl.when(has_above & (z > 0))
            def _():
                qg_copy(qb, 0, k, p).start()
                if p == 0:
                    st_copy(qb, 0, k).start()

        def turn(c, carry):
            dist = k - c
            other = jnp.where(c == 0, y, 1 - y)
            bz, qz = z - dist, z + dist
            use_kv = (bz >= 0) & (dist < nz) & ((dist > 0) | (y == 1))
            use_qg = (qz < nz) & (dist < nz) & ((dist > 0) | (y == 0))
            kblk = jnp.maximum(bz, 0) * 2 + other
            qblk = jnp.minimum(qz, nz - 1) * 2 + other

            @pl.when(use_kv)
            def _():
                @pl.when(c == 1)
                def _():
                    for p in range(2):
                        kv_copy(kblk, 1, 0, p).wait_recv()
                query_side(kvb.at[kblk, 0], kvb.at[kblk, 1], False)

            @pl.when(use_qg)
            def _():
                @pl.when(c == 1)
                def _():
                    for p in range(2):
                        qg_copy(qblk, 1, 0, p).wait_recv()
                    st_copy(qblk, 1, 0).wait_recv()
                key_side(qgb.at[qblk, 0], qgb.at[qblk, 1], stb.at[qblk], False)
            return carry
        lax.fori_loop(0, 2, turn, 0)
        return carry

    lax.fori_loop(1, nz + 1, step, 0)

    own_dq[...] = (dq_acc[...] * score_scale).astype(BF16)
    half = rows // 2

    def dq_copy(block, lane, idx, p, own=False):
        to = (jnp.minimum(s + 2, nsp - 2 + y), jnp.maximum(s - 2, y), side)[lane]
        at = pl.ds(p * half, half)
        return copy(own_dq.at[at] if own else dqb.at[block, at], dqb.at[block, at],
                    dq_s.at[lane, p, idx], dq_r.at[p, block], to)

    for p in range(2):
        @pl.when(z < nz - 1)
        def _():
            dq_copy(s, 0, z, p, True).start()

        @pl.when(z > 0)
        def _():
            dq_copy(s, 1, z, p, True).start()

        dq_copy(s, 2, z, p, True).start()

    for h in range(heads):
        at = slice(h * width, (h + 1) * width)
        dq_out[:, h, :] = own_dq[:, at]
        dk_out[:, h, :] = (dk_acc[:, at] * score_scale).astype(BF16)
        dv_out[:, h, :] = dv_acc[:, at].astype(BF16)

    own_lat().wait()
    for d in range(1, nsp):
        lat_copy(d).wait_recv()
    for d in range(1, ntp):
        share_copy(d).start()
    for d in range(1, ntp):
        share_copy(d).wait_recv()

    wg_out[...] = dot_tn(latb[s], own_dq[...])

    def add_block(block):
        wg_out[...] += dot_tn(latb[block], dqb[block])

    def gather(k, carry):
        for p in range(2):
            for lane, there, ok, more in (
                (0, z - k, z - k >= 0, z < nz - 1),
                (1, z + k, z + k < nz, z > 0),
            ):
                bz = jnp.clip(there, 0, nz - 1)
                block = bz * 2 + y

                @pl.when(ok)
                def _():
                    dq_copy(block, lane, bz, p).wait_recv()
                    dq_copy(block, 2, bz, p).start()

                @pl.when(ok & more)
                def _():
                    dq_copy(block, lane, bz, p).start()

        def turn(c, carry):
            dist = jnp.where(c < 2, k, k - 1)
            up = lax.rem(c, 2)
            bz = jnp.where(up == 0, z - dist, z + dist)
            ok = (bz >= 0) & (bz < nz) & (dist < nz) & ((dist > 0) | (up == 0))
            other = jnp.where(c < 2, y, 1 - y)
            block = jnp.clip(bz, 0, nz - 1) * 2 + other

            @pl.when(ok)
            def _():
                @pl.when(c >= 2)
                def _():
                    for p in range(2):
                        dq_copy(block, 2, 0, p).wait_recv()
                add_block(block)
            return carry
        lax.fori_loop(0, 4, turn, 0)
        return carry

    lax.fori_loop(1, nz + 1, gather, 0)

    def drain(k, carry):
        below, above = z - k, z + k
        has_below, has_above = below >= 0, above < nz

        for p in range(2):
            @pl.when(has_below & (z < nz - 1))
            def _():
                kv_copy(s, 0, k, p).wait_send()

            @pl.when(has_below & ((k > 0) | (y == 0)))
            def _():
                kv_copy(s, 1, k, p).wait_send()

            @pl.when(has_above & (z > 0))
            def _():
                qg_copy(s, 0, k, p).wait_send()
                if p == 0:
                    st_copy(s, 0, k).wait_send()

            @pl.when(has_above & ((k > 0) | (y == 1)))
            def _():
                qg_copy(s, 1, k, p).wait_send()
                if p == 0:
                    st_copy(s, 1, k).wait_send()

            @pl.when((k <= z) & (z < nz - 1))
            def _():
                dq_copy(s, 0, k, p).wait_send()

            @pl.when((k >= z) & (z > 0))
            def _():
                dq_copy(s, 1, k, p).wait_send()

            dq_copy(s, 2, k, p).wait_send()
        return carry

    lax.fori_loop(0, nz, drain, 0)
    for d in range(1, nsp):
        lat_copy(d).wait_send()
    for d in range(1, ntp):
        share_copy(d).wait_send()


def vmem():
    return pl.BlockSpec(memory_space=pltpu.VMEM)


def body(nsp, ntp, latents, query_heads, key_heads, value_heads, map_outputs, log_sums, out_grad,
         mix_lambda, norm_gain):
    rows, heads, width = query_heads.shape
    flat = (rows, heads * width)
    slab = latents.shape[1] // nsp
    nz = nsp // 2
    dma = pltpu.SemaphoreType.DMA
    dq, dk, dv, wg = pl.pallas_call(
        functools.partial(main_kernel, nsp, ntp, heads, width),
        out_shape=(
            jax.ShapeDtypeStruct(query_heads.shape, BF16),
            jax.ShapeDtypeStruct(query_heads.shape, BF16),
            jax.ShapeDtypeStruct(query_heads.shape, BF16),
            jax.ShapeDtypeStruct((slab, heads * width), F32),
        ),
        in_specs=[pl.BlockSpec(memory_space=pltpu.SMEM)] + [vmem()] * 8,
        out_specs=(vmem(),) * 4,
        scratch_shapes=[
            pltpu.VMEM(flat, BF16),
            pltpu.VMEM((heads, rows, width), F32),
            pltpu.VMEM((heads, 4, rows), F32),
            pltpu.VMEM(flat, BF16),
            pltpu.VMEM((nsp, 2) + flat, BF16),
            pltpu.VMEM((nsp, 2) + flat, BF16),
            pltpu.VMEM((nsp, heads, 4, rows), F32),
            pltpu.VMEM((nsp,) + flat, BF16),
            pltpu.VMEM((nsp, rows, slab), BF16),
            pltpu.VMEM(flat, F32),
            pltpu.VMEM(flat, F32),
            pltpu.VMEM(flat, F32),
            dma((2, 2, nz)), dma((2, 2, nz)), dma((2, nz)), dma((3, 2, nz)),
            dma((2, nsp)), dma((2, nsp)), dma((nsp,)), dma((2, nsp)),
            dma((nsp,)), dma((nsp,)), dma((ntp,)), dma((ntp,)),
            dma,
        ],
        compiler_params=pltpu.CompilerParams(collective_id=0, has_side_effects=True),
        name="main",
    )(
        mix_lambda,
        norm_gain[None, :],
        latents,
        key_heads.reshape(flat),
        value_heads.reshape(flat),
        query_heads.reshape(flat),
        map_outputs,
        out_grad,
        jnp.transpose(log_sums, (1, 0, 2)),
    )
    return dq, dk, dv, wg


def row_norm_backward(heads, width, lam_ref, gain_ref, mo_ref, og_ref, lse_ref, grad_ref, row_ref):
    for h in range(heads):
        first = mo_ref[:, 0, h, :].astype(F32)
        second = mo_ref[:, 1, h, :].astype(F32)
        lam = lam_ref[h]
        combined = first - lam * second
        inverse = lax.rsqrt(jnp.mean(combined * combined, axis=-1, keepdims=True) + EPSILON)
        weighted = gain_ref[...] * og_ref[:, h, :].astype(F32)
        grad = (
            inverse * weighted
            - inverse**3 * combined * jnp.mean(combined * weighted, axis=-1, keepdims=True)
        ).astype(BF16)
        grad_ref[:, h * width : (h + 1) * width] = grad
        wide = grad.astype(F32)
        lse = lse_ref[h] * LOG2E
        log_lam = jnp.log(jnp.full((1, 1), lam, F32)) * LOG2E
        lane = lax.broadcasted_iota(jnp.int32, wide.shape, 1)
        stats = jnp.where(lane == 0, lse[:, 0:1], lse[:, 1:2] - log_lam)
        stats = jnp.where(lane == 2, jnp.sum(wide * first, axis=-1, keepdims=True), stats)
        stats = jnp.where(lane == 3, jnp.sum(wide * second, axis=-1, keepdims=True), stats)
        row_ref[h] = jnp.transpose(stats)[0:4]


def hub_kernel(nsp, ntp, heads, width, lam, gain, lat, own_k, own_v, own_q, mo, og, lse,
               dq_out, dk_out, dv_out, wg_out,
               own_g, row, blk, stb, dq_acc, dk_acc, dv_acc, db, out_b, in_b, in_a, kt, kin, kst, kret, latb,
               f_s, z_s, b_r, st_r, d_s, d_r, ob_s, ib_r, ia_r, kt_s, kin_r, kst_s, kret_r,
               la_s, la_r, lb_s, lb_r, own_sem):
    nz = nsp // 2
    low, high, top = nz // 2 - 1, nz // 2, nz - 1
    s = lax.axis_index("sp")
    t = lax.axis_index("tp")
    z, y = s // 2, lax.rem(s, 2)
    rows = own_k.shape[0]
    span = 2 * rows
    pair = heads // 2
    lanes = pair * width
    part = rows // ntp
    slab = lat.shape[1] // nsp
    score_scale = (width // 2) ** (-0.5)
    exp_scale = score_scale * LOG2E
    partner = 2 * z + 1 - y
    Q, K, V, G, ST = range(5)

    barrier = pltpu.get_barrier_semaphore()
    for d in range(1, nsp):
        pl.semaphore_signal(barrier, inc=1, device_id={"sp": lax.rem(s + d, nsp)}, device_id_type=MESH)
    for d in range(1, ntp):
        pl.semaphore_signal(barrier, inc=1, device_id={"tp": lax.rem(t + d, ntp)}, device_id_type=MESH)
    pl.semaphore_wait(barrier, nsp - 1 + ntp - 1)

    def copy(src, dst, send, recv, to):
        return pltpu.make_async_remote_copy(
            src_ref=src, dst_ref=dst, send_sem=send, recv_sem=recv,
            device_id={"sp": to}, device_id_type=MESH)

    def at_level(level):
        return 2 * level + y

    def lane_of(p):
        return pl.ds(pl.multiple_of(p * lanes, lanes), lanes)

    def half_of(p):
        return pl.ds(pl.multiple_of(p * rows, rows), rows)

    owned = (own_q, own_k, own_v, own_g)

    def source(a, p):
        if a == ST:
            return row.at[pl.ds(p * pair, pair)]
        return owned[a].at[:, lane_of(p)]

    def landing(a, level, half):
        return stb.at[level, half] if a == ST else blk.at[a, level, half_of(half), :]

    def landed(a, level, half):
        return st_r.at[level, half] if a == ST else b_r.at[a, level, half]

    def swap(a):
        return copy(source(a, 1 - y), landing(a, z, y), f_s.at[a], landed(a, z, y), partner)

    def arrive(a, level, half):
        copy(landing(a, level, half), landing(a, level, half), f_s.at[a], landed(a, level, half), partner).wait_recv()

    def pass_on(a, own, lane):
        half = y if own else 1 - y
        to = low if lane == 0 else high
        return copy(source(a, y) if own else landing(a, z, half), landing(a, z, half),
                    z_s.at[lane, a, 0 if own else 1], landed(a, z, half), at_level(to))

    def passes(action, arrays, own):
        for a in arrays:
            if a in (K, V):
                @pl.when(z < low)
                def _():
                    action(pass_on(a, own, 0))
            else:
                @pl.when(z >= high)
                def _():
                    action(pass_on(a, own, 0))

                @pl.when(z > high)
                def _():
                    action(pass_on(a, own, 1))

    def start(c):
        c.start()

    swap(Q).start()
    passes(start, (Q, K, V), True)
    swap(K).start()
    swap(V).start()

    row_norm_backward(heads, width, lam, gain, mo, og, lse, own_g, row)

    swap(G).start()
    swap(ST).start()
    passes(start, (ST, G), True)

    for a in (Q, K, V, G):
        blk[a, z, half_of(y), :] = owned[a][:, lane_of(y)]
    stb[z, y] = row[pl.ds(y * pair, pair)]
    dq_acc[...] = jnp.zeros_like(dq_acc)
    dk_acc[...] = jnp.zeros_like(dk_acc)
    dv_acc[...] = jnp.zeros_like(dv_acc)

    for a in (Q, K, V, ST, G):
        arrive(a, z, 1 - y)
        passes(start, (a,), False)

    lane_id = lax.broadcasted_iota(jnp.int32, (1, width), 1)
    first_map = jnp.where(lane_id < width // 2, 1.0, 0.0).astype(BF16)
    second_map = jnp.where(lane_id < width // 2, 0.0, 1.0).astype(BF16)

    def split(x):
        return jnp.concatenate([x * first_map, x * second_map], axis=0)

    def visit(qz, kz, slot, diagonal):
        def one(h, carry):
            at = pl.ds(pl.multiple_of(h * width, width), width)
            for a in range(2):
                start_row = a * rows if diagonal else 0
                kr = pl.ds(a * rows, rows)
                qr = pl.ds(start_row, span - start_row)
                count = span - start_row
                keys = split(blk[K, kz, kr, at])
                queries = split(blk[Q, qz, qr, at])
                grads = blk[G, qz, qr, at]
                scores = dot_nt(blk[K, kz, kr, at], queries)
                mixed = dot_nt(blk[V, kz, kr, at], grads)
                stats = jnp.concatenate([stb[qz, p, h] for p in range(start_row // rows, 2)], axis=1)
                x1 = scores[:, :count] * exp_scale - stats[0:1]
                x2 = scores[:, count:] * exp_scale - stats[1:2]
                if diagonal:
                    seen = (lax.broadcasted_iota(jnp.int32, (rows, count), 0)
                            <= lax.broadcasted_iota(jnp.int32, (rows, count), 1))
                    x1 = jnp.where(seen, x1, -jnp.inf)
                    x2 = jnp.where(seen, x2, -jnp.inf)
                p1 = jnp.exp2(x1)
                p2 = jnp.exp2(x2)
                g1 = (p1 * (mixed - stats[2:3])).astype(BF16)
                g2 = (p2 * (stats[3:4] - mixed)).astype(BF16)
                dv_acc[slot, kr, at] += dot_nn((p1 - p2).astype(BF16), grads)
                dk_acc[slot, kr, at] += dot_nn(jnp.concatenate([g1, g2], axis=1), queries)
                dq_acc[qz, h, :, qr] += dot_tn(keys, jnp.concatenate([g1, g2], axis=0))
            return carry
        lax.fori_loop(0, pair, one, 0)

    def dq_value(level):
        return jnp.concatenate([jnp.transpose(dq_acc[level, h]) for h in range(pair)], axis=1) * score_scale

    def grad_copy(level, lane):
        if lane == 0:
            to = partner
        elif lane == 1:
            to = at_level(jnp.where(z == low, 0, jnp.where(z == high, top, low)))
        else:
            to = at_level(high)
        return copy(db.at[level, y], db.at[level, y], d_s.at[level, lane], d_r.at[level, y], to)

    def grad_lanes(level):
        chained = (z == high) | ((z == low) if level >= low else (z < low))
        if level > low:
            return ((0, None), (1, chained))
        return ((0, None), (1, chained), (2, z == level))

    def grad_each(level, action):
        for lane, ok in reversed(grad_lanes(level)):
            if ok is None:
                action(grad_copy(level, lane))
            else:
                @pl.when(ok)
                def _():
                    action(grad_copy(level, lane))

    def grad_arrive(level, p):
        copy(db.at[level, p], db.at[level, p], d_s.at[level, 0], d_r.at[level, p], partner).wait_recv()

    def part_copy(i):
        return copy(out_b.at[i], in_b.at[i], ob_s.at[i], ib_r.at[i], at_level(jnp.where(z == low, high, low)))

    def top_copy():
        return copy(out_b.at[0], in_a, ob_s.at[0], ia_r, at_level(high))

    def key_copy(i):
        return copy(kt.at[i], kin.at[i], kt_s.at[i], kin_r.at[i], at_level(0))

    def return_copy(i):
        return copy(kst.at[i], kret.at[i, y], kst_s.at[i], kret_r.at[i], partner)

    def lat_copy(d):
        to = lax.rem(s + d, nsp)
        mine = pl.ds(pl.multiple_of(t * part, part), part)
        return copy(lat.at[mine, pl.ds(pl.multiple_of(to * slab, slab), slab)],
                    latb.at[s, mine, :], la_s.at[d], la_r.at[s], to)

    def own_lat():
        return pltpu.make_async_copy(
            lat.at[:, pl.ds(pl.multiple_of(s * slab, slab), slab)], latb.at[s], own_sem)

    def share_copy(b, d):
        mine = pl.ds(pl.multiple_of(t * part, part), part)
        return pltpu.make_async_remote_copy(
            src_ref=latb.at[b, mine, :], dst_ref=latb.at[b, mine, :],
            send_sem=lb_s.at[b, d], recv_sem=lb_r.at[b, d],
            device_id={"tp": lax.rem(t + d, ntp)}, device_id_type=MESH)

    def lat_send(descending):
        for d in range(1, nsp):
            to = lax.rem(s + d, nsp)
            down = (z >= high) & (to // 2 < high)

            @pl.when(down if descending else jnp.logical_not(down))
            def _():
                lat_copy(d).start()

    def lat_share(descending):
        def step(d, carry):
            b = lax.rem(s + d, nsp)
            down = (z < high) & (b // 2 >= high)

            @pl.when(down if descending else jnp.logical_not(down))
            def _():
                mine = pl.ds(pl.multiple_of(t * part, part), part)
                copy(latb.at[b, mine, :], latb.at[b, mine, :], la_s.at[1], la_r.at[b], partner).wait_recv()
                for e in range(1, ntp):
                    share_copy(b, e).start()
            return carry
        lax.fori_loop(1, nsp, step, 0)

    own_lat().start()
    visit(z, z, 0, True)

    @pl.when(z < low)
    def _():
        db[0, y] = dq_value(0).astype(BF16)
        grad_each(0, start)

    @pl.when(z >= high)
    def _():
        out_b[0] = dq_value(z).astype(BF16)

    @pl.when(z == high)
    def _():
        part_copy(0).start()

    @pl.when(z > high)
    def _():
        top_copy().start()

    lat_send(False)

    @pl.when(z == low)
    def _():
        def step(i, carry):
            qz = jnp.where(i == 0, low, high + (i - 1) // 2)
            kz = jnp.where(i == 0, 0, lax.rem(i - 1, 2))

            @pl.when(i == 0)
            def _():
                for half in range(2):
                    arrive(K, 0, half)
                    arrive(V, 0, half)

            @pl.when((i > 0) & (kz == 0))
            def _():
                for a in (Q, ST, G):
                    for half in range(2):
                        arrive(a, qz, half)

            visit(qz, kz, 1 - kz, False)

            @pl.when(i == 0)
            def _():
                db[low, y] = dq_value(low).astype(BF16)
                grad_each(low, start)

            @pl.when((i > 0) & (kz == 1))
            def _():
                out_b[qz - high] = dq_value(qz).astype(BF16)
                part_copy(qz - high).start()

            @pl.when((qz == top) & (kz == 0))
            def _():
                kt[0] = (dk_acc[1] * score_scale).astype(BF16)
                kt[1] = dv_acc[1].astype(BF16)
                key_copy(0).start()
                key_copy(1).start()
            return carry
        lax.fori_loop(0, 5, step, 0)

    @pl.when(z == high)
    def _():
        for a in (Q, ST, G):
            for half in range(2):
                arrive(a, top, half)
        visit(top, high, 0, False)
        top_copy().wait_recv()
        out_b[1] = (dq_value(top) + in_a[...].astype(F32)).astype(BF16)
        part_copy(1).start()

    lat_send(True)

    def finish_keys(extra):
        for i, acc, scale in ((0, dk_acc, score_scale), (1, dv_acc, 1.0)):
            other = acc[0, half_of(1 - y), :] * scale
            mine = acc[0, half_of(y), :] * scale
            if extra:
                other += kin[i, half_of(1 - y), :].astype(F32)
                mine += kin[i, half_of(y), :].astype(F32)
            kst[i] = other.astype(BF16)
            return_copy(i).start()
            kret[i, y] = mine.astype(BF16)

    @pl.when(z >= low)
    def _():
        finish_keys(False)

    for level in (0, low):
        @pl.when(z != level)
        def _():
            grad_arrive(level, y)
            grad_each(level, start)

    lat_share(False)

    @pl.when(z < low)
    def _():
        for i in range(2):
            key_copy(i).wait_recv()
        finish_keys(True)

    for level in (high, top):
        i = level - high

        @pl.when((z == low) | (z == high))
        def _():
            part_copy(i).wait_recv()
            total = dq_value(level) + in_b[i].astype(F32)
            if level == top:
                above = in_a[...].astype(F32)
                total = total + jnp.where(z == high, above, jnp.zeros_like(above))
            db[level, y] = total.astype(BF16)

        @pl.when((z != low) & (z != high))
        def _():
            grad_arrive(level, y)
        grad_each(level, start)

    lat_share(True)
    own_lat().wait()

    for level in range(nz):
        grad_arrive(level, 1 - y)
        for half in range(2):
            b = 2 * level + half

            @pl.when(s != b)
            def _():
                for e in range(1, ntp):
                    share_copy(b, e).wait_recv()
        feed = latb[2 * level : 2 * level + 2].reshape(span, slab)
        for p in range(2):
            at = slice(p * lanes, (p + 1) * lanes)
            term = dot_tn(feed, db[level, p])
            if level == 0:
                wg_out[:, at] = term
            else:
                wg_out[:, at] += term

    for i in range(2):
        return_copy(i).wait_recv()
        out = dk_out if i == 0 else dv_out
        for p in range(2):
            for h in range(pair):
                out[:, p * pair + h, :] = kret[i, p, :, h * width : (h + 1) * width]
    for p in range(2):
        for h in range(pair):
            dq_out[:, p * pair + h, :] = db[z, p, half_of(y), h * width : (h + 1) * width]

    def sent(c):
        c.wait_send()

    for a in range(5):
        sent(swap(a))
    for own in (True, False):
        passes(sent, (Q, K, V, ST, G), own)
    for level in range(nz):
        grad_each(level, sent)
    for i in range(2):
        sent(return_copy(i))

        @pl.when((z == low) | (z == high))
        def _():
            sent(part_copy(i))

        @pl.when(z == low)
        def _():
            sent(key_copy(i))

    @pl.when(z > high)
    def _():
        sent(top_copy())
    for d in range(1, nsp):
        sent(lat_copy(d))

    def drain(d, carry):
        for e in range(1, ntp):
            sent(share_copy(lax.rem(s + d, nsp), e))
        return carry
    lax.fori_loop(1, nsp, drain, 0)


def hub_body(nsp, ntp, latents, query_heads, key_heads, value_heads, map_outputs, log_sums, out_grad,
             mix_lambda, norm_gain):
    rows, heads, width = query_heads.shape
    flat = (rows, heads * width)
    slab = latents.shape[1] // nsp
    nz = nsp // 2
    pair = heads // 2
    block = (2 * rows, pair * width)
    half = (rows, pair * width)
    dma = pltpu.SemaphoreType.DMA
    return pl.pallas_call(
        functools.partial(hub_kernel, nsp, ntp, heads, width),
        out_shape=(
            jax.ShapeDtypeStruct(query_heads.shape, BF16),
            jax.ShapeDtypeStruct(query_heads.shape, BF16),
            jax.ShapeDtypeStruct(query_heads.shape, BF16),
            jax.ShapeDtypeStruct((slab, heads * width), F32),
        ),
        in_specs=[pl.BlockSpec(memory_space=pltpu.SMEM)] + [vmem()] * 8,
        out_specs=(vmem(),) * 4,
        scratch_shapes=[
            pltpu.VMEM(flat, BF16),
            pltpu.VMEM((heads, 4, rows), F32),
            pltpu.VMEM((4, nz) + block, BF16),
            pltpu.VMEM((nz, 2, pair, 4, rows), F32),
            pltpu.VMEM((nz, pair, width, 2 * rows), F32),
            pltpu.VMEM((2,) + block, F32),
            pltpu.VMEM((2,) + block, F32),
            pltpu.VMEM((nz, 2) + block, BF16),
            pltpu.VMEM((2,) + block, BF16),
            pltpu.VMEM((2,) + block, BF16),
            pltpu.VMEM(block, BF16),
            pltpu.VMEM((2,) + block, BF16),
            pltpu.VMEM((2,) + block, BF16),
            pltpu.VMEM((2,) + half, BF16),
            pltpu.VMEM((2, 2) + half, BF16),
            pltpu.VMEM((nsp, rows, slab), BF16),
            dma((5,)), dma((2, 5, 2)), dma((4, nz, 2)), dma((nz, 2)), dma((nz, 3)), dma((nz, 2)),
            dma((2,)), dma((2,)), dma, dma((2,)), dma((2,)), dma((2,)), dma((2,)),
            dma((nsp,)), dma((nsp,)), dma((nsp, ntp)), dma((nsp, ntp)),
            dma,
        ],
        compiler_params=pltpu.CompilerParams(collective_id=0, has_side_effects=True),
        name="hub",
    )(
        mix_lambda,
        norm_gain[None, :],
        latents,
        key_heads.reshape(flat),
        value_heads.reshape(flat),
        query_heads.reshape(flat),
        map_outputs,
        out_grad,
        jnp.transpose(log_sums, (1, 0, 2)),
    )


def solution(mesh):
    placed = (
        P("sp", None),
        P("sp", "tp", None),
        P("sp", "tp", None),
        P("sp", "tp", None),
        P("sp", None, "tp", None),
        P("sp", "tp", None),
        P("sp", "tp", None),
        P("tp"),
        P(),
    )
    nsp, ntp = mesh.shape["sp"], mesh.shape["tp"]

    def chosen(*args):
        heads = args[1].shape[1]
        return (hub_body if nsp == 8 and heads % 2 == 0 else body)(nsp, ntp, *args)

    return jax.shard_map(
        chosen,
        mesh=mesh,
        in_specs=placed,
        out_specs=(P("sp", "tp", None), P("sp", "tp", None), P("sp", "tp", None), P("sp", "tp")),
        check_vma=False,
    )
```

```python
import functools
import math

import jax
import jax.numpy as jnp
from jax import lax
from jax.experimental import pallas as pl
from jax.experimental.pallas import tpu as pltpu
from jax.sharding import PartitionSpec as P

EPSILON = 1e-05
LOG2E = math.log2(math.e)
F32 = jnp.float32
BF16 = jnp.bfloat16
MESH = pl.DeviceIdType.MESH


def dot_nn(a, b):
    return lax.dot_general(a, b, (((1,), (0,)), ((), ())), preferred_element_type=F32)


def dot_nt(a, b):
    return lax.dot_general(a, b, (((1,), (1,)), ((), ())), preferred_element_type=F32)


def dot_tn(a, b):
    return lax.dot_general(a, b, (((0,), (0,)), ((), ())), preferred_element_type=F32)


def norm_backward(heads, width, lam_ref, gain_ref, mo_ref, og_ref, lse_ref, grad_ref, col_ref, row_ref):
    for h in range(heads):
        first = mo_ref[:, 0, h, :].astype(F32)
        second = mo_ref[:, 1, h, :].astype(F32)
        lam = lam_ref[h]
        combined = first - lam * second
        inverse = lax.rsqrt(jnp.mean(combined * combined, axis=-1, keepdims=True) + EPSILON)
        weighted = gain_ref[...] * og_ref[:, h, :].astype(F32)
        grad = (
            inverse * weighted
            - inverse**3 * combined * jnp.mean(combined * weighted, axis=-1, keepdims=True)
        ).astype(BF16)
        grad_ref[:, h * width : (h + 1) * width] = grad
        wide = grad.astype(F32)
        lse = lse_ref[h] * LOG2E
        log_lam = jnp.log(jnp.full((1, 1), lam, F32)) * LOG2E
        lane = lax.broadcasted_iota(jnp.int32, wide.shape, 1)
        stats = jnp.where(lane == 0, lse[:, 0:1], lse[:, 1:2] - log_lam)
        stats = jnp.where(lane == 2, jnp.sum(wide * first, axis=-1, keepdims=True), stats)
        stats = jnp.where(lane == 3, jnp.sum(wide * second, axis=-1, keepdims=True), stats)
        col_ref[h] = stats
        row_ref[h] = jnp.transpose(stats)[0:4]


def main_kernel(nsp, ntp, heads, width, lam, gain, lat, own_k, own_v, own_q, mo, og, lse,
                dq_out, dk_out, dv_out, wg_out,
                own_g, col, row, own_dq, kvb, qgb, stb, dqb, latb, dq_acc, dk_acc, dv_acc,
                kv_s, qg_s, st_s, dq_s, kv_r, qg_r, st_r, dq_r,
                la_s, la_r, lb_s, lb_r, own_sem):
    nz = nsp // 2
    s = lax.axis_index("sp")
    t = lax.axis_index("tp")
    z, y = s // 2, lax.rem(s, 2)
    rows = own_k.shape[0]
    part = rows // ntp
    slab = lat.shape[1] // nsp
    score_scale = (width // 2) ** (-0.5)
    exp_scale = score_scale * LOG2E

    barrier = pltpu.get_barrier_semaphore()
    for d in range(1, nsp):
        pl.semaphore_signal(barrier, inc=1, device_id={"sp": lax.rem(s + d, nsp)}, device_id_type=MESH)
    for d in range(1, ntp):
        pl.semaphore_signal(barrier, inc=1, device_id={"tp": lax.rem(t + d, ntp)}, device_id_type=MESH)
    pl.semaphore_wait(barrier, nsp - 1 + ntp - 1)

    def copy(src, dst, send, recv, to):
        return pltpu.make_async_remote_copy(
            src_ref=src, dst_ref=dst, send_sem=send, recv_sem=recv,
            device_id={"sp": to}, device_id_type=MESH)

    side = 2 * z + (1 - y)

    def kv_copy(block, lane, k, p, src=None):
        to = jnp.minimum(s + 2, nsp - 1) if lane == 0 else side
        return copy(kvb.at[block, p] if src is None else src, kvb.at[block, p],
                    kv_s.at[lane, p, k], kv_r.at[p, block], to)

    def qg_copy(block, lane, k, p, src=None):
        to = jnp.maximum(s - 2, 0) if lane == 0 else side
        return copy(qgb.at[block, p] if src is None else src, qgb.at[block, p],
                    qg_s.at[lane, p, k], qg_r.at[p, block], to)

    def st_copy(block, lane, k, src=None):
        to = jnp.maximum(s - 2, 0) if lane == 0 else side
        return copy(stb.at[block] if src is None else src, stb.at[block],
                    st_s.at[lane, k], st_r.at[block], to)

    for p, src in ((0, own_k), (1, own_v)):
        @pl.when(z < nz - 1)
        def _():
            kv_copy(s, 0, 0, p, src).start()

        @pl.when(y == 0)
        def _():
            kv_copy(s, 1, 0, p, src).start()

    @pl.when(z > 0)
    def _():
        qg_copy(s, 0, 0, 0, own_q).start()

    @pl.when(y == 1)
    def _():
        qg_copy(s, 1, 0, 0, own_q).start()

    norm_backward(heads, width, lam, gain, mo, og, lse, own_g, col, row)

    @pl.when(z > 0)
    def _():
        st_copy(s, 0, 0, row).start()
        qg_copy(s, 0, 0, 1, own_g).start()

    @pl.when(y == 1)
    def _():
        st_copy(s, 1, 0, row).start()
        qg_copy(s, 1, 0, 1, own_g).start()

    lane_id = lax.broadcasted_iota(jnp.int32, (1, width), 1)
    low = jnp.where(lane_id < width // 2, 1.0, 0.0).astype(BF16)
    high = jnp.where(lane_id < width // 2, 0.0, 1.0).astype(BF16)

    def split(x):
        return jnp.concatenate([x * low, x * high], axis=0)

    def query_side(k_at, v_at, diagonal):
        def one(h, carry):
            at = pl.ds(pl.multiple_of(h * width, width), width)
            keys = split(k_at[:, at])
            scores = dot_nt(own_q[:, at], keys)
            mixed = dot_nt(own_g[:, at], v_at[:, at])
            stats = col[h]
            x1 = scores[:, :rows] * exp_scale - stats[:, 0:1]
            x2 = scores[:, rows:] * exp_scale - stats[:, 1:2]
            if diagonal:
                seen = (lax.broadcasted_iota(jnp.int32, (rows, rows), 1)
                        <= lax.broadcasted_iota(jnp.int32, (rows, rows), 0))
                x1 = jnp.where(seen, x1, -jnp.inf)
                x2 = jnp.where(seen, x2, -jnp.inf)
            g1 = (jnp.exp2(x1) * (mixed - stats[:, 2:3])).astype(BF16)
            g2 = (jnp.exp2(x2) * (stats[:, 3:4] - mixed)).astype(BF16)
            part_dq = dot_nn(jnp.concatenate([g1, g2], axis=1), keys)
            if diagonal:
                dq_acc[:, at] = part_dq
            else:
                dq_acc[:, at] += part_dq
            return carry
        lax.fori_loop(0, heads, one, 0)

    def key_side(q_at, g_at, row_at, diagonal):
        def one(h, carry):
            at = pl.ds(pl.multiple_of(h * width, width), width)
            queries = split(q_at[:, at])
            grads = g_at[:, at]
            scores = dot_nt(own_k[:, at], queries)
            mixed = dot_nt(own_v[:, at], grads)
            stats = row_at[h]
            x1 = scores[:, :rows] * exp_scale - stats[0:1]
            x2 = scores[:, rows:] * exp_scale - stats[1:2]
            if diagonal:
                seen = (lax.broadcasted_iota(jnp.int32, (rows, rows), 0)
                        <= lax.broadcasted_iota(jnp.int32, (rows, rows), 1))
                x1 = jnp.where(seen, x1, -jnp.inf)
                x2 = jnp.where(seen, x2, -jnp.inf)
            p1 = jnp.exp2(x1)
            p2 = jnp.exp2(x2)
            g1 = (p1 * (mixed - stats[2:3])).astype(BF16)
            g2 = (p2 * (stats[3:4] - mixed)).astype(BF16)
            part_dv = dot_nn((p1 - p2).astype(BF16), grads)
            part_dk = dot_nn(jnp.concatenate([g1, g2], axis=1), queries)
            if diagonal:
                dv_acc[:, at] = part_dv
                dk_acc[:, at] = part_dk
            else:
                dv_acc[:, at] += part_dv
                dk_acc[:, at] += part_dk
            return carry
        lax.fori_loop(0, heads, one, 0)

    def lat_copy(d):
        to = lax.rem(s + d, nsp)
        mine = pl.ds(pl.multiple_of(t * part, part), part)
        return copy(lat.at[mine, pl.ds(pl.multiple_of(to * slab, slab), slab)],
                    latb.at[s, mine, :], la_s.at[d], la_r.at[d], to)

    def own_lat():
        return pltpu.make_async_copy(
            lat.at[pl.ds(pl.multiple_of(t * part, part), part), pl.ds(pl.multiple_of(s * slab, slab), slab)],
            latb.at[s, pl.ds(pl.multiple_of(t * part, part), part), :], own_sem)

    def share_copy(d):
        mine = pl.ds(pl.multiple_of(t * part, part), part)
        return pltpu.make_async_remote_copy(
            src_ref=latb.at[:, mine, :], dst_ref=latb.at[:, mine, :],
            send_sem=lb_s.at[d], recv_sem=lb_r.at[d],
            device_id={"tp": lax.rem(t + d, ntp)}, device_id_type=MESH)

    own_lat().start()
    query_side(own_k, own_v, True)
    key_side(own_q, own_g, row, True)
    for d in range(1, nsp):
        lat_copy(d).start()

    def step(k, carry):
        below, above = z - k, z + k
        has_below, has_above = below >= 0, above < nz
        kb = jnp.maximum(below, 0) * 2 + y
        qb = jnp.minimum(above, nz - 1) * 2 + y

        for p in range(2):
            @pl.when(has_below)
            def _():
                kv_copy(kb, 0, 0, p).wait_recv()
                kv_copy(kb, 1, k, p).start()

            @pl.when(has_below & (z < nz - 1))
            def _():
                kv_copy(kb, 0, k, p).start()

            @pl.when(has_above)
            def _():
                qg_copy(qb, 0, 0, p).wait_recv()
                qg_copy(qb, 1, k, p).start()
                if p == 0:
                    st_copy(qb, 0, 0).wait_recv()
                    st_copy(qb, 1, k).start()

            @pl.when(has_above & (z > 0))
            def _():
                qg_copy(qb, 0, k, p).start()
                if p == 0:
                    st_copy(qb, 0, k).start()

        def turn(c, carry):
            dist = k - c
            other = jnp.where(c == 0, y, 1 - y)
            bz, qz = z - dist, z + dist
            use_kv = (bz >= 0) & (dist < nz) & ((dist > 0) | (y == 1))
            use_qg = (qz < nz) & (dist < nz) & ((dist > 0) | (y == 0))
            kblk = jnp.maximum(bz, 0) * 2 + other
            qblk = jnp.minimum(qz, nz - 1) * 2 + other

            @pl.when(use_kv)
            def _():
                @pl.when(c == 1)
                def _():
                    for p in range(2):
                        kv_copy(kblk, 1, 0, p).wait_recv()
                query_side(kvb.at[kblk, 0], kvb.at[kblk, 1], False)

            @pl.when(use_qg)
            def _():
                @pl.when(c == 1)
                def _():
                    for p in range(2):
                        qg_copy(qblk, 1, 0, p).wait_recv()
                    st_copy(qblk, 1, 0).wait_recv()
                key_side(qgb.at[qblk, 0], qgb.at[qblk, 1], stb.at[qblk], False)
            return carry
        lax.fori_loop(0, 2, turn, 0)
        return carry

    lax.fori_loop(1, nz + 1, step, 0)

    own_dq[...] = (dq_acc[...] * score_scale).astype(BF16)
    half = rows // 2

    def dq_copy(block, lane, idx, p, own=False):
        to = (jnp.minimum(s + 2, nsp - 2 + y), jnp.maximum(s - 2, y), side)[lane]
        at = pl.ds(p * half, half)
        return copy(own_dq.at[at] if own else dqb.at[block, at], dqb.at[block, at],
                    dq_s.at[lane, p, idx], dq_r.at[p, block], to)

    for p in range(2):
        @pl.when(z < nz - 1)
        def _():
            dq_copy(s, 0, z, p, True).start()

        @pl.when(z > 0)
        def _():
            dq_copy(s, 1, z, p, True).start()

        dq_copy(s, 2, z, p, True).start()

    for h in range(heads):
        at = slice(h * width, (h + 1) * width)
        dq_out[:, h, :] = own_dq[:, at]
        dk_out[:, h, :] = (dk_acc[:, at] * score_scale).astype(BF16)
        dv_out[:, h, :] = dv_acc[:, at].astype(BF16)

    own_lat().wait()
    for d in range(1, nsp):
        lat_copy(d).wait_recv()
    for d in range(1, ntp):
        share_copy(d).start()
    for d in range(1, ntp):
        share_copy(d).wait_recv()

    wg_out[...] = dot_tn(latb[s], own_dq[...])

    def add_block(block):
        wg_out[...] += dot_tn(latb[block], dqb[block])

    def gather(k, carry):
        for p in range(2):
            for lane, there, ok, more in (
                (0, z - k, z - k >= 0, z < nz - 1),
                (1, z + k, z + k < nz, z > 0),
            ):
                bz = jnp.clip(there, 0, nz - 1)
                block = bz * 2 + y

                @pl.when(ok)
                def _():
                    dq_copy(block, lane, bz, p).wait_recv()
                    dq_copy(block, 2, bz, p).start()

                @pl.when(ok & more)
                def _():
                    dq_copy(block, lane, bz, p).start()

        def turn(c, carry):
            dist = jnp.where(c < 2, k, k - 1)
            up = lax.rem(c, 2)
            bz = jnp.where(up == 0, z - dist, z + dist)
            ok = (bz >= 0) & (bz < nz) & (dist < nz) & ((dist > 0) | (up == 0))
            other = jnp.where(c < 2, y, 1 - y)
            block = jnp.clip(bz, 0, nz - 1) * 2 + other

            @pl.when(ok)
            def _():
                @pl.when(c >= 2)
                def _():
                    for p in range(2):
                        dq_copy(block, 2, 0, p).wait_recv()
                add_block(block)
            return carry
        lax.fori_loop(0, 4, turn, 0)
        return carry

    lax.fori_loop(1, nz + 1, gather, 0)

    def drain(k, carry):
        below, above = z - k, z + k
        has_below, has_above = below >= 0, above < nz

        for p in range(2):
            @pl.when(has_below & (z < nz - 1))
            def _():
                kv_copy(s, 0, k, p).wait_send()

            @pl.when(has_below & ((k > 0) | (y == 0)))
            def _():
                kv_copy(s, 1, k, p).wait_send()

            @pl.when(has_above & (z > 0))
            def _():
                qg_copy(s, 0, k, p).wait_send()
                if p == 0:
                    st_copy(s, 0, k).wait_send()

            @pl.when(has_above & ((k > 0) | (y == 1)))
            def _():
                qg_copy(s, 1, k, p).wait_send()
                if p == 0:
                    st_copy(s, 1, k).wait_send()

            @pl.when((k <= z) & (z < nz - 1))
            def _():
                dq_copy(s, 0, k, p).wait_send()

            @pl.when((k >= z) & (z > 0))
            def _():
                dq_copy(s, 1, k, p).wait_send()

            dq_copy(s, 2, k, p).wait_send()
        return carry

    lax.fori_loop(0, nz, drain, 0)
    for d in range(1, nsp):
        lat_copy(d).wait_send()
    for d in range(1, ntp):
        share_copy(d).wait_send()


def vmem():
    return pl.BlockSpec(memory_space=pltpu.VMEM)


def body(nsp, ntp, latents, query_heads, key_heads, value_heads, map_outputs, log_sums, out_grad,
         mix_lambda, norm_gain):
    rows, heads, width = query_heads.shape
    flat = (rows, heads * width)
    slab = latents.shape[1] // nsp
    nz = nsp // 2
    dma = pltpu.SemaphoreType.DMA
    dq, dk, dv, wg = pl.pallas_call(
        functools.partial(main_kernel, nsp, ntp, heads, width),
        out_shape=(
            jax.ShapeDtypeStruct(query_heads.shape, BF16),
            jax.ShapeDtypeStruct(query_heads.shape, BF16),
            jax.ShapeDtypeStruct(query_heads.shape, BF16),
            jax.ShapeDtypeStruct((slab, heads * width), F32),
        ),
        in_specs=[pl.BlockSpec(memory_space=pltpu.SMEM)] + [vmem()] * 8,
        out_specs=(vmem(),) * 4,
        scratch_shapes=[
            pltpu.VMEM(flat, BF16),
            pltpu.VMEM((heads, rows, width), F32),
            pltpu.VMEM((heads, 4, rows), F32),
            pltpu.VMEM(flat, BF16),
            pltpu.VMEM((nsp, 2) + flat, BF16),
            pltpu.VMEM((nsp, 2) + flat, BF16),
            pltpu.VMEM((nsp, heads, 4, rows), F32),
            pltpu.VMEM((nsp,) + flat, BF16),
            pltpu.VMEM((nsp, rows, slab), BF16),
            pltpu.VMEM(flat, F32),
            pltpu.VMEM(flat, F32),
            pltpu.VMEM(flat, F32),
            dma((2, 2, nz)), dma((2, 2, nz)), dma((2, nz)), dma((3, 2, nz)),
            dma((2, nsp)), dma((2, nsp)), dma((nsp,)), dma((2, nsp)),
            dma((nsp,)), dma((nsp,)), dma((ntp,)), dma((ntp,)),
            dma,
        ],
        compiler_params=pltpu.CompilerParams(collective_id=0, has_side_effects=True),
        name="main",
    )(
        mix_lambda,
        norm_gain[None, :],
        latents,
        key_heads.reshape(flat),
        value_heads.reshape(flat),
        query_heads.reshape(flat),
        map_outputs,
        out_grad,
        jnp.transpose(log_sums, (1, 0, 2)),
    )
    return dq, dk, dv, wg


def row_norm_backward(heads, width, lam_ref, gain_ref, mo_ref, og_ref, lse_ref, grad_ref, row_ref):
    for h in range(heads):
        first = mo_ref[:, 0, h, :].astype(F32)
        second = mo_ref[:, 1, h, :].astype(F32)
        lam = lam_ref[h]
        combined = first - lam * second
        inverse = lax.rsqrt(jnp.mean(combined * combined, axis=-1, keepdims=True) + EPSILON)
        weighted = gain_ref[...] * og_ref[:, h, :].astype(F32)
        grad = (
            inverse * weighted
            - inverse**3 * combined * jnp.mean(combined * weighted, axis=-1, keepdims=True)
        ).astype(BF16)
        grad_ref[:, h * width : (h + 1) * width] = grad
        wide = grad.astype(F32)
        log_lam = jnp.log(jnp.full((1, 1), lam, F32)) * LOG2E
        row_ref[h, 0:1] = lse_ref[h, 0:1] * LOG2E
        row_ref[h, 1:2] = lse_ref[h, 1:2] * LOG2E - log_lam
        lane = lax.broadcasted_iota(jnp.int32, wide.shape, 1)
        terms = jnp.where(lane == 0, jnp.sum(wide * first, axis=-1, keepdims=True),
                          jnp.sum(wide * second, axis=-1, keepdims=True))
        row_ref[h, 2:4] = jnp.transpose(terms)[0:2]


def hub_kernel(nsp, ntp, heads, width, lam, gain, lat, own_k, own_v, own_q, mo, og, lse,
               dq_out, dk_out, dv_out, wg_out,
               own_g, row, blk, stb, dq_acc, dk_acc, dv_acc, db, out_b, in_b, in_a, kt, kin, kst, kret, latb,
               f_s, z_s, r_s, b_r, st_r, d_s, d_r, ob_s, ib_r, ia_r, kt_s, kin_r, tot_s, kst_s, kret_r,
               la_s, la_r, lb_s, lb_r, own_sem):
    nz = nsp // 2
    low, high, top = nz // 2 - 1, nz // 2, nz - 1
    s = lax.axis_index("sp")
    t = lax.axis_index("tp")
    z, y = s // 2, lax.rem(s, 2)
    rows = own_k.shape[0]
    span = 2 * rows
    pair = heads // 2
    lanes = pair * width
    part = rows // ntp
    slab = lat.shape[1] // nsp
    score_scale = (width // 2) ** (-0.5)
    exp_scale = score_scale * LOG2E
    partner = 2 * z + 1 - y
    Q, K, V, G, ST = range(5)

    barrier = pltpu.get_barrier_semaphore()
    for d in range(1, nsp):
        pl.semaphore_signal(barrier, inc=1, device_id={"sp": lax.rem(s + d, nsp)}, device_id_type=MESH)
    for d in range(1, ntp):
        pl.semaphore_signal(barrier, inc=1, device_id={"tp": lax.rem(t + d, ntp)}, device_id_type=MESH)
    pl.semaphore_wait(barrier, nsp - 1 + ntp - 1)

    def copy(src, dst, send, recv, to):
        return pltpu.make_async_remote_copy(
            src_ref=src, dst_ref=dst, send_sem=send, recv_sem=recv,
            device_id={"sp": to}, device_id_type=MESH)

    def at_level(level):
        return 2 * level + y

    def lane_of(p):
        return pl.ds(pl.multiple_of(p * lanes, lanes), lanes)

    def half_of(p):
        return pl.ds(pl.multiple_of(p * rows, rows), rows)

    owned = (own_q, own_k, own_v, own_g)

    def source(a, p):
        if a == ST:
            return row.at[pl.ds(p * pair, pair)]
        return owned[a].at[:, lane_of(p)]

    def landing(a, level, half):
        return stb.at[level, half] if a == ST else blk.at[a, level, half_of(half), :]

    def landed(a, level, half):
        return st_r.at[level, half] if a == ST else b_r.at[a, level, half]

    def swap(a):
        return copy(source(a, 1 - y), landing(a, z, y), f_s.at[a], landed(a, z, y), partner)

    def arrive(a, level, half):
        copy(landing(a, level, half), landing(a, level, half), f_s.at[a], landed(a, level, half), partner).wait_recv()

    def pass_on(a, own):
        half = y if own else 1 - y
        return copy(source(a, y) if own else landing(a, z, half), landing(a, z, half),
                    z_s.at[a, 0 if own else 1], landed(a, z, half), at_level(jnp.where(z > high, high, low)))

    def passes(action, arrays, own):
        for a in arrays:
            if a in (K, V):
                @pl.when(z < low)
                def _():
                    action(pass_on(a, own))
            else:
                @pl.when(z >= high)
                def _():
                    action(pass_on(a, own))

    def relay(a, half):
        return copy(landing(a, top, half), landing(a, top, half), r_s.at[a, half], landed(a, top, half), at_level(low))

    def relays(arrays, half):
        @pl.when(z == high)
        def _():
            for a in arrays:
                arrive(a, top, half)
                relay(a, half).start()

    def start(c):
        c.start()

    def lat_copy(d):
        to = lax.rem(s + d, nsp)
        mine = pl.ds(pl.multiple_of(t * part, part), part)
        return copy(lat.at[mine, pl.ds(pl.multiple_of(to * slab, slab), slab)],
                    latb.at[s, mine, :], la_s.at[d], la_r.at[s], to)

    def own_lat():
        return pltpu.make_async_copy(
            lat.at[:, pl.ds(pl.multiple_of(s * slab, slab), slab)], latb.at[s], own_sem)

    def share_copy(b, d):
        mine = pl.ds(pl.multiple_of(t * part, part), part)
        return pltpu.make_async_remote_copy(
            src_ref=latb.at[b, mine, :], dst_ref=latb.at[b, mine, :],
            send_sem=lb_s.at[b, d], recv_sem=lb_r.at[b, d],
            device_id={"tp": lax.rem(t + d, ntp)}, device_id_type=MESH)

    def group_of(src, dst, group):
        sz, dz = src // 2, dst // 2
        first = (lax.rem(src, 2) == lax.rem(dst, 2)) & ((dz > sz) | ((dz < sz) & (sz < high)))
        last = (sz >= high) & (dz < high)
        return first if group == 0 else last if group == 2 else jnp.logical_not(first | last)

    def lat_send(group):
        for d in range(1, nsp):
            @pl.when(group_of(s, lax.rem(s + d, nsp), group))
            def _():
                lat_copy(d).start()

    def lat_share(group):
        def step(d, carry):
            b = lax.rem(s + d, nsp)

            @pl.when(group_of(b, s, group))
            def _():
                mine = pl.ds(pl.multiple_of(t * part, part), part)
                copy(latb.at[b, mine, :], latb.at[b, mine, :], la_s.at[1], la_r.at[b], partner).wait_recv()
                for e in range(1, ntp):
                    share_copy(b, e).start()
            return carry
        lax.fori_loop(1, nsp, step, 0)

    swap(Q).start()
    passes(start, (Q, K, V), True)
    swap(K).start()
    swap(V).start()
    lat_send(0)
    own_lat().start()

    row_norm_backward(heads, width, lam, gain, mo, og, lse, own_g, row)

    swap(G).start()
    swap(ST).start()
    passes(start, (ST, G), True)

    for a in (Q, K, V, G):
        blk[a, z, half_of(y), :] = owned[a][:, lane_of(y)]
    stb[z, y] = row[pl.ds(y * pair, pair)]
    dq_acc[...] = jnp.zeros_like(dq_acc)
    dk_acc[...] = jnp.zeros_like(dk_acc)
    dv_acc[...] = jnp.zeros_like(dv_acc)

    for a in (Q, K, V, ST, G):
        arrive(a, z, 1 - y)
        passes(start, (a,), False)
        if a == Q:
            relays((Q,), y)
        if a == G:
            relays((Q,), 1 - y)
            relays((ST, G), y)

    lane_id = lax.broadcasted_iota(jnp.int32, (1, width), 1)
    first_map = jnp.where(lane_id < width // 2, 1.0, 0.0).astype(BF16)
    second_map = jnp.where(lane_id < width // 2, 0.0, 1.0).astype(BF16)

    def split(x):
        return jnp.concatenate([x * first_map, x * second_map], axis=0)

    def visit(qz, kz, slot, diagonal):
        def one(h, carry):
            at = pl.ds(pl.multiple_of(h * width, width), width)
            for a in range(2):
                start_row = a * rows if diagonal else 0
                kr = pl.ds(a * rows, rows)
                qr = pl.ds(start_row, span - start_row)
                count = span - start_row
                keys = split(blk[K, kz, kr, at])
                queries = split(blk[Q, qz, qr, at])
                grads = blk[G, qz, qr, at]
                scores = dot_nt(blk[K, kz, kr, at], queries)
                mixed = dot_nt(blk[V, kz, kr, at], grads)
                stats = jnp.concatenate([stb[qz, p, h] for p in range(start_row // rows, 2)], axis=1)
                x1 = scores[:, :count] * exp_scale - stats[0:1]
                x2 = scores[:, count:] * exp_scale - stats[1:2]
                if diagonal:
                    seen = (lax.broadcasted_iota(jnp.int32, (rows, count), 0)
                            <= lax.broadcasted_iota(jnp.int32, (rows, count), 1))
                    x1 = jnp.where(seen, x1, -jnp.inf)
                    x2 = jnp.where(seen, x2, -jnp.inf)
                p1 = jnp.exp2(x1)
                p2 = jnp.exp2(x2)
                g1 = (p1 * (mixed - stats[2:3])).astype(BF16)
                g2 = (p2 * (stats[3:4] - mixed)).astype(BF16)
                dv_acc[slot, kr, at] += dot_nn((p1 - p2).astype(BF16), grads)
                dk_acc[slot, kr, at] += dot_nn(jnp.concatenate([g1, g2], axis=1), queries)
                dq_acc[qz, h, :, qr] += dot_tn(keys, jnp.concatenate([g1, g2], axis=0))
            return carry
        lax.fori_loop(0, pair, one, 0)

    def dq_value(level):
        return jnp.concatenate([jnp.transpose(dq_acc[level, h]) for h in range(pair)], axis=1) * score_scale

    def grad_copy(level, lane):
        if lane == 0:
            to = partner
        elif lane == 1:
            to = at_level(jnp.where(z == low, 0, jnp.where(z == high, top, low)))
        else:
            to = at_level(high)
        return copy(db.at[level, y], db.at[level, y], d_s.at[level, lane], d_r.at[level, y], to)

    def grad_lanes(level):
        chained = (z == high) | ((z == low) if level >= low else (z < low))
        if level > low:
            return ((0, None), (1, chained))
        return ((0, None), (1, chained), (2, z == level))

    def grad_each(level, action):
        for lane, ok in reversed(grad_lanes(level)):
            if ok is None:
                action(grad_copy(level, lane))
            else:
                @pl.when(ok)
                def _():
                    action(grad_copy(level, lane))

    def grad_arrive(level, p):
        copy(db.at[level, p], db.at[level, p], d_s.at[level, 0], d_r.at[level, p], partner).wait_recv()

    def part_copy(i):
        return copy(out_b.at[i], in_b.at[i], ob_s.at[i], ib_r.at[i], at_level(jnp.where(z == low, high, low)))

    def top_copy():
        return copy(out_b.at[0], in_a, ob_s.at[0], ia_r, at_level(high))

    def key_copy(i):
        return copy(kt.at[i], kin.at[i], kt_s.at[i], kin_r.at[i], at_level(low))

    def total_copy(i, half):
        return copy(kt.at[i, half_of(half), :], kret.at[i, y], tot_s.at[i, half], kret_r.at[i, y], half)

    def return_copy(i):
        return copy(kst.at[i], kret.at[i, y], kst_s.at[i], kret_r.at[i, y], partner)

    visit(z, z, 0, True)

    @pl.when(z < low)
    def _():
        db[0, y] = dq_value(0).astype(BF16)
        grad_each(0, start)
        for i in range(2):
            kt[i] = (dv_acc[0] if i else dk_acc[0] * score_scale).astype(BF16)
            key_copy(i).start()

    @pl.when(z >= high)
    def _():
        out_b[0] = dq_value(z).astype(BF16)

    @pl.when(z == high)
    def _():
        part_copy(0).start()

    @pl.when(z > high)
    def _():
        top_copy().start()

    lat_send(1)
    lat_share(0)

    @pl.when(z == low)
    def _():
        def step(i, carry):
            qz = jnp.where(i == 0, low, high + (i - 1) // 2)
            kz = jnp.where(i == 0, 0, lax.rem(i - 1, 2))

            @pl.when(i == 0)
            def _():
                for half in range(2):
                    arrive(K, 0, half)
                    arrive(V, 0, half)

            @pl.when((i > 0) & (kz == 0))
            def _():
                for a in (Q, ST, G):
                    for half in range(2):
                        arrive(a, qz, half)

            visit(qz, kz, 1 - kz, False)

            @pl.when(i == 0)
            def _():
                db[low, y] = dq_value(low).astype(BF16)
                grad_each(low, start)

            @pl.when((i > 0) & (kz == 1))
            def _():
                out_b[qz - high] = dq_value(qz).astype(BF16)
                part_copy(qz - high).start()

            @pl.when((qz == top) & (kz == 0))
            def _():
                for j in range(2):
                    key_copy(j).wait_recv()
                    acc = dv_acc[1] if j else dk_acc[1] * score_scale
                    kt[j] = (acc + kin[j].astype(F32)).astype(BF16)
                    for half in range(2):
                        total_copy(j, half).start()
            return carry
        lax.fori_loop(0, 5, step, 0)

    relays((ST, G), 1 - y)

    @pl.when(z == high)
    def _():
        visit(top, high, 0, False)
        top_copy().wait_recv()
        out_b[1] = (dq_value(top) + in_a[...].astype(F32)).astype(BF16)
        part_copy(1).start()

    lat_send(2)

    @pl.when(z >= low)
    def _():
        for i, acc, scale in ((0, dk_acc, score_scale), (1, dv_acc, 1.0)):
            kst[i] = (acc[0, half_of(1 - y), :] * scale).astype(BF16)
            return_copy(i).start()
            kret[i, y] = (acc[0, half_of(y), :] * scale).astype(BF16)

    for level in (0, low):
        @pl.when(z != level)
        def _():
            grad_arrive(level, y)
            grad_each(level, start)

    lat_share(1)

    for level in (high, top):
        i = level - high

        @pl.when((z == low) | (z == high))
        def _():
            part_copy(i).wait_recv()
            total = dq_value(level) + in_b[i].astype(F32)
            if level == top:
                above = in_a[...].astype(F32)
                total = total + jnp.where(z == high, above, jnp.zeros_like(above))
            db[level, y] = total.astype(BF16)

        @pl.when((z != low) & (z != high))
        def _():
            grad_arrive(level, y)
        grad_each(level, start)

    lat_share(2)
    own_lat().wait()

    for level in range(nz):
        grad_arrive(level, 1 - y)
        for half in range(2):
            b = 2 * level + half

            @pl.when(s != b)
            def _():
                for e in range(1, ntp):
                    share_copy(b, e).wait_recv()
        feed = latb[2 * level : 2 * level + 2].reshape(span, slab)
        for p in range(2):
            at = slice(p * lanes, (p + 1) * lanes)
            term = dot_tn(feed, db[level, p])
            if level == 0:
                wg_out[:, at] = term
            else:
                wg_out[:, at] += term

    for i in range(2):
        copy(kst.at[i], kret.at[i, 1 - y], kst_s.at[i], kret_r.at[i, 1 - y], partner).wait_recv()

        @pl.when(z < low)
        def _():
            copy(kst.at[i], kret.at[i, y], kst_s.at[i], kret_r.at[i, y], partner).wait_recv()
        out = dk_out if i == 0 else dv_out
        for p in range(2):
            out[:, p * lanes : (p + 1) * lanes] = kret[i, p]
    for p in range(2):
        dq_out[:, p * lanes : (p + 1) * lanes] = db[z, p, half_of(y), :]

    def sent(c):
        c.wait_send()

    for a in range(5):
        sent(swap(a))
    for own in (True, False):
        passes(sent, (Q, K, V, ST, G), own)
    for a in (Q, ST, G):
        @pl.when(z == high)
        def _():
            for half in range(2):
                sent(relay(a, half))
    for level in range(nz):
        grad_each(level, sent)
    for i in range(2):
        @pl.when(z >= low)
        def _():
            sent(return_copy(i))

        @pl.when((z == low) | (z == high))
        def _():
            sent(part_copy(i))

        @pl.when(z == low)
        def _():
            for half in range(2):
                sent(total_copy(i, half))

        @pl.when(z < low)
        def _():
            sent(key_copy(i))

    @pl.when(z > high)
    def _():
        sent(top_copy())
    for d in range(1, nsp):
        sent(lat_copy(d))

    def drain(d, carry):
        for e in range(1, ntp):
            sent(share_copy(lax.rem(s + d, nsp), e))
        return carry
    lax.fori_loop(1, nsp, drain, 0)


def hub_body(nsp, ntp, latents, query_heads, key_heads, value_heads, map_outputs, log_sums, out_grad,
             mix_lambda, norm_gain):
    rows, heads, width = query_heads.shape
    flat = (rows, heads * width)
    slab = latents.shape[1] // nsp
    nz = nsp // 2
    pair = heads // 2
    block = (2 * rows, pair * width)
    half = (rows, pair * width)
    dma = pltpu.SemaphoreType.DMA
    dq, dk, dv, wg = pl.pallas_call(
        functools.partial(hub_kernel, nsp, ntp, heads, width),
        out_shape=(
            jax.ShapeDtypeStruct(flat, BF16),
            jax.ShapeDtypeStruct(flat, BF16),
            jax.ShapeDtypeStruct(flat, BF16),
            jax.ShapeDtypeStruct((slab, heads * width), F32),
        ),
        in_specs=[pl.BlockSpec(memory_space=pltpu.SMEM)] + [vmem()] * 8,
        out_specs=(vmem(),) * 4,
        scratch_shapes=[
            pltpu.VMEM(flat, BF16),
            pltpu.VMEM((heads, 4, rows), F32),
            pltpu.VMEM((4, nz) + block, BF16),
            pltpu.VMEM((nz, 2, pair, 4, rows), F32),
            pltpu.VMEM((nz, pair, width, 2 * rows), F32),
            pltpu.VMEM((2,) + block, F32),
            pltpu.VMEM((2,) + block, F32),
            pltpu.VMEM((nz, 2) + block, BF16),
            pltpu.VMEM((2,) + block, BF16),
            pltpu.VMEM((2,) + block, BF16),
            pltpu.VMEM(block, BF16),
            pltpu.VMEM((2,) + block, BF16),
            pltpu.VMEM((2,) + block, BF16),
            pltpu.VMEM((2,) + half, BF16),
            pltpu.VMEM((2, 2) + half, BF16),
            pltpu.VMEM((nsp, rows, slab), BF16),
            dma((5,)), dma((5, 2)), dma((5, 2)), dma((4, nz, 2)), dma((nz, 2)), dma((nz, 3)), dma((nz, 2)),
            dma((2,)), dma((2,)), dma, dma((2,)), dma((2,)), dma((2, 2)), dma((2,)), dma((2, 2)),
            dma((nsp,)), dma((nsp,)), dma((nsp, ntp)), dma((nsp, ntp)),
            dma,
        ],
        compiler_params=pltpu.CompilerParams(collective_id=0, has_side_effects=True),
        name="hub",
    )(
        mix_lambda,
        norm_gain[None, :],
        latents,
        key_heads.reshape(flat),
        value_heads.reshape(flat),
        query_heads.reshape(flat),
        map_outputs,
        out_grad,
        jnp.transpose(log_sums, (1, 2, 0)),
    )
    return tuple(a.reshape(query_heads.shape) for a in (dq, dk, dv)) + (wg,)


def solution(mesh):
    placed = (
        P("sp", None),
        P("sp", "tp", None),
        P("sp", "tp", None),
        P("sp", "tp", None),
        P("sp", None, "tp", None),
        P("sp", "tp", None),
        P("sp", "tp", None),
        P("tp"),
        P(),
    )
    nsp, ntp = mesh.shape["sp"], mesh.shape["tp"]

    def chosen(*args):
        heads = args[1].shape[1]
        return (hub_body if nsp == 8 and heads % 2 == 0 else body)(nsp, ntp, *args)

    return jax.shard_map(
        chosen,
        mesh=mesh,
        in_specs=placed,
        out_specs=(P("sp", "tp", None), P("sp", "tp", None), P("sp", "tp", None), P("sp", "tp")),
        check_vma=False,
    )
```

```python
import functools
import math

import jax
import jax.numpy as jnp
from jax import lax
from jax.experimental import pallas as pl
from jax.experimental.pallas import tpu as pltpu
from jax.sharding import PartitionSpec as P

EPSILON = 1e-05
LOG2E = math.log2(math.e)
F32 = jnp.float32
BF16 = jnp.bfloat16
MESH = pl.DeviceIdType.MESH


def dot_nn(a, b):
    return lax.dot_general(a, b, (((1,), (0,)), ((), ())), preferred_element_type=F32)


def dot_nt(a, b):
    return lax.dot_general(a, b, (((1,), (1,)), ((), ())), preferred_element_type=F32)


def dot_tn(a, b):
    return lax.dot_general(a, b, (((0,), (0,)), ((), ())), preferred_element_type=F32)


def norm_backward(heads, width, lam_ref, gain_ref, mo_ref, og_ref, lse_ref, grad_ref, col_ref, row_ref):
    for h in range(heads):
        first = mo_ref[:, 0, h, :].astype(F32)
        second = mo_ref[:, 1, h, :].astype(F32)
        lam = lam_ref[h]
        combined = first - lam * second
        inverse = lax.rsqrt(jnp.mean(combined * combined, axis=-1, keepdims=True) + EPSILON)
        weighted = gain_ref[...] * og_ref[:, h, :].astype(F32)
        grad = (
            inverse * weighted
            - inverse**3 * combined * jnp.mean(combined * weighted, axis=-1, keepdims=True)
        ).astype(BF16)
        grad_ref[:, h * width : (h + 1) * width] = grad
        wide = grad.astype(F32)
        lse = lse_ref[h] * LOG2E
        log_lam = jnp.log(jnp.full((1, 1), lam, F32)) * LOG2E
        lane = lax.broadcasted_iota(jnp.int32, wide.shape, 1)
        stats = jnp.where(lane == 0, lse[:, 0:1], lse[:, 1:2] - log_lam)
        stats = jnp.where(lane == 2, jnp.sum(wide * first, axis=-1, keepdims=True), stats)
        stats = jnp.where(lane == 3, jnp.sum(wide * second, axis=-1, keepdims=True), stats)
        col_ref[h] = stats
        row_ref[h] = jnp.transpose(stats)[0:4]


def main_kernel(nsp, ntp, heads, width, lam, gain, lat, own_k, own_v, own_q, mo, og, lse,
                dq_out, dk_out, dv_out, wg_out,
                own_g, col, row, own_dq, kvb, qgb, stb, dqb, latb, dq_acc, dk_acc, dv_acc,
                kv_s, qg_s, st_s, dq_s, kv_r, qg_r, st_r, dq_r,
                la_s, la_r, lb_s, lb_r, own_sem):
    nz = nsp // 2
    s = lax.axis_index("sp")
    t = lax.axis_index("tp")
    z, y = s // 2, lax.rem(s, 2)
    rows = own_k.shape[0]
    part = rows // ntp
    slab = lat.shape[1] // nsp
    score_scale = (width // 2) ** (-0.5)
    exp_scale = score_scale * LOG2E

    barrier = pltpu.get_barrier_semaphore()
    for d in range(1, nsp):
        pl.semaphore_signal(barrier, inc=1, device_id={"sp": lax.rem(s + d, nsp)}, device_id_type=MESH)
    for d in range(1, ntp):
        pl.semaphore_signal(barrier, inc=1, device_id={"tp": lax.rem(t + d, ntp)}, device_id_type=MESH)
    pl.semaphore_wait(barrier, nsp - 1 + ntp - 1)

    def copy(src, dst, send, recv, to):
        return pltpu.make_async_remote_copy(
            src_ref=src, dst_ref=dst, send_sem=send, recv_sem=recv,
            device_id={"sp": to}, device_id_type=MESH)

    side = 2 * z + (1 - y)

    def kv_copy(block, lane, k, p, src=None):
        to = jnp.minimum(s + 2, nsp - 1) if lane == 0 else side
        return copy(kvb.at[block, p] if src is None else src, kvb.at[block, p],
                    kv_s.at[lane, p, k], kv_r.at[p, block], to)

    def qg_copy(block, lane, k, p, src=None):
        to = jnp.maximum(s - 2, 0) if lane == 0 else side
        return copy(qgb.at[block, p] if src is None else src, qgb.at[block, p],
                    qg_s.at[lane, p, k], qg_r.at[p, block], to)

    def st_copy(block, lane, k, src=None):
        to = jnp.maximum(s - 2, 0) if lane == 0 else side
        return copy(stb.at[block] if src is None else src, stb.at[block],
                    st_s.at[lane, k], st_r.at[block], to)

    for p, src in ((0, own_k), (1, own_v)):
        @pl.when(z < nz - 1)
        def _():
            kv_copy(s, 0, 0, p, src).start()

        @pl.when(y == 0)
        def _():
            kv_copy(s, 1, 0, p, src).start()

    @pl.when(z > 0)
    def _():
        qg_copy(s, 0, 0, 0, own_q).start()

    @pl.when(y == 1)
    def _():
        qg_copy(s, 1, 0, 0, own_q).start()

    norm_backward(heads, width, lam, gain, mo, og, lse, own_g, col, row)

    @pl.when(z > 0)
    def _():
        st_copy(s, 0, 0, row).start()
        qg_copy(s, 0, 0, 1, own_g).start()

    @pl.when(y == 1)
    def _():
        st_copy(s, 1, 0, row).start()
        qg_copy(s, 1, 0, 1, own_g).start()

    lane_id = lax.broadcasted_iota(jnp.int32, (1, width), 1)
    low = jnp.where(lane_id < width // 2, 1.0, 0.0).astype(BF16)
    high = jnp.where(lane_id < width // 2, 0.0, 1.0).astype(BF16)

    def split(x):
        return jnp.concatenate([x * low, x * high], axis=0)

    def query_side(k_at, v_at, diagonal):
        def one(h, carry):
            at = pl.ds(pl.multiple_of(h * width, width), width)
            keys = split(k_at[:, at])
            scores = dot_nt(own_q[:, at], keys)
            mixed = dot_nt(own_g[:, at], v_at[:, at])
            stats = col[h]
            x1 = scores[:, :rows] * exp_scale - stats[:, 0:1]
            x2 = scores[:, rows:] * exp_scale - stats[:, 1:2]
            if diagonal:
                seen = (lax.broadcasted_iota(jnp.int32, (rows, rows), 1)
                        <= lax.broadcasted_iota(jnp.int32, (rows, rows), 0))
                x1 = jnp.where(seen, x1, -jnp.inf)
                x2 = jnp.where(seen, x2, -jnp.inf)
            g1 = (jnp.exp2(x1) * (mixed - stats[:, 2:3])).astype(BF16)
            g2 = (jnp.exp2(x2) * (stats[:, 3:4] - mixed)).astype(BF16)
            part_dq = dot_nn(jnp.concatenate([g1, g2], axis=1), keys)
            if diagonal:
                dq_acc[:, at] = part_dq
            else:
                dq_acc[:, at] += part_dq
            return carry
        lax.fori_loop(0, heads, one, 0)

    def key_side(q_at, g_at, row_at, diagonal):
        def one(h, carry):
            at = pl.ds(pl.multiple_of(h * width, width), width)
            queries = split(q_at[:, at])
            grads = g_at[:, at]
            scores = dot_nt(own_k[:, at], queries)
            mixed = dot_nt(own_v[:, at], grads)
            stats = row_at[h]
            x1 = scores[:, :rows] * exp_scale - stats[0:1]
            x2 = scores[:, rows:] * exp_scale - stats[1:2]
            if diagonal:
                seen = (lax.broadcasted_iota(jnp.int32, (rows, rows), 0)
                        <= lax.broadcasted_iota(jnp.int32, (rows, rows), 1))
                x1 = jnp.where(seen, x1, -jnp.inf)
                x2 = jnp.where(seen, x2, -jnp.inf)
            p1 = jnp.exp2(x1)
            p2 = jnp.exp2(x2)
            g1 = (p1 * (mixed - stats[2:3])).astype(BF16)
            g2 = (p2 * (stats[3:4] - mixed)).astype(BF16)
            part_dv = dot_nn((p1 - p2).astype(BF16), grads)
            part_dk = dot_nn(jnp.concatenate([g1, g2], axis=1), queries)
            if diagonal:
                dv_acc[:, at] = part_dv
                dk_acc[:, at] = part_dk
            else:
                dv_acc[:, at] += part_dv
                dk_acc[:, at] += part_dk
            return carry
        lax.fori_loop(0, heads, one, 0)

    def lat_copy(d):
        to = lax.rem(s + d, nsp)
        mine = pl.ds(pl.multiple_of(t * part, part), part)
        return copy(lat.at[mine, pl.ds(pl.multiple_of(to * slab, slab), slab)],
                    latb.at[s, mine, :], la_s.at[d], la_r.at[d], to)

    def own_lat():
        return pltpu.make_async_copy(
            lat.at[pl.ds(pl.multiple_of(t * part, part), part), pl.ds(pl.multiple_of(s * slab, slab), slab)],
            latb.at[s, pl.ds(pl.multiple_of(t * part, part), part), :], own_sem)

    def share_copy(d):
        mine = pl.ds(pl.multiple_of(t * part, part), part)
        return pltpu.make_async_remote_copy(
            src_ref=latb.at[:, mine, :], dst_ref=latb.at[:, mine, :],
            send_sem=lb_s.at[d], recv_sem=lb_r.at[d],
            device_id={"tp": lax.rem(t + d, ntp)}, device_id_type=MESH)

    own_lat().start()
    query_side(own_k, own_v, True)
    key_side(own_q, own_g, row, True)
    for d in range(1, nsp):
        lat_copy(d).start()

    def step(k, carry):
        below, above = z - k, z + k
        has_below, has_above = below >= 0, above < nz
        kb = jnp.maximum(below, 0) * 2 + y
        qb = jnp.minimum(above, nz - 1) * 2 + y

        for p in range(2):
            @pl.when(has_below)
            def _():
                kv_copy(kb, 0, 0, p).wait_recv()
                kv_copy(kb, 1, k, p).start()

            @pl.when(has_below & (z < nz - 1))
            def _():
                kv_copy(kb, 0, k, p).start()

            @pl.when(has_above)
            def _():
                qg_copy(qb, 0, 0, p).wait_recv()
                qg_copy(qb, 1, k, p).start()
                if p == 0:
                    st_copy(qb, 0, 0).wait_recv()
                    st_copy(qb, 1, k).start()

            @pl.when(has_above & (z > 0))
            def _():
                qg_copy(qb, 0, k, p).start()
                if p == 0:
                    st_copy(qb, 0, k).start()

        def turn(c, carry):
            dist = k - c
            other = jnp.where(c == 0, y, 1 - y)
            bz, qz = z - dist, z + dist
            use_kv = (bz >= 0) & (dist < nz) & ((dist > 0) | (y == 1))
            use_qg = (qz < nz) & (dist < nz) & ((dist > 0) | (y == 0))
            kblk = jnp.maximum(bz, 0) * 2 + other
            qblk = jnp.minimum(qz, nz - 1) * 2 + other

            @pl.when(use_kv)
            def _():
                @pl.when(c == 1)
                def _():
                    for p in range(2):
                        kv_copy(kblk, 1, 0, p).wait_recv()
                query_side(kvb.at[kblk, 0], kvb.at[kblk, 1], False)

            @pl.when(use_qg)
            def _():
                @pl.when(c == 1)
                def _():
                    for p in range(2):
                        qg_copy(qblk, 1, 0, p).wait_recv()
                    st_copy(qblk, 1, 0).wait_recv()
                key_side(qgb.at[qblk, 0], qgb.at[qblk, 1], stb.at[qblk], False)
            return carry
        lax.fori_loop(0, 2, turn, 0)
        return carry

    lax.fori_loop(1, nz + 1, step, 0)

    own_dq[...] = (dq_acc[...] * score_scale).astype(BF16)
    half = rows // 2

    def dq_copy(block, lane, idx, p, own=False):
        to = (jnp.minimum(s + 2, nsp - 2 + y), jnp.maximum(s - 2, y), side)[lane]
        at = pl.ds(p * half, half)
        return copy(own_dq.at[at] if own else dqb.at[block, at], dqb.at[block, at],
                    dq_s.at[lane, p, idx], dq_r.at[p, block], to)

    for p in range(2):
        @pl.when(z < nz - 1)
        def _():
            dq_copy(s, 0, z, p, True).start()

        @pl.when(z > 0)
        def _():
            dq_copy(s, 1, z, p, True).start()

        dq_copy(s, 2, z, p, True).start()

    for h in range(heads):
        at = slice(h * width, (h + 1) * width)
        dq_out[:, h, :] = own_dq[:, at]
        dk_out[:, h, :] = (dk_acc[:, at] * score_scale).astype(BF16)
        dv_out[:, h, :] = dv_acc[:, at].astype(BF16)

    own_lat().wait()
    for d in range(1, nsp):
        lat_copy(d).wait_recv()
    for d in range(1, ntp):
        share_copy(d).start()
    for d in range(1, ntp):
        share_copy(d).wait_recv()

    wg_out[...] = dot_tn(latb[s], own_dq[...])

    def add_block(block):
        wg_out[...] += dot_tn(latb[block], dqb[block])

    def gather(k, carry):
        for p in range(2):
            for lane, there, ok, more in (
                (0, z - k, z - k >= 0, z < nz - 1),
                (1, z + k, z + k < nz, z > 0),
            ):
                bz = jnp.clip(there, 0, nz - 1)
                block = bz * 2 + y

                @pl.when(ok)
                def _():
                    dq_copy(block, lane, bz, p).wait_recv()
                    dq_copy(block, 2, bz, p).start()

                @pl.when(ok & more)
                def _():
                    dq_copy(block, lane, bz, p).start()

        def turn(c, carry):
            dist = jnp.where(c < 2, k, k - 1)
            up = lax.rem(c, 2)
            bz = jnp.where(up == 0, z - dist, z + dist)
            ok = (bz >= 0) & (bz < nz) & (dist < nz) & ((dist > 0) | (up == 0))
            other = jnp.where(c < 2, y, 1 - y)
            block = jnp.clip(bz, 0, nz - 1) * 2 + other

            @pl.when(ok)
            def _():
                @pl.when(c >= 2)
                def _():
                    for p in range(2):
                        dq_copy(block, 2, 0, p).wait_recv()
                add_block(block)
            return carry
        lax.fori_loop(0, 4, turn, 0)
        return carry

    lax.fori_loop(1, nz + 1, gather, 0)

    def drain(k, carry):
        below, above = z - k, z + k
        has_below, has_above = below >= 0, above < nz

        for p in range(2):
            @pl.when(has_below & (z < nz - 1))
            def _():
                kv_copy(s, 0, k, p).wait_send()

            @pl.when(has_below & ((k > 0) | (y == 0)))
            def _():
                kv_copy(s, 1, k, p).wait_send()

            @pl.when(has_above & (z > 0))
            def _():
                qg_copy(s, 0, k, p).wait_send()
                if p == 0:
                    st_copy(s, 0, k).wait_send()

            @pl.when(has_above & ((k > 0) | (y == 1)))
            def _():
                qg_copy(s, 1, k, p).wait_send()
                if p == 0:
                    st_copy(s, 1, k).wait_send()

            @pl.when((k <= z) & (z < nz - 1))
            def _():
                dq_copy(s, 0, k, p).wait_send()

            @pl.when((k >= z) & (z > 0))
            def _():
                dq_copy(s, 1, k, p).wait_send()

            dq_copy(s, 2, k, p).wait_send()
        return carry

    lax.fori_loop(0, nz, drain, 0)
    for d in range(1, nsp):
        lat_copy(d).wait_send()
    for d in range(1, ntp):
        share_copy(d).wait_send()


def vmem():
    return pl.BlockSpec(memory_space=pltpu.VMEM)


def body(nsp, ntp, latents, query_heads, key_heads, value_heads, map_outputs, log_sums, out_grad,
         mix_lambda, norm_gain):
    rows, heads, width = query_heads.shape
    flat = (rows, heads * width)
    slab = latents.shape[1] // nsp
    nz = nsp // 2
    dma = pltpu.SemaphoreType.DMA
    dq, dk, dv, wg = pl.pallas_call(
        functools.partial(main_kernel, nsp, ntp, heads, width),
        out_shape=(
            jax.ShapeDtypeStruct(query_heads.shape, BF16),
            jax.ShapeDtypeStruct(query_heads.shape, BF16),
            jax.ShapeDtypeStruct(query_heads.shape, BF16),
            jax.ShapeDtypeStruct((slab, heads * width), F32),
        ),
        in_specs=[pl.BlockSpec(memory_space=pltpu.SMEM)] + [vmem()] * 8,
        out_specs=(vmem(),) * 4,
        scratch_shapes=[
            pltpu.VMEM(flat, BF16),
            pltpu.VMEM((heads, rows, width), F32),
            pltpu.VMEM((heads, 4, rows), F32),
            pltpu.VMEM(flat, BF16),
            pltpu.VMEM((nsp, 2) + flat, BF16),
            pltpu.VMEM((nsp, 2) + flat, BF16),
            pltpu.VMEM((nsp, heads, 4, rows), F32),
            pltpu.VMEM((nsp,) + flat, BF16),
            pltpu.VMEM((nsp, rows, slab), BF16),
            pltpu.VMEM(flat, F32),
            pltpu.VMEM(flat, F32),
            pltpu.VMEM(flat, F32),
            dma((2, 2, nz)), dma((2, 2, nz)), dma((2, nz)), dma((3, 2, nz)),
            dma((2, nsp)), dma((2, nsp)), dma((nsp,)), dma((2, nsp)),
            dma((nsp,)), dma((nsp,)), dma((ntp,)), dma((ntp,)),
            dma,
        ],
        compiler_params=pltpu.CompilerParams(collective_id=0, has_side_effects=True),
        name="main",
    )(
        mix_lambda,
        norm_gain[None, :],
        latents,
        key_heads.reshape(flat),
        value_heads.reshape(flat),
        query_heads.reshape(flat),
        map_outputs,
        out_grad,
        jnp.transpose(log_sums, (1, 0, 2)),
    )
    return dq, dk, dv, wg


def row_norm_backward(heads, width, lam_ref, gain_ref, mo_ref, og_ref, lse_ref, grad_ref, row_ref):
    for h in range(heads):
        first = mo_ref[:, 0, h, :].astype(F32)
        second = mo_ref[:, 1, h, :].astype(F32)
        lam = lam_ref[h]
        combined = first - lam * second
        inverse = lax.rsqrt(jnp.mean(combined * combined, axis=-1, keepdims=True) + EPSILON)
        weighted = gain_ref[...] * og_ref[:, h, :].astype(F32)
        grad = (
            inverse * weighted
            - inverse**3 * combined * jnp.mean(combined * weighted, axis=-1, keepdims=True)
        ).astype(BF16)
        grad_ref[:, h * width : (h + 1) * width] = grad
        wide = grad.astype(F32)
        log_lam = jnp.log(jnp.full((1, 1), lam, F32)) * LOG2E
        row_ref[h, 0:1] = lse_ref[h, 0:1] * LOG2E
        row_ref[h, 1:2] = lse_ref[h, 1:2] * LOG2E - log_lam
        lane = lax.broadcasted_iota(jnp.int32, wide.shape, 1)
        terms = jnp.where(lane == 0, jnp.sum(wide * first, axis=-1, keepdims=True),
                          jnp.sum(wide * second, axis=-1, keepdims=True))
        row_ref[h, 2:4] = jnp.transpose(terms)[0:2]


def hub_kernel(nsp, ntp, heads, width, lam_far, gain_far, lat, own_k, own_v, own_q, mo_far, og_far, lse_far,
               dq_out, dk_out, dv_out, wg_out,
               own_g, row, blk, stb, dq_acc, dk_acc, dv_acc, db, out_b, in_b, in_a, kt, kin, kst, kret, latb,
               f_s, z_s, r_s, b_r, st_r, d_s, d_r, ob_s, ib_r, ia_r, kt_s, kin_r, tot_s, kst_s, kret_r,
               la_s, la_r, lb_s, lb_r, own_sem, lam, gain, mo, og, lse, near):
    nz = nsp // 2
    low, high, top = nz // 2 - 1, nz // 2, nz - 1
    s = lax.axis_index("sp")
    t = lax.axis_index("tp")
    z, y = s // 2, lax.rem(s, 2)
    rows = own_k.shape[0]
    span = 2 * rows
    pair = heads // 2
    lanes = pair * width
    part = rows // ntp
    slab = lat.shape[1] // nsp
    score_scale = (width // 2) ** (-0.5)
    exp_scale = score_scale * LOG2E
    partner = 2 * z + 1 - y
    Q, K, V, G, ST = range(5)

    fetches = [
        pltpu.make_async_copy(src, dst, near.at[i])
        for i, (src, dst) in enumerate(((mo_far, mo), (og_far, og), (lse_far, lse), (gain_far, gain), (lam_far, lam)))
    ]
    for fetch in fetches:
        fetch.start()

    barrier = pltpu.get_barrier_semaphore()
    for d in range(1, nsp):
        pl.semaphore_signal(barrier, inc=1, device_id={"sp": lax.rem(s + d, nsp)}, device_id_type=MESH)
    for d in range(1, ntp):
        pl.semaphore_signal(barrier, inc=1, device_id={"tp": lax.rem(t + d, ntp)}, device_id_type=MESH)
    pl.semaphore_wait(barrier, nsp - 1 + ntp - 1)

    def copy(src, dst, send, recv, to):
        return pltpu.make_async_remote_copy(
            src_ref=src, dst_ref=dst, send_sem=send, recv_sem=recv,
            device_id={"sp": to}, device_id_type=MESH)

    def at_level(level):
        return 2 * level + y

    def lane_of(p):
        return pl.ds(pl.multiple_of(p * lanes, lanes), lanes)

    def half_of(p):
        return pl.ds(pl.multiple_of(p * rows, rows), rows)

    owned = (own_q, own_k, own_v, own_g)

    def source(a, p):
        if a == ST:
            return row.at[pl.ds(p * pair, pair)]
        return owned[a].at[:, lane_of(p)]

    def landing(a, level, half):
        return stb.at[level, half] if a == ST else blk.at[a, level, half_of(half), :]

    def landed(a, level, half):
        return st_r.at[level, half] if a == ST else b_r.at[a, level, half]

    def swap(a):
        return copy(source(a, 1 - y), landing(a, z, y), f_s.at[a], landed(a, z, y), partner)

    def arrive(a, level, half):
        copy(landing(a, level, half), landing(a, level, half), f_s.at[a], landed(a, level, half), partner).wait_recv()

    def pass_on(a, own):
        half = y if own else 1 - y
        return copy(source(a, y) if own else landing(a, z, half), landing(a, z, half),
                    z_s.at[a, 0 if own else 1], landed(a, z, half), at_level(jnp.where(z > high, high, low)))

    def passes(action, arrays, own):
        for a in arrays:
            if a in (K, V):
                @pl.when(z < low)
                def _():
                    action(pass_on(a, own))
            else:
                @pl.when(z >= high)
                def _():
                    action(pass_on(a, own))

    def relay(a, half):
        return copy(landing(a, top, half), landing(a, top, half), r_s.at[a, half], landed(a, top, half), at_level(low))

    def relays(arrays, half):
        @pl.when(z == high)
        def _():
            for a in arrays:
                arrive(a, top, half)
                relay(a, half).start()

    def start(c):
        c.start()

    def lat_copy(d):
        to = lax.rem(s + d, nsp)
        mine = pl.ds(pl.multiple_of(t * part, part), part)
        return copy(lat.at[mine, pl.ds(pl.multiple_of(to * slab, slab), slab)],
                    latb.at[s, mine, :], la_s.at[d], la_r.at[s], to)

    def own_lat():
        return pltpu.make_async_copy(
            lat.at[:, pl.ds(pl.multiple_of(s * slab, slab), slab)], latb.at[s], own_sem)

    sides = ntp // 2
    side, core = t // 2, lax.rem(t, 2)

    def share_copy(b, k):
        away = lax.rem(side + (k if k < sides else k - sides), sides)
        quarter = t if k < sides else 2 * away + core
        to = 2 * away + core if 0 < k < sides else 2 * side + 1 - core
        at = pl.ds(pl.multiple_of(quarter * part, part), part)
        return pltpu.make_async_remote_copy(
            src_ref=latb.at[b, at, :], dst_ref=latb.at[b, at, :],
            send_sem=lb_s.at[b, k], recv_sem=lb_r.at[b, quarter],
            device_id={"tp": to}, device_id_type=MESH)

    def share_arrive(b, quarter):
        at = pl.ds(pl.multiple_of(quarter * part, part), part)
        pltpu.make_async_remote_copy(
            src_ref=latb.at[b, at, :], dst_ref=latb.at[b, at, :],
            send_sem=lb_s.at[b, 0], recv_sem=lb_r.at[b, quarter],
            device_id={"tp": 2 * side + 1 - core}, device_id_type=MESH).wait_recv()

    def group_of(src, dst, group):
        sz, dz = src // 2, dst // 2
        late = (sz >= high) & (dz < high)
        upper = (sz >= high) & (dz >= high) & (dz < sz)
        first = (lax.rem(src, 2) == lax.rem(dst, 2)) & ((dz > sz) | (sz < high))
        if group == 3:
            return late
        if group == 2:
            return upper
        rest = jnp.logical_not(late | upper)
        return rest & (first if group == 0 else jnp.logical_not(first))

    def lat_send(group):
        for d in range(1, nsp):
            @pl.when(group_of(s, lax.rem(s + d, nsp), group))
            def _():
                lat_copy(d).start()

    def share_send(group):
        def step(d, carry):
            b = lax.rem(s + d, nsp)

            @pl.when(group_of(b, s, group))
            def _():
                mine = pl.ds(pl.multiple_of(t * part, part), part)
                copy(latb.at[b, mine, :], latb.at[b, mine, :], la_s.at[1], la_r.at[b], partner).wait_recv()
                for k in reversed(range(sides)):
                    share_copy(b, k).start()
            return carry
        lax.fori_loop(1, nsp, step, 0)

    def share_hand(group):
        def hand(d, carry):
            b = lax.rem(s + d, nsp)

            @pl.when(group_of(b, s, group))
            def _():
                for k in range(sides + 1, 2 * sides):
                    share_arrive(b, 2 * lax.rem(side + k - sides, sides) + core)
                    share_copy(b, k).start()
            return carry
        lax.fori_loop(1, nsp, hand, 0)

    def lat_share(group):
        share_send(group)
        share_hand(group)

    swap(Q).start()
    passes(start, (Q, K, V), True)
    swap(K).start()
    swap(V).start()
    lat_send(0)
    own_lat().start()

    for fetch in fetches:
        fetch.wait()
    row_norm_backward(heads, width, lam, gain, mo, og, lse, own_g, row)

    swap(G).start()
    swap(ST).start()
    passes(start, (ST, G), True)
    lat_send(1)

    for a in (Q, K, V, G):
        blk[a, z, half_of(y), :] = owned[a][:, lane_of(y)]
    stb[z, y] = row[pl.ds(y * pair, pair)]
    dq_acc[...] = jnp.zeros_like(dq_acc)
    dk_acc[...] = jnp.zeros_like(dk_acc)
    dv_acc[...] = jnp.zeros_like(dv_acc)

    for a in (Q, K, V, ST, G):
        arrive(a, z, 1 - y)
        passes(start, (a,), False)
        if a == Q:
            relays((Q,), y)
        if a == G:
            relays((Q,), 1 - y)
            relays((ST, G), y)

    lane_id = lax.broadcasted_iota(jnp.int32, (1, width), 1)
    first_map = jnp.where(lane_id < width // 2, 1.0, 0.0).astype(BF16)
    second_map = jnp.where(lane_id < width // 2, 0.0, 1.0).astype(BF16)

    def split(x):
        return jnp.concatenate([x * first_map, x * second_map], axis=0)

    def visit(qz, kz, slot, diagonal):
        def one(h, carry):
            at = pl.ds(pl.multiple_of(h * width, width), width)
            for a in range(2):
                start_row = a * rows if diagonal else 0
                kr = pl.ds(a * rows, rows)
                qr = pl.ds(start_row, span - start_row)
                count = span - start_row
                keys = split(blk[K, kz, kr, at])
                queries = split(blk[Q, qz, qr, at])
                grads = blk[G, qz, qr, at]
                scores = dot_nt(blk[K, kz, kr, at], queries)
                mixed = dot_nt(blk[V, kz, kr, at], grads)
                stats = jnp.concatenate([stb[qz, p, h] for p in range(start_row // rows, 2)], axis=1)
                x1 = scores[:, :count] * exp_scale - stats[0:1]
                x2 = scores[:, count:] * exp_scale - stats[1:2]
                if diagonal:
                    seen = (lax.broadcasted_iota(jnp.int32, (rows, count), 0)
                            <= lax.broadcasted_iota(jnp.int32, (rows, count), 1))
                    x1 = jnp.where(seen, x1, -jnp.inf)
                    x2 = jnp.where(seen, x2, -jnp.inf)
                p1 = jnp.exp2(x1)
                p2 = jnp.exp2(x2)
                g1 = (p1 * (mixed - stats[2:3])).astype(BF16)
                g2 = (p2 * (stats[3:4] - mixed)).astype(BF16)
                dv_acc[slot, kr, at] += dot_nn((p1 - p2).astype(BF16), grads)
                dk_acc[slot, kr, at] += dot_nn(jnp.concatenate([g1, g2], axis=1), queries)
                dq_acc[qz, h, :, qr] += dot_tn(keys, jnp.concatenate([g1, g2], axis=0))
            return carry
        lax.fori_loop(0, pair, one, 0)

    def dq_value(level):
        return jnp.concatenate([jnp.transpose(dq_acc[level, h]) for h in range(pair)], axis=1) * score_scale

    def grad_copy(level, lane):
        if lane == 0:
            to = partner
        elif lane == 1:
            down = high if level == 0 else 0
            to = at_level(jnp.where(z == low, down, jnp.where(z == high, top, low)))
        else:
            to = at_level(high)
        return copy(db.at[level, y], db.at[level, y], d_s.at[level, lane], d_r.at[level, y], to)

    def grad_lanes(level):
        chained = (z <= high) if level == 0 else (z == high) | (z == low)
        if level != low:
            return ((0, None), (1, chained))
        return ((0, None), (1, chained), (2, z == low))

    def grad_each(level, action):
        for lane, ok in reversed(grad_lanes(level)):
            if ok is None:
                action(grad_copy(level, lane))
            else:
                @pl.when(ok)
                def _():
                    action(grad_copy(level, lane))

    def grad_arrive(level, p):
        copy(db.at[level, p], db.at[level, p], d_s.at[level, 0], d_r.at[level, p], partner).wait_recv()

    def part_copy(i):
        return copy(out_b.at[i], in_b.at[i], ob_s.at[i], ib_r.at[i], at_level(jnp.where(z == low, high, low)))

    def top_copy():
        return copy(out_b.at[0], in_a, ob_s.at[0], ia_r, at_level(high))

    def key_copy(i):
        return copy(kt.at[i], kin.at[i], kt_s.at[i], kin_r.at[i], at_level(low))

    def total_copy(i, half):
        return copy(kt.at[i, half_of(half), :], kret.at[i, y], tot_s.at[i, half], kret_r.at[i, y], half)

    def return_copy(i):
        return copy(kst.at[i], kret.at[i, y], kst_s.at[i], kret_r.at[i, y], partner)

    visit(z, z, 0, True)
    relays((ST, G), 1 - y)

    @pl.when(z >= high)
    def _():
        out_b[0] = dq_value(z).astype(BF16)

    @pl.when(z == high)
    def _():
        part_copy(0).start()

    @pl.when(z > high)
    def _():
        top_copy().start()
        lat_send(2)

    @pl.when(z < low)
    def _():
        db[0, y] = dq_value(0).astype(BF16)
        grad_each(0, start)
        for i in range(2):
            kt[i] = (dv_acc[0] if i else dk_acc[0] * score_scale).astype(BF16)
            key_copy(i).start()

    def return_keys():
        for i, acc, scale in ((0, dk_acc, score_scale), (1, dv_acc, 1.0)):
            kst[i] = (acc[0, half_of(1 - y), :] * scale).astype(BF16)
            return_copy(i).start()
            kret[i, y] = (acc[0, half_of(y), :] * scale).astype(BF16)

    def hand_on(level):
        grad_arrive(level, y)
        grad_each(level, start)

    def total(level):
        i = level - high
        part_copy(i).wait_recv()
        whole = dq_value(level) + in_b[i].astype(F32)
        if level == top:
            above = in_a[...].astype(F32)
            whole = whole + jnp.where(z == high, above, jnp.zeros_like(above))
        db[level, y] = whole.astype(BF16)
        grad_each(level, start)

    @pl.when(z == low)
    def _():
        def step(i, carry):
            qz = jnp.where(i == 0, low, high + (i - 1) // 2)
            kz = jnp.where(i == 0, 0, lax.rem(i - 1, 2))

            @pl.when(i == 0)
            def _():
                for half in range(2):
                    arrive(K, 0, half)
                    arrive(V, 0, half)

            @pl.when((i > 0) & (kz == 0))
            def _():
                for a in (Q, ST, G):
                    for half in range(2):
                        arrive(a, qz, half)

            visit(qz, kz, 1 - kz, False)

            @pl.when(i == 0)
            def _():
                db[low, y] = dq_value(low).astype(BF16)
                grad_each(low, start)
                share_send(0)

            @pl.when((i > 0) & (kz == 1))
            def _():
                out_b[qz - high] = dq_value(qz).astype(BF16)
                part_copy(qz - high).start()

            @pl.when((qz == high) & (kz == 1))
            def _():
                share_hand(0)

            @pl.when((qz == top) & (kz == 0))
            def _():
                hand_on(0)
            return carry
        lax.fori_loop(0, 5, step, 0)
        total(high)
        total(top)
        for j in range(2):
            key_copy(j).wait_recv()
            acc = dv_acc[1] if j else dk_acc[1] * score_scale
            kt[j] = (acc + kin[j].astype(F32)).astype(BF16)
            for half in range(2):
                total_copy(j, half).start()
        return_keys()
        lat_share(1)

    @pl.when(z == high)
    def _():
        visit(top, high, 0, False)
        top_copy().wait_recv()
        out_b[1] = (dq_value(top) + in_a[...].astype(F32)).astype(BF16)
        part_copy(1).start()
        return_keys()
        lat_share(0)
        hand_on(low)
        lat_send(3)
        hand_on(0)
        total(high)
        lat_share(1)
        lat_share(2)
        total(top)

    @pl.when(z < low)
    def _():
        lat_share(0)
        hand_on(low)
        lat_share(1)

    @pl.when(z > high)
    def _():
        return_keys()
        lat_share(0)
        hand_on(low)
        lat_send(3)
        hand_on(0)
        lat_share(1)

    def key_results():
        for i in range(2):
            copy(kst.at[i], kret.at[i, 1 - y], kst_s.at[i], kret_r.at[i, 1 - y], partner).wait_recv()

            @pl.when(z < low)
            def _():
                copy(kst.at[i], kret.at[i, y], kst_s.at[i], kret_r.at[i, y], partner).wait_recv()
            out = dv_out if i else dk_out
            for p in range(2):
                for h in range(pair):
                    out[:, p * pair + h, :] = kret[i, p, :, h * width : (h + 1) * width]

    def query_results():
        for p in range(2):
            for h in range(pair):
                dq_out[:, p * pair + h, :] = db[z, p, half_of(y), h * width : (h + 1) * width]

    def weights(level):
        grad_arrive(level, 1 - y)
        for half in range(2):
            b = 2 * level + half

            @pl.when(s != b)
            def _():
                for k in range(sides):
                    share_arrive(b, 2 * lax.rem(side + k, sides) + 1 - core)
        feed = latb[2 * level : 2 * level + 2].reshape(span, slab)
        for p in range(2):
            at = slice(p * lanes, (p + 1) * lanes)
            term = dot_tn(feed, db[level, p])
            if level == 0:
                wg_out[:, at] = term
            else:
                wg_out[:, at] += term

    own_lat().wait()

    @pl.when(z >= high)
    def _():
        key_results()

    for level in range(high):
        weights(level)

        @pl.when((z < low) | (z > high))
        def _():
            hand_on(high + level)

    @pl.when(z < high)
    def _():
        query_results()
        lat_share(3)

    for level in range(high, nz):
        weights(level)

    @pl.when(z < high)
    def _():
        key_results()

    @pl.when(z >= high)
    def _():
        query_results()

    def sent(c):
        c.wait_send()

    for a in range(5):
        sent(swap(a))
    for own in (True, False):
        passes(sent, (Q, K, V, ST, G), own)
    for a in (Q, ST, G):
        @pl.when(z == high)
        def _():
            for half in range(2):
                sent(relay(a, half))
    for level in range(nz):
        grad_each(level, sent)
    for i in range(2):
        @pl.when(z >= low)
        def _():
            sent(return_copy(i))

        @pl.when((z == low) | (z == high))
        def _():
            sent(part_copy(i))

        @pl.when(z == low)
        def _():
            for half in range(2):
                sent(total_copy(i, half))

        @pl.when(z < low)
        def _():
            sent(key_copy(i))

    @pl.when(z > high)
    def _():
        sent(top_copy())
    for d in range(1, nsp):
        sent(lat_copy(d))

    def drain(d, carry):
        for k in range(2 * sides):
            if k != sides:
                sent(share_copy(lax.rem(s + d, nsp), k))
        return carry
    lax.fori_loop(1, nsp, drain, 0)


def finish_kernel(a, b, c, d, a_out, b_out, c_out, d_out):
    for src, dst in ((a, a_out), (b, b_out), (c, c_out), (d, d_out)):
        dst[...] = src[...]


def far():
    return pl.BlockSpec(memory_space=pltpu.HBM)


def hub_body(nsp, ntp, latents, query_heads, key_heads, value_heads, map_outputs, log_sums, out_grad,
             mix_lambda, norm_gain):
    rows, heads, width = query_heads.shape
    flat = (rows, heads * width)
    slab = latents.shape[1] // nsp
    nz = nsp // 2
    pair = heads // 2
    block = (2 * rows, pair * width)
    half = (rows, pair * width)
    dma = pltpu.SemaphoreType.DMA
    results = pl.pallas_call(
        functools.partial(hub_kernel, nsp, ntp, heads, width),
        out_shape=(
            jax.ShapeDtypeStruct(query_heads.shape, BF16),
            jax.ShapeDtypeStruct(query_heads.shape, BF16),
            jax.ShapeDtypeStruct(query_heads.shape, BF16),
            jax.ShapeDtypeStruct((slab, heads * width), F32),
        ),
        in_specs=[far()] * 3 + [vmem()] * 3 + [far()] * 3,
        out_specs=(vmem(),) * 4,
        scratch_shapes=[
            pltpu.VMEM(flat, BF16),
            pltpu.VMEM((heads, 4, rows), F32),
            pltpu.VMEM((4, nz) + block, BF16),
            pltpu.VMEM((nz, 2, pair, 4, rows), F32),
            pltpu.VMEM((nz, pair, width, 2 * rows), F32),
            pltpu.VMEM((2,) + block, F32),
            pltpu.VMEM((2,) + block, F32),
            pltpu.VMEM((nz, 2) + block, BF16),
            pltpu.VMEM((2,) + block, BF16),
            pltpu.VMEM((2,) + block, BF16),
            pltpu.VMEM(block, BF16),
            pltpu.VMEM((2,) + block, BF16),
            pltpu.VMEM((2,) + block, BF16),
            pltpu.VMEM((2,) + half, BF16),
            pltpu.VMEM((2, 2) + half, BF16),
            pltpu.VMEM((nsp, rows, slab), BF16),
            dma((5,)), dma((5, 2)), dma((5, 2)), dma((4, nz, 2)), dma((nz, 2)), dma((nz, 3)), dma((nz, 2)),
            dma((2,)), dma((2,)), dma, dma((2,)), dma((2,)), dma((2, 2)), dma((2,)), dma((2, 2)),
            dma((nsp,)), dma((nsp,)), dma((nsp, ntp)), dma((nsp, ntp)),
            dma,
            pltpu.SMEM(mix_lambda.shape, F32),
            pltpu.VMEM((1, width), F32),
            pltpu.VMEM(map_outputs.shape, BF16),
            pltpu.VMEM(out_grad.shape, BF16),
            pltpu.VMEM((heads, 2, rows), F32),
            dma((5,)),
        ],
        compiler_params=pltpu.CompilerParams(
            collective_id=0, has_side_effects=True, vmem_limit_bytes=54800000),
        name="hub",
    )(
        mix_lambda,
        norm_gain[None, :],
        latents,
        key_heads.reshape(flat),
        value_heads.reshape(flat),
        query_heads.reshape(flat),
        map_outputs,
        out_grad,
        jnp.transpose(log_sums, (1, 2, 0)),
    )
    return pl.pallas_call(
        finish_kernel,
        out_shape=tuple(jax.ShapeDtypeStruct(a.shape, a.dtype) for a in results),
        in_specs=[vmem()] * 4,
        out_specs=(vmem(),) * 4,
        compiler_params=pltpu.CompilerParams(vmem_limit_bytes=8 * 2**20),
        name="finish",
    )(*results)


def solution(mesh):
    placed = (
        P("sp", None),
        P("sp", "tp", None),
        P("sp", "tp", None),
        P("sp", "tp", None),
        P("sp", None, "tp", None),
        P("sp", "tp", None),
        P("sp", "tp", None),
        P("tp"),
        P(),
    )
    nsp, ntp = mesh.shape["sp"], mesh.shape["tp"]

    def chosen(*args):
        heads = args[1].shape[1]
        return (hub_body if nsp == 8 and heads % 2 == 0 else body)(nsp, ntp, *args)

    return jax.shard_map(
        chosen,
        mesh=mesh,
        in_specs=placed,
        out_specs=(P("sp", "tp", None), P("sp", "tp", None), P("sp", "tp", None), P("sp", "tp")),
        check_vma=False,
    )
```

```python
import functools
import math

import jax
import jax.numpy as jnp
from jax import lax
from jax.experimental import pallas as pl
from jax.experimental.pallas import tpu as pltpu
from jax.sharding import PartitionSpec as P

EPSILON = 1e-05
LOG2E = math.log2(math.e)
F32 = jnp.float32
BF16 = jnp.bfloat16
MESH = pl.DeviceIdType.MESH


def dot_nn(a, b):
    return lax.dot_general(a, b, (((1,), (0,)), ((), ())), preferred_element_type=F32)


def dot_nt(a, b):
    return lax.dot_general(a, b, (((1,), (1,)), ((), ())), preferred_element_type=F32)


def dot_tn(a, b):
    return lax.dot_general(a, b, (((0,), (0,)), ((), ())), preferred_element_type=F32)


def norm_backward(heads, width, lam_ref, gain_ref, mo_ref, og_ref, lse_ref, grad_ref, col_ref, row_ref):
    for h in range(heads):
        first = mo_ref[:, 0, h, :].astype(F32)
        second = mo_ref[:, 1, h, :].astype(F32)
        lam = lam_ref[h]
        combined = first - lam * second
        inverse = lax.rsqrt(jnp.mean(combined * combined, axis=-1, keepdims=True) + EPSILON)
        weighted = gain_ref[...] * og_ref[:, h, :].astype(F32)
        grad = (
            inverse * weighted
            - inverse**3 * combined * jnp.mean(combined * weighted, axis=-1, keepdims=True)
        ).astype(BF16)
        grad_ref[:, h * width : (h + 1) * width] = grad
        wide = grad.astype(F32)
        lse = lse_ref[h] * LOG2E
        log_lam = jnp.log(jnp.full((1, 1), lam, F32)) * LOG2E
        lane = lax.broadcasted_iota(jnp.int32, wide.shape, 1)
        stats = jnp.where(lane == 0, lse[:, 0:1], lse[:, 1:2] - log_lam)
        stats = jnp.where(lane == 2, jnp.sum(wide * first, axis=-1, keepdims=True), stats)
        stats = jnp.where(lane == 3, jnp.sum(wide * second, axis=-1, keepdims=True), stats)
        col_ref[h] = stats
        row_ref[h] = jnp.transpose(stats)[0:4]


def main_kernel(nsp, ntp, heads, width, lam, gain, lat, own_k, own_v, own_q, mo, og, lse,
                dq_out, dk_out, dv_out, wg_out,
                own_g, col, row, own_dq, kvb, qgb, stb, dqb, latb, dq_acc, dk_acc, dv_acc,
                kv_s, qg_s, st_s, dq_s, kv_r, qg_r, st_r, dq_r,
                la_s, la_r, lb_s, lb_r, own_sem):
    nz = nsp // 2
    s = lax.axis_index("sp")
    t = lax.axis_index("tp")
    z, y = s // 2, lax.rem(s, 2)
    rows = own_k.shape[0]
    part = rows // ntp
    slab = lat.shape[1] // nsp
    score_scale = (width // 2) ** (-0.5)
    exp_scale = score_scale * LOG2E

    barrier = pltpu.get_barrier_semaphore()
    for d in range(1, nsp):
        pl.semaphore_signal(barrier, inc=1, device_id={"sp": lax.rem(s + d, nsp)}, device_id_type=MESH)
    for d in range(1, ntp):
        pl.semaphore_signal(barrier, inc=1, device_id={"tp": lax.rem(t + d, ntp)}, device_id_type=MESH)
    pl.semaphore_wait(barrier, nsp - 1 + ntp - 1)

    def copy(src, dst, send, recv, to):
        return pltpu.make_async_remote_copy(
            src_ref=src, dst_ref=dst, send_sem=send, recv_sem=recv,
            device_id={"sp": to}, device_id_type=MESH)

    side = 2 * z + (1 - y)

    def kv_copy(block, lane, k, p, src=None):
        to = jnp.minimum(s + 2, nsp - 1) if lane == 0 else side
        return copy(kvb.at[block, p] if src is None else src, kvb.at[block, p],
                    kv_s.at[lane, p, k], kv_r.at[p, block], to)

    def qg_copy(block, lane, k, p, src=None):
        to = jnp.maximum(s - 2, 0) if lane == 0 else side
        return copy(qgb.at[block, p] if src is None else src, qgb.at[block, p],
                    qg_s.at[lane, p, k], qg_r.at[p, block], to)

    def st_copy(block, lane, k, src=None):
        to = jnp.maximum(s - 2, 0) if lane == 0 else side
        return copy(stb.at[block] if src is None else src, stb.at[block],
                    st_s.at[lane, k], st_r.at[block], to)

    for p, src in ((0, own_k), (1, own_v)):
        @pl.when(z < nz - 1)
        def _():
            kv_copy(s, 0, 0, p, src).start()

        @pl.when(y == 0)
        def _():
            kv_copy(s, 1, 0, p, src).start()

    @pl.when(z > 0)
    def _():
        qg_copy(s, 0, 0, 0, own_q).start()

    @pl.when(y == 1)
    def _():
        qg_copy(s, 1, 0, 0, own_q).start()

    norm_backward(heads, width, lam, gain, mo, og, lse, own_g, col, row)

    @pl.when(z > 0)
    def _():
        st_copy(s, 0, 0, row).start()
        qg_copy(s, 0, 0, 1, own_g).start()

    @pl.when(y == 1)
    def _():
        st_copy(s, 1, 0, row).start()
        qg_copy(s, 1, 0, 1, own_g).start()

    lane_id = lax.broadcasted_iota(jnp.int32, (1, width), 1)
    low = jnp.where(lane_id < width // 2, 1.0, 0.0).astype(BF16)
    high = jnp.where(lane_id < width // 2, 0.0, 1.0).astype(BF16)

    def split(x):
        return jnp.concatenate([x * low, x * high], axis=0)

    def query_side(k_at, v_at, diagonal):
        def one(h, carry):
            at = pl.ds(pl.multiple_of(h * width, width), width)
            keys = split(k_at[:, at])
            scores = dot_nt(own_q[:, at], keys)
            mixed = dot_nt(own_g[:, at], v_at[:, at])
            stats = col[h]
            x1 = scores[:, :rows] * exp_scale - stats[:, 0:1]
            x2 = scores[:, rows:] * exp_scale - stats[:, 1:2]
            if diagonal:
                seen = (lax.broadcasted_iota(jnp.int32, (rows, rows), 1)
                        <= lax.broadcasted_iota(jnp.int32, (rows, rows), 0))
                x1 = jnp.where(seen, x1, -jnp.inf)
                x2 = jnp.where(seen, x2, -jnp.inf)
            g1 = (jnp.exp2(x1) * (mixed - stats[:, 2:3])).astype(BF16)
            g2 = (jnp.exp2(x2) * (stats[:, 3:4] - mixed)).astype(BF16)
            part_dq = dot_nn(jnp.concatenate([g1, g2], axis=1), keys)
            if diagonal:
                dq_acc[:, at] = part_dq
            else:
                dq_acc[:, at] += part_dq
            return carry
        lax.fori_loop(0, heads, one, 0)

    def key_side(q_at, g_at, row_at, diagonal):
        def one(h, carry):
            at = pl.ds(pl.multiple_of(h * width, width), width)
            queries = split(q_at[:, at])
            grads = g_at[:, at]
            scores = dot_nt(own_k[:, at], queries)
            mixed = dot_nt(own_v[:, at], grads)
            stats = row_at[h]
            x1 = scores[:, :rows] * exp_scale - stats[0:1]
            x2 = scores[:, rows:] * exp_scale - stats[1:2]
            if diagonal:
                seen = (lax.broadcasted_iota(jnp.int32, (rows, rows), 0)
                        <= lax.broadcasted_iota(jnp.int32, (rows, rows), 1))
                x1 = jnp.where(seen, x1, -jnp.inf)
                x2 = jnp.where(seen, x2, -jnp.inf)
            p1 = jnp.exp2(x1)
            p2 = jnp.exp2(x2)
            g1 = (p1 * (mixed - stats[2:3])).astype(BF16)
            g2 = (p2 * (stats[3:4] - mixed)).astype(BF16)
            part_dv = dot_nn((p1 - p2).astype(BF16), grads)
            part_dk = dot_nn(jnp.concatenate([g1, g2], axis=1), queries)
            if diagonal:
                dv_acc[:, at] = part_dv
                dk_acc[:, at] = part_dk
            else:
                dv_acc[:, at] += part_dv
                dk_acc[:, at] += part_dk
            return carry
        lax.fori_loop(0, heads, one, 0)

    def lat_copy(d):
        to = lax.rem(s + d, nsp)
        mine = pl.ds(pl.multiple_of(t * part, part), part)
        return copy(lat.at[mine, pl.ds(pl.multiple_of(to * slab, slab), slab)],
                    latb.at[s, mine, :], la_s.at[d], la_r.at[d], to)

    def own_lat():
        return pltpu.make_async_copy(
            lat.at[pl.ds(pl.multiple_of(t * part, part), part), pl.ds(pl.multiple_of(s * slab, slab), slab)],
            latb.at[s, pl.ds(pl.multiple_of(t * part, part), part), :], own_sem)

    def share_copy(d):
        mine = pl.ds(pl.multiple_of(t * part, part), part)
        return pltpu.make_async_remote_copy(
            src_ref=latb.at[:, mine, :], dst_ref=latb.at[:, mine, :],
            send_sem=lb_s.at[d], recv_sem=lb_r.at[d],
            device_id={"tp": lax.rem(t + d, ntp)}, device_id_type=MESH)

    own_lat().start()
    query_side(own_k, own_v, True)
    key_side(own_q, own_g, row, True)
    for d in range(1, nsp):
        lat_copy(d).start()

    def step(k, carry):
        below, above = z - k, z + k
        has_below, has_above = below >= 0, above < nz
        kb = jnp.maximum(below, 0) * 2 + y
        qb = jnp.minimum(above, nz - 1) * 2 + y

        for p in range(2):
            @pl.when(has_below)
            def _():
                kv_copy(kb, 0, 0, p).wait_recv()
                kv_copy(kb, 1, k, p).start()

            @pl.when(has_below & (z < nz - 1))
            def _():
                kv_copy(kb, 0, k, p).start()

            @pl.when(has_above)
            def _():
                qg_copy(qb, 0, 0, p).wait_recv()
                qg_copy(qb, 1, k, p).start()
                if p == 0:
                    st_copy(qb, 0, 0).wait_recv()
                    st_copy(qb, 1, k).start()

            @pl.when(has_above & (z > 0))
            def _():
                qg_copy(qb, 0, k, p).start()
                if p == 0:
                    st_copy(qb, 0, k).start()

        def turn(c, carry):
            dist = k - c
            other = jnp.where(c == 0, y, 1 - y)
            bz, qz = z - dist, z + dist
            use_kv = (bz >= 0) & (dist < nz) & ((dist > 0) | (y == 1))
            use_qg = (qz < nz) & (dist < nz) & ((dist > 0) | (y == 0))
            kblk = jnp.maximum(bz, 0) * 2 + other
            qblk = jnp.minimum(qz, nz - 1) * 2 + other

            @pl.when(use_kv)
            def _():
                @pl.when(c == 1)
                def _():
                    for p in range(2):
                        kv_copy(kblk, 1, 0, p).wait_recv()
                query_side(kvb.at[kblk, 0], kvb.at[kblk, 1], False)

            @pl.when(use_qg)
            def _():
                @pl.when(c == 1)
                def _():
                    for p in range(2):
                        qg_copy(qblk, 1, 0, p).wait_recv()
                    st_copy(qblk, 1, 0).wait_recv()
                key_side(qgb.at[qblk, 0], qgb.at[qblk, 1], stb.at[qblk], False)
            return carry
        lax.fori_loop(0, 2, turn, 0)
        return carry

    lax.fori_loop(1, nz + 1, step, 0)

    own_dq[...] = (dq_acc[...] * score_scale).astype(BF16)
    half = rows // 2

    def dq_copy(block, lane, idx, p, own=False):
        to = (jnp.minimum(s + 2, nsp - 2 + y), jnp.maximum(s - 2, y), side)[lane]
        at = pl.ds(p * half, half)
        return copy(own_dq.at[at] if own else dqb.at[block, at], dqb.at[block, at],
                    dq_s.at[lane, p, idx], dq_r.at[p, block], to)

    for p in range(2):
        @pl.when(z < nz - 1)
        def _():
            dq_copy(s, 0, z, p, True).start()

        @pl.when(z > 0)
        def _():
            dq_copy(s, 1, z, p, True).start()

        dq_copy(s, 2, z, p, True).start()

    for h in range(heads):
        at = slice(h * width, (h + 1) * width)
        dq_out[:, h, :] = own_dq[:, at]
        dk_out[:, h, :] = (dk_acc[:, at] * score_scale).astype(BF16)
        dv_out[:, h, :] = dv_acc[:, at].astype(BF16)

    own_lat().wait()
    for d in range(1, nsp):
        lat_copy(d).wait_recv()
    for d in range(1, ntp):
        share_copy(d).start()
    for d in range(1, ntp):
        share_copy(d).wait_recv()

    wg_out[...] = dot_tn(latb[s], own_dq[...])

    def add_block(block):
        wg_out[...] += dot_tn(latb[block], dqb[block])

    def gather(k, carry):
        for p in range(2):
            for lane, there, ok, more in (
                (0, z - k, z - k >= 0, z < nz - 1),
                (1, z + k, z + k < nz, z > 0),
            ):
                bz = jnp.clip(there, 0, nz - 1)
                block = bz * 2 + y

                @pl.when(ok)
                def _():
                    dq_copy(block, lane, bz, p).wait_recv()
                    dq_copy(block, 2, bz, p).start()

                @pl.when(ok & more)
                def _():
                    dq_copy(block, lane, bz, p).start()

        def turn(c, carry):
            dist = jnp.where(c < 2, k, k - 1)
            up = lax.rem(c, 2)
            bz = jnp.where(up == 0, z - dist, z + dist)
            ok = (bz >= 0) & (bz < nz) & (dist < nz) & ((dist > 0) | (up == 0))
            other = jnp.where(c < 2, y, 1 - y)
            block = jnp.clip(bz, 0, nz - 1) * 2 + other

            @pl.when(ok)
            def _():
                @pl.when(c >= 2)
                def _():
                    for p in range(2):
                        dq_copy(block, 2, 0, p).wait_recv()
                add_block(block)
            return carry
        lax.fori_loop(0, 4, turn, 0)
        return carry

    lax.fori_loop(1, nz + 1, gather, 0)

    def drain(k, carry):
        below, above = z - k, z + k
        has_below, has_above = below >= 0, above < nz

        for p in range(2):
            @pl.when(has_below & (z < nz - 1))
            def _():
                kv_copy(s, 0, k, p).wait_send()

            @pl.when(has_below & ((k > 0) | (y == 0)))
            def _():
                kv_copy(s, 1, k, p).wait_send()

            @pl.when(has_above & (z > 0))
            def _():
                qg_copy(s, 0, k, p).wait_send()
                if p == 0:
                    st_copy(s, 0, k).wait_send()

            @pl.when(has_above & ((k > 0) | (y == 1)))
            def _():
                qg_copy(s, 1, k, p).wait_send()
                if p == 0:
                    st_copy(s, 1, k).wait_send()

            @pl.when((k <= z) & (z < nz - 1))
            def _():
                dq_copy(s, 0, k, p).wait_send()

            @pl.when((k >= z) & (z > 0))
            def _():
                dq_copy(s, 1, k, p).wait_send()

            dq_copy(s, 2, k, p).wait_send()
        return carry

    lax.fori_loop(0, nz, drain, 0)
    for d in range(1, nsp):
        lat_copy(d).wait_send()
    for d in range(1, ntp):
        share_copy(d).wait_send()


def vmem():
    return pl.BlockSpec(memory_space=pltpu.VMEM)


def body(nsp, ntp, latents, query_heads, key_heads, value_heads, map_outputs, log_sums, out_grad,
         mix_lambda, norm_gain):
    rows, heads, width = query_heads.shape
    flat = (rows, heads * width)
    slab = latents.shape[1] // nsp
    nz = nsp // 2
    dma = pltpu.SemaphoreType.DMA
    dq, dk, dv, wg = pl.pallas_call(
        functools.partial(main_kernel, nsp, ntp, heads, width),
        out_shape=(
            jax.ShapeDtypeStruct(query_heads.shape, BF16),
            jax.ShapeDtypeStruct(query_heads.shape, BF16),
            jax.ShapeDtypeStruct(query_heads.shape, BF16),
            jax.ShapeDtypeStruct((slab, heads * width), F32),
        ),
        in_specs=[pl.BlockSpec(memory_space=pltpu.SMEM)] + [vmem()] * 8,
        out_specs=(vmem(),) * 4,
        scratch_shapes=[
            pltpu.VMEM(flat, BF16),
            pltpu.VMEM((heads, rows, width), F32),
            pltpu.VMEM((heads, 4, rows), F32),
            pltpu.VMEM(flat, BF16),
            pltpu.VMEM((nsp, 2) + flat, BF16),
            pltpu.VMEM((nsp, 2) + flat, BF16),
            pltpu.VMEM((nsp, heads, 4, rows), F32),
            pltpu.VMEM((nsp,) + flat, BF16),
            pltpu.VMEM((nsp, rows, slab), BF16),
            pltpu.VMEM(flat, F32),
            pltpu.VMEM(flat, F32),
            pltpu.VMEM(flat, F32),
            dma((2, 2, nz)), dma((2, 2, nz)), dma((2, nz)), dma((3, 2, nz)),
            dma((2, nsp)), dma((2, nsp)), dma((nsp,)), dma((2, nsp)),
            dma((nsp,)), dma((nsp,)), dma((ntp,)), dma((ntp,)),
            dma,
        ],
        compiler_params=pltpu.CompilerParams(collective_id=0, has_side_effects=True),
        name="main",
    )(
        mix_lambda,
        norm_gain[None, :],
        latents,
        key_heads.reshape(flat),
        value_heads.reshape(flat),
        query_heads.reshape(flat),
        map_outputs,
        out_grad,
        jnp.transpose(log_sums, (1, 0, 2)),
    )
    return dq, dk, dv, wg


def row_norm_backward(heads, width, small, maps, grad_ref, row_ref):
    count = maps.shape[0]
    for h in range(heads):
        first = maps[:, 0, h, :].astype(F32)
        second = maps[:, 1, h, :].astype(F32)
        lam = small[heads, 1:2, h : h + 1]
        combined = first - lam * second
        inverse = lax.rsqrt(jnp.mean(combined * combined, axis=-1, keepdims=True) + EPSILON)
        weighted = small[heads, 0:1, :width] * maps[:, 2, h, :].astype(F32)
        grad = (
            inverse * weighted
            - inverse**3 * combined * jnp.mean(combined * weighted, axis=-1, keepdims=True)
        ).astype(BF16)
        grad_ref[:, h * width : (h + 1) * width] = grad
        wide = grad.astype(F32)
        row_ref[h, 0:1] = small[h, 0:1, :count] * LOG2E
        row_ref[h, 1:2] = small[h, 1:2, :count] * LOG2E - jnp.log(lam) * LOG2E
        lane = lax.broadcasted_iota(jnp.int32, wide.shape, 1)
        terms = jnp.where(lane == 0, jnp.sum(wide * first, axis=-1, keepdims=True),
                          jnp.sum(wide * second, axis=-1, keepdims=True))
        row_ref[h, 2:4] = jnp.transpose(terms)[0:2]


def hub_kernel(nsp, ntp, heads, width, small, lat, own_k, own_v, own_q, maps,
               dq_out, dk_out, dv_out, wg_out,
               own_g, row, blk, stb, dq_acc, dk_acc, dv_acc, db, out_b, in_b, in_a, kt, kin, kst, kret, latb,
               f_s, z_s, r_s, b_r, st_r, d_s, d_r, ob_s, ib_r, ia_r, kt_s, kin_r, tot_s, kst_s, kret_r,
               la_s, la_r, lb_s, lb_r, own_sem):
    nz = nsp // 2
    low, high, top = nz // 2 - 1, nz // 2, nz - 1
    s = lax.axis_index("sp")
    t = lax.axis_index("tp")
    z, y = s // 2, lax.rem(s, 2)
    rows = own_k.shape[0]
    span = 2 * rows
    pair = heads // 2
    lanes = pair * width
    part = rows // ntp
    slab = lat.shape[1] // nsp
    score_scale = (width // 2) ** (-0.5)
    exp_scale = score_scale * LOG2E
    partner = 2 * z + 1 - y
    Q, K, V, G, ST = range(5)

    barrier = pltpu.get_barrier_semaphore()
    for d in range(1, nsp):
        pl.semaphore_signal(barrier, inc=1, device_id={"sp": lax.rem(s + d, nsp)}, device_id_type=MESH)
    for d in range(1, ntp):
        pl.semaphore_signal(barrier, inc=1, device_id={"tp": lax.rem(t + d, ntp)}, device_id_type=MESH)
    pl.semaphore_wait(barrier, nsp - 1 + ntp - 1)

    def copy(src, dst, send, recv, to):
        return pltpu.make_async_remote_copy(
            src_ref=src, dst_ref=dst, send_sem=send, recv_sem=recv,
            device_id={"sp": to}, device_id_type=MESH)

    def at_level(level):
        return 2 * level + y

    def lane_of(p):
        return pl.ds(pl.multiple_of(p * lanes, lanes), lanes)

    def half_of(p):
        return pl.ds(pl.multiple_of(p * rows, rows), rows)

    owned = (own_q, own_k, own_v, own_g)

    def source(a, p):
        if a == ST:
            return row.at[pl.ds(p * pair, pair)]
        return owned[a].at[:, lane_of(p)]

    def landing(a, level, half):
        return stb.at[level, half] if a == ST else blk.at[a, level, half_of(half), :]

    def landed(a, level, half):
        return st_r.at[level, half] if a == ST else b_r.at[a, level, half]

    def swap(a):
        return copy(source(a, 1 - y), landing(a, z, y), f_s.at[a], landed(a, z, y), partner)

    def arrive(a, level, half):
        copy(landing(a, level, half), landing(a, level, half), f_s.at[a], landed(a, level, half), partner).wait_recv()

    def pass_on(a, own):
        half = y if own else 1 - y
        return copy(source(a, y) if own else landing(a, z, half), landing(a, z, half),
                    z_s.at[a, 0 if own else 1], landed(a, z, half), at_level(jnp.where(z > high, high, low)))

    def passes(action, arrays, own):
        for a in arrays:
            if a in (K, V):
                @pl.when(z < low)
                def _():
                    action(pass_on(a, own))
            else:
                @pl.when(z >= high)
                def _():
                    action(pass_on(a, own))

    def relay(a, half):
        return copy(landing(a, top, half), landing(a, top, half), r_s.at[a, half], landed(a, top, half), at_level(low))

    def relays(arrays, half):
        @pl.when(z == high)
        def _():
            for a in arrays:
                arrive(a, top, half)
                relay(a, half).start()

    def start(c):
        c.start()

    def lat_copy(d):
        to = lax.rem(s + d, nsp)
        mine = pl.ds(pl.multiple_of(t * part, part), part)
        return copy(lat.at[mine, pl.ds(pl.multiple_of(to * slab, slab), slab)],
                    latb.at[s, mine, :], la_s.at[d], la_r.at[s], to)

    def own_lat():
        return pltpu.make_async_copy(
            lat.at[:, pl.ds(pl.multiple_of(s * slab, slab), slab)], latb.at[s], own_sem)

    sides = ntp // 2
    side, core = t // 2, lax.rem(t, 2)

    def share_copy(b, k):
        away = lax.rem(side + (k if k < sides else k - sides), sides)
        quarter = t if k < sides else 2 * away + core
        to = 2 * away + core if 0 < k < sides else 2 * side + 1 - core
        at = pl.ds(pl.multiple_of(quarter * part, part), part)
        return pltpu.make_async_remote_copy(
            src_ref=latb.at[b, at, :], dst_ref=latb.at[b, at, :],
            send_sem=lb_s.at[b, k], recv_sem=lb_r.at[b, quarter],
            device_id={"tp": to}, device_id_type=MESH)

    def share_arrive(b, quarter):
        at = pl.ds(pl.multiple_of(quarter * part, part), part)
        pltpu.make_async_remote_copy(
            src_ref=latb.at[b, at, :], dst_ref=latb.at[b, at, :],
            send_sem=lb_s.at[b, 0], recv_sem=lb_r.at[b, quarter],
            device_id={"tp": 2 * side + 1 - core}, device_id_type=MESH).wait_recv()

    def group_of(src, dst, group):
        sz, dz = src // 2, dst // 2
        late = (sz >= high) & (dz < high)
        upper = (sz >= high) & (dz >= high) & (dz < sz)
        first = (lax.rem(src, 2) == lax.rem(dst, 2)) & ((dz > sz) | (sz < high))
        if group >= 3:
            return late & ((dz < low) if group == 3 else (dz >= low))
        if group == 2:
            return upper
        rest = jnp.logical_not(late | upper)
        return rest & (first if group == 0 else jnp.logical_not(first))

    def lat_send(group):
        for d in range(1, nsp):
            @pl.when(group_of(s, lax.rem(s + d, nsp), group))
            def _():
                lat_copy(d).start()

    def share_send(group):
        def step(d, carry):
            b = lax.rem(s + d, nsp)

            @pl.when(group_of(b, s, group))
            def _():
                mine = pl.ds(pl.multiple_of(t * part, part), part)
                copy(latb.at[b, mine, :], latb.at[b, mine, :], la_s.at[1], la_r.at[b], partner).wait_recv()
                for k in reversed(range(sides)):
                    share_copy(b, k).start()
            return carry
        lax.fori_loop(1, nsp, step, 0)

    def share_hand(group):
        def hand(d, carry):
            b = lax.rem(s + d, nsp)

            @pl.when(group_of(b, s, group))
            def _():
                for k in range(sides + 1, 2 * sides):
                    share_arrive(b, 2 * lax.rem(side + k - sides, sides) + core)
                    share_copy(b, k).start()
            return carry
        lax.fori_loop(1, nsp, hand, 0)

    def lat_share(group):
        share_send(group)
        share_hand(group)

    swap(Q).start()
    passes(start, (Q, K, V), True)
    swap(K).start()
    swap(V).start()
    @pl.when(z >= low)
    def _():
        lat_send(0)
    own_lat().start()

    row_norm_backward(heads, width, small, maps, own_g, row)

    swap(G).start()
    swap(ST).start()
    passes(start, (ST, G), True)

    for a in (Q, K, V, G):
        blk[a, z, half_of(y), :] = owned[a][:, lane_of(y)]
    stb[z, y] = row[pl.ds(y * pair, pair)]
    dq_acc[...] = jnp.zeros_like(dq_acc)
    dk_acc[...] = jnp.zeros_like(dk_acc)
    dv_acc[...] = jnp.zeros_like(dv_acc)

    for a in (Q, K, V, ST, G):
        arrive(a, z, 1 - y)
        passes(start, (a,), False)
        if a == Q:
            relays((Q,), y)
        if a == K:
            relays((ST, G), y)
        if a == V:
            relays((Q,), 1 - y)

            @pl.when(z < low)
            def _():
                lat_send(0)


    lane_id = lax.broadcasted_iota(jnp.int32, (1, width), 1)
    first_map = jnp.where(lane_id < width // 2, 1.0, 0.0).astype(BF16)
    second_map = jnp.where(lane_id < width // 2, 0.0, 1.0).astype(BF16)

    def split(x):
        return jnp.concatenate([x * first_map, x * second_map], axis=0)

    def visit(qz, kz, slot, diagonal):
        def one(h, carry):
            at = pl.ds(pl.multiple_of(h * width, width), width)
            for a in range(2):
                start_row = a * rows if diagonal else 0
                kr = pl.ds(a * rows, rows)
                qr = pl.ds(start_row, span - start_row)
                count = span - start_row
                keys = split(blk[K, kz, kr, at])
                queries = split(blk[Q, qz, qr, at])
                grads = blk[G, qz, qr, at]
                scores = dot_nt(blk[K, kz, kr, at], queries)
                mixed = dot_nt(blk[V, kz, kr, at], grads)
                stats = jnp.concatenate([stb[qz, p, h] for p in range(start_row // rows, 2)], axis=1)
                x1 = scores[:, :count] * exp_scale - stats[0:1]
                x2 = scores[:, count:] * exp_scale - stats[1:2]
                if diagonal:
                    seen = (lax.broadcasted_iota(jnp.int32, (rows, count), 0)
                            <= lax.broadcasted_iota(jnp.int32, (rows, count), 1))
                    x1 = jnp.where(seen, x1, -jnp.inf)
                    x2 = jnp.where(seen, x2, -jnp.inf)
                p1 = jnp.exp2(x1)
                p2 = jnp.exp2(x2)
                g1 = (p1 * (mixed - stats[2:3])).astype(BF16)
                g2 = (p2 * (stats[3:4] - mixed)).astype(BF16)
                dv_acc[slot, kr, at] += dot_nn((p1 - p2).astype(BF16), grads)
                dk_acc[slot, kr, at] += dot_nn(jnp.concatenate([g1, g2], axis=1), queries)
                dq_acc[qz, h, :, qr] += dot_tn(keys, jnp.concatenate([g1, g2], axis=0))
            return carry
        lax.fori_loop(0, pair, one, 0)

    def dq_value(level, c):
        at = pl.ds(c * rows, rows)
        return jnp.concatenate([jnp.transpose(dq_acc[level, h, :, at]) for h in range(pair)], axis=1) * score_scale

    def grad_copy(level, lane, c):
        if lane == 0:
            to = partner
        elif lane == 1:
            down = high if level == 0 else 0
            to = at_level(jnp.where(z == low, down, jnp.where(z == high, top, low)))
        else:
            to = at_level(high)
        piece = db.at[level, y, half_of(c), :]
        return copy(piece, piece, d_s.at[level, lane, c], d_r.at[level, y, c], to)

    def grad_lanes(level):
        chained = (z <= high) if level == 0 else (z == high) | (z == low)
        if level != low:
            return ((0, None), (1, chained))
        return ((0, None), (1, chained), (2, z == low))

    def grad_each(level, action, chunks=(0, 1), only=(0, 1, 2)):
        for c in chunks:
            for lane, ok in reversed(grad_lanes(level)):
                if lane not in only:
                    continue
                if ok is None:
                    action(grad_copy(level, lane, c))
                else:
                    @pl.when(ok)
                    def _():
                        action(grad_copy(level, lane, c))

    def grad_arrive(level, p, c):
        piece = db.at[level, p, half_of(c), :]
        copy(piece, piece, d_s.at[level, 0, c], d_r.at[level, p, c], partner).wait_recv()

    def part_copy(i, c):
        return copy(out_b.at[i, half_of(c), :], in_b.at[i, half_of(c), :], ob_s.at[i, c], ib_r.at[i, c],
                    at_level(jnp.where(z == low, high, low)))

    def top_copy(c):
        return copy(out_b.at[0, half_of(c), :], in_a.at[half_of(c), :], ob_s.at[0, c], ia_r.at[c], at_level(high))

    def rows_of(c):
        return slice(c * rows, (c + 1) * rows)

    def key_copy(i):
        return copy(kt.at[i], kin.at[i], kt_s.at[i], kin_r.at[i], at_level(low))

    def total_copy(i, half):
        return copy(kt.at[i, half_of(half), :], kret.at[i, y], tot_s.at[i, half], kret_r.at[i, y], half)

    def return_copy(i):
        return copy(kst.at[i], kret.at[i, y], kst_s.at[i], kret_r.at[i, y], partner)

    @pl.when(z >= low)
    def _():
        lat_send(1)

    visit(z, z, 0, True)
    relays((ST, G), 1 - y)

    @pl.when(z >= high)
    def _():
        for c in range(2):
            out_b[0, rows_of(c)] = dq_value(z, c).astype(BF16)

    @pl.when(z == high)
    def _():
        lat_send(3)
        for c in range(2):
            part_copy(0, c).start()

    @pl.when(z > high)
    def _():
        for c in range(2):
            top_copy(c).start()
        lat_send(3)
        lat_send(2)

    @pl.when(z < low)
    def _():
        for c in range(2):
            db[0, y, rows_of(c)] = dq_value(0, c).astype(BF16)
        grad_each(0, start)
        for i in range(2):
            kt[i] = (dv_acc[0] if i else dk_acc[0] * score_scale).astype(BF16)
            key_copy(i).start()
        lat_send(1)

    def return_keys():
        for i, acc, scale in ((0, dk_acc, score_scale), (1, dv_acc, 1.0)):
            kst[i] = (acc[0, half_of(1 - y), :] * scale).astype(BF16)
            return_copy(i).start()
            kret[i, y] = (acc[0, half_of(y), :] * scale).astype(BF16)

    def hand_on(level):
        for c in range(2):
            grad_arrive(level, y, c)
            grad_each(level, start, (c,))

    def total(level):
        i = level - high
        for c in range(2):
            part_copy(i, c).wait_recv()
            whole = dq_value(level, c) + in_b[i, rows_of(c)].astype(F32)
            if level == top:
                above = in_a[rows_of(c)].astype(F32)
                whole = whole + jnp.where(z == high, above, jnp.zeros_like(above))
            db[level, y, rows_of(c)] = whole.astype(BF16)
            grad_each(level, start, (c,))

    def key_results(which=(0, 1)):
        for i in which:
            copy(kst.at[i], kret.at[i, 1 - y], kst_s.at[i], kret_r.at[i, 1 - y], partner).wait_recv()

            @pl.when(z < low)
            def _():
                copy(kst.at[i], kret.at[i, y], kst_s.at[i], kret_r.at[i, y], partner).wait_recv()
            out = dv_out if i else dk_out
            for p in range(2):
                for h in range(pair):
                    out[:, p * pair + h, :] = kret[i, p, :, h * width : (h + 1) * width]

    def query_results():
        for p in range(2):
            for h in range(pair):
                dq_out[:, p * pair + h, :] = db[z, p, half_of(y), h * width : (h + 1) * width]

    def weights(level):
        for c in range(2):
            grad_arrive(level, 1 - y, c)
        for half in range(2):
            b = 2 * level + half

            @pl.when(s != b)
            def _():
                for k in range(sides):
                    share_arrive(b, 2 * lax.rem(side + k, sides) + 1 - core)
        feed = latb[2 * level : 2 * level + 2].reshape(span, slab)
        for p in range(2):
            at = slice(p * lanes, (p + 1) * lanes)
            term = dot_tn(feed, db[level, p])
            if level == 0:
                wg_out[:, at] = term
            else:
                wg_out[:, at] += term

    @pl.when(z == low)
    def _():
        def step(i, carry):
            qz = jnp.where(i == 0, low, high + (i - 1) // 2)
            kz = jnp.where(i == 0, 0, lax.rem(i - 1, 2))

            @pl.when(i == 0)
            def _():
                for half in range(2):
                    arrive(K, 0, half)
                    arrive(V, 0, half)

            @pl.when((i > 0) & (kz == 0))
            def _():
                for a in (Q, ST, G):
                    for half in range(2):
                        arrive(a, qz, half)

            visit(qz, kz, 1 - kz, False)

            @pl.when(i == 0)
            def _():
                for c in range(2):
                    db[low, y, rows_of(c)] = dq_value(low, c).astype(BF16)
                grad_each(low, start)
                share_send(0)

            @pl.when((i > 0) & (kz == 1))
            def _():
                for c in range(2):
                    out_b[qz - high, rows_of(c)] = dq_value(qz, c).astype(BF16)
                    part_copy(qz - high, c).start()

            @pl.when((qz == high) & (kz == 1))
            def _():
                share_hand(0)

            @pl.when((qz == top) & (kz == 0))
            def _():
                for c in range(2):
                    grad_arrive(0, y, c)
                grad_each(0, start, only=(0,))
            return carry
        lax.fori_loop(0, 5, step, 0)
        grad_each(0, start, only=(1,))
        return_keys()

        def key_total(j):
            key_copy(j).wait_recv()
            acc = dv_acc[1] if j else dk_acc[1] * score_scale
            kt[j] = (acc + kin[j].astype(F32)).astype(BF16)
            for half in range(2):
                total_copy(j, half).start()

        key_total(0)
        total(high)
        total(top)
        key_total(1)
        lat_share(1)

    @pl.when(z == high)
    def _():
        visit(top, high, 0, False)
        for c in range(2):
            top_copy(c).wait_recv()
            out_b[1, rows_of(c)] = (dq_value(top, c) + in_a[rows_of(c)].astype(F32)).astype(BF16)
            part_copy(1, c).start()
        return_keys()
        share_send(0)
        hand_on(low)
        share_hand(0)
        total(high)
        lat_send(4)
        share_send(2)
        key_results()
        share_hand(2)
        total(top)
        hand_on(0)
        share_send(1)
        share_hand(1)

    @pl.when(z < low)
    def _():
        share_send(0)
        hand_on(low)
        share_hand(0)
        share_send(1)
        share_hand(1)
        share_send(3)
        share_hand(3)

    @pl.when(z > high)
    def _():
        return_keys()
        share_send(0)
        hand_on(low)
        share_hand(0)
        key_results()
        lat_send(4)
        hand_on(high)
        hand_on(top)
        hand_on(0)
        share_send(1)
        share_hand(1)

    own_lat().wait()
    for level in range(high):
        weights(level)

        @pl.when(z < low)
        def _():
            hand_on(high + level)

    @pl.when(z < high)
    def _():
        query_results()
        share_send(4)

        @pl.when(z == low)
        def _():
            key_results()

        @pl.when(z < low)
        def _():
            key_results((0,))
        share_hand(4)

    for level in range(high, nz):
        weights(level)

        @pl.when(z == level)
        def _():
            query_results()

    @pl.when(z < low)
    def _():
        key_results((1,))

    def sent(c):
        c.wait_send()


    for a in range(5):
        sent(swap(a))
    for own in (True, False):
        passes(sent, (Q, K, V, ST, G), own)
    for a in (Q, ST, G):
        @pl.when(z == high)
        def _():
            for half in range(2):
                sent(relay(a, half))
    for level in range(nz):
        grad_each(level, sent)
    for i in range(2):
        @pl.when(z >= low)
        def _():
            sent(return_copy(i))

        @pl.when((z == low) | (z == high))
        def _():
            for c in range(2):
                sent(part_copy(i, c))

        @pl.when(z == low)
        def _():
            for half in range(2):
                sent(total_copy(i, half))

        @pl.when(z < low)
        def _():
            sent(key_copy(i))

    @pl.when(z > high)
    def _():
        for c in range(2):
            sent(top_copy(c))
    for d in range(1, nsp):
        sent(lat_copy(d))

    def drain(d, carry):
        for k in range(2 * sides):
            if k != sides:
                sent(share_copy(lax.rem(s + d, nsp), k))
        return carry
    lax.fori_loop(1, nsp, drain, 0)


def finish_kernel(a, b, c, d, a_out, b_out, c_out, d_out, sems):
    stores = [
        pltpu.make_async_copy(src, dst, sems.at[i])
        for i, (src, dst) in enumerate(((a, a_out), (b, b_out), (c, c_out), (d, d_out)))
    ]
    for store in stores:
        store.start()
    for store in stores:
        store.wait()


def far():
    return pl.BlockSpec(memory_space=pltpu.HBM)


def hub_body(nsp, ntp, latents, query_heads, key_heads, value_heads, map_outputs, log_sums, out_grad,
             mix_lambda, norm_gain):
    rows, heads, width = query_heads.shape
    flat = (rows, heads * width)
    slab = latents.shape[1] // nsp
    nz = nsp // 2
    pair = heads // 2
    block = (2 * rows, pair * width)
    half = (rows, pair * width)
    dma = pltpu.SemaphoreType.DMA
    room = max(rows, width, heads)

    sums = jnp.transpose(log_sums, (1, 2, 0))
    small = (
        jnp.pad(sums, ((0, 1), (0, 0), (0, room - rows)))
        + jnp.pad(norm_gain[None, None, :], ((heads, 0), (0, 1), (0, room - width)))
        + jnp.pad(mix_lambda[None, None, :], ((heads, 0), (1, 0), (0, room - heads)))
    )
    results = pl.pallas_call(
        functools.partial(hub_kernel, nsp, ntp, heads, width),
        out_shape=(
            jax.ShapeDtypeStruct(query_heads.shape, BF16),
            jax.ShapeDtypeStruct(query_heads.shape, BF16),
            jax.ShapeDtypeStruct(query_heads.shape, BF16),
            jax.ShapeDtypeStruct((slab, heads * width), F32),
        ),
        in_specs=[vmem(), far()] + [vmem()] * 4,
        out_specs=(vmem(),) * 4,
        scratch_shapes=[
            pltpu.VMEM(flat, BF16),
            pltpu.VMEM((heads, 4, rows), F32),
            pltpu.VMEM((4, nz) + block, BF16),
            pltpu.VMEM((nz, 2, pair, 4, rows), F32),
            pltpu.VMEM((nz, pair, width, 2 * rows), F32),
            pltpu.VMEM((2,) + block, F32),
            pltpu.VMEM((2,) + block, F32),
            pltpu.VMEM((nz, 2) + block, BF16),
            pltpu.VMEM((2,) + block, BF16),
            pltpu.VMEM((2,) + block, BF16),
            pltpu.VMEM(block, BF16),
            pltpu.VMEM((2,) + block, BF16),
            pltpu.VMEM((2,) + block, BF16),
            pltpu.VMEM((2,) + half, BF16),
            pltpu.VMEM((2, 2) + half, BF16),
            pltpu.VMEM((nsp, rows, slab), BF16),
            dma((5,)), dma((5, 2)), dma((5, 2)), dma((4, nz, 2)), dma((nz, 2)), dma((nz, 3, 2)), dma((nz, 2, 2)),
            dma((2, 2)), dma((2, 2)), dma((2,)), dma((2,)), dma((2,)), dma((2, 2)), dma((2,)), dma((2, 2)),
            dma((nsp,)), dma((nsp,)), dma((nsp, ntp)), dma((nsp, ntp)),
            dma,
        ],
        compiler_params=pltpu.CompilerParams(
            collective_id=0, has_side_effects=True, vmem_limit_bytes=52500000),
        name="hub",
    )(
        small,
        latents,
        key_heads.reshape(flat),
        value_heads.reshape(flat),
        query_heads.reshape(flat),
        jnp.concatenate([map_outputs, out_grad[:, None]], axis=1),
    )
    return pl.pallas_call(
        finish_kernel,
        out_shape=tuple(jax.ShapeDtypeStruct(a.shape, a.dtype) for a in results),
        in_specs=[vmem()] * 4,
        out_specs=(far(),) * 4,
        scratch_shapes=[pltpu.SemaphoreType.DMA((4,))],
        compiler_params=pltpu.CompilerParams(vmem_limit_bytes=52500000),
        name="finish",
    )(*results)


def solution(mesh):
    placed = (
        P("sp", None),
        P("sp", "tp", None),
        P("sp", "tp", None),
        P("sp", "tp", None),
        P("sp", None, "tp", None),
        P("sp", "tp", None),
        P("sp", "tp", None),
        P("tp"),
        P(),
    )
    nsp, ntp = mesh.shape["sp"], mesh.shape["tp"]

    def chosen(*args):
        heads = args[1].shape[1]
        return (hub_body if nsp == 8 and heads % 2 == 0 else body)(nsp, ntp, *args)

    return jax.shard_map(
        chosen,
        mesh=mesh,
        in_specs=placed,
        out_specs=(P("sp", "tp", None), P("sp", "tp", None), P("sp", "tp", None), P("sp", "tp")),
        check_vma=False,
    )
```

```python
import functools
import math

import jax
import jax.numpy as jnp
from jax import lax
from jax.experimental import pallas as pl
from jax.experimental.pallas import tpu as pltpu
from jax.sharding import PartitionSpec as P

EPSILON = 1e-05
LOG2E = math.log2(math.e)
F32 = jnp.float32
BF16 = jnp.bfloat16
MESH = pl.DeviceIdType.MESH


def dot_nn(a, b):
    return lax.dot_general(a, b, (((1,), (0,)), ((), ())), preferred_element_type=F32)


def dot_nt(a, b):
    return lax.dot_general(a, b, (((1,), (1,)), ((), ())), preferred_element_type=F32)


def dot_tn(a, b):
    return lax.dot_general(a, b, (((0,), (0,)), ((), ())), preferred_element_type=F32)


def norm_backward(heads, width, lam_ref, gain_ref, mo_ref, og_ref, lse_ref, grad_ref, col_ref, row_ref):
    for h in range(heads):
        first = mo_ref[:, 0, h, :].astype(F32)
        second = mo_ref[:, 1, h, :].astype(F32)
        lam = lam_ref[h]
        combined = first - lam * second
        inverse = lax.rsqrt(jnp.mean(combined * combined, axis=-1, keepdims=True) + EPSILON)
        weighted = gain_ref[...] * og_ref[:, h, :].astype(F32)
        grad = (
            inverse * weighted
            - inverse**3 * combined * jnp.mean(combined * weighted, axis=-1, keepdims=True)
        ).astype(BF16)
        grad_ref[:, h * width : (h + 1) * width] = grad
        wide = grad.astype(F32)
        lse = lse_ref[h] * LOG2E
        log_lam = jnp.log(jnp.full((1, 1), lam, F32)) * LOG2E
        lane = lax.broadcasted_iota(jnp.int32, wide.shape, 1)
        stats = jnp.where(lane == 0, lse[:, 0:1], lse[:, 1:2] - log_lam)
        stats = jnp.where(lane == 2, jnp.sum(wide * first, axis=-1, keepdims=True), stats)
        stats = jnp.where(lane == 3, jnp.sum(wide * second, axis=-1, keepdims=True), stats)
        col_ref[h] = stats
        row_ref[h] = jnp.transpose(stats)[0:4]


def main_kernel(nsp, ntp, heads, width, lam, gain, lat, own_k, own_v, own_q, mo, og, lse,
                dq_out, dk_out, dv_out, wg_out,
                own_g, col, row, own_dq, kvb, qgb, stb, dqb, latb, dq_acc, dk_acc, dv_acc,
                kv_s, qg_s, st_s, dq_s, kv_r, qg_r, st_r, dq_r,
                la_s, la_r, lb_s, lb_r, own_sem):
    nz = nsp // 2
    s = lax.axis_index("sp")
    t = lax.axis_index("tp")
    z, y = s // 2, lax.rem(s, 2)
    rows = own_k.shape[0]
    part = rows // ntp
    slab = lat.shape[1] // nsp
    score_scale = (width // 2) ** (-0.5)
    exp_scale = score_scale * LOG2E

    barrier = pltpu.get_barrier_semaphore()
    for d in range(1, nsp):
        pl.semaphore_signal(barrier, inc=1, device_id={"sp": lax.rem(s + d, nsp)}, device_id_type=MESH)
    for d in range(1, ntp):
        pl.semaphore_signal(barrier, inc=1, device_id={"tp": lax.rem(t + d, ntp)}, device_id_type=MESH)
    pl.semaphore_wait(barrier, nsp - 1 + ntp - 1)

    def copy(src, dst, send, recv, to):
        return pltpu.make_async_remote_copy(
            src_ref=src, dst_ref=dst, send_sem=send, recv_sem=recv,
            device_id={"sp": to}, device_id_type=MESH)

    side = 2 * z + (1 - y)

    def kv_copy(block, lane, k, p, src=None):
        to = jnp.minimum(s + 2, nsp - 1) if lane == 0 else side
        return copy(kvb.at[block, p] if src is None else src, kvb.at[block, p],
                    kv_s.at[lane, p, k], kv_r.at[p, block], to)

    def qg_copy(block, lane, k, p, src=None):
        to = jnp.maximum(s - 2, 0) if lane == 0 else side
        return copy(qgb.at[block, p] if src is None else src, qgb.at[block, p],
                    qg_s.at[lane, p, k], qg_r.at[p, block], to)

    def st_copy(block, lane, k, src=None):
        to = jnp.maximum(s - 2, 0) if lane == 0 else side
        return copy(stb.at[block] if src is None else src, stb.at[block],
                    st_s.at[lane, k], st_r.at[block], to)

    for p, src in ((0, own_k), (1, own_v)):
        @pl.when(z < nz - 1)
        def _():
            kv_copy(s, 0, 0, p, src).start()

        @pl.when(y == 0)
        def _():
            kv_copy(s, 1, 0, p, src).start()

    @pl.when(z > 0)
    def _():
        qg_copy(s, 0, 0, 0, own_q).start()

    @pl.when(y == 1)
    def _():
        qg_copy(s, 1, 0, 0, own_q).start()

    norm_backward(heads, width, lam, gain, mo, og, lse, own_g, col, row)

    @pl.when(z > 0)
    def _():
        st_copy(s, 0, 0, row).start()
        qg_copy(s, 0, 0, 1, own_g).start()

    @pl.when(y == 1)
    def _():
        st_copy(s, 1, 0, row).start()
        qg_copy(s, 1, 0, 1, own_g).start()

    lane_id = lax.broadcasted_iota(jnp.int32, (1, width), 1)
    low = jnp.where(lane_id < width // 2, 1.0, 0.0).astype(BF16)
    high = jnp.where(lane_id < width // 2, 0.0, 1.0).astype(BF16)

    def split(x):
        return jnp.concatenate([x * low, x * high], axis=0)

    def query_side(k_at, v_at, diagonal):
        def one(h, carry):
            at = pl.ds(pl.multiple_of(h * width, width), width)
            keys = split(k_at[:, at])
            scores = dot_nt(own_q[:, at], keys)
            mixed = dot_nt(own_g[:, at], v_at[:, at])
            stats = col[h]
            x1 = scores[:, :rows] * exp_scale - stats[:, 0:1]
            x2 = scores[:, rows:] * exp_scale - stats[:, 1:2]
            if diagonal:
                seen = (lax.broadcasted_iota(jnp.int32, (rows, rows), 1)
                        <= lax.broadcasted_iota(jnp.int32, (rows, rows), 0))
                x1 = jnp.where(seen, x1, -jnp.inf)
                x2 = jnp.where(seen, x2, -jnp.inf)
            g1 = (jnp.exp2(x1) * (mixed - stats[:, 2:3])).astype(BF16)
            g2 = (jnp.exp2(x2) * (stats[:, 3:4] - mixed)).astype(BF16)
            part_dq = dot_nn(jnp.concatenate([g1, g2], axis=1), keys)
            if diagonal:
                dq_acc[:, at] = part_dq
            else:
                dq_acc[:, at] += part_dq
            return carry
        lax.fori_loop(0, heads, one, 0)

    def key_side(q_at, g_at, row_at, diagonal):
        def one(h, carry):
            at = pl.ds(pl.multiple_of(h * width, width), width)
            queries = split(q_at[:, at])
            grads = g_at[:, at]
            scores = dot_nt(own_k[:, at], queries)
            mixed = dot_nt(own_v[:, at], grads)
            stats = row_at[h]
            x1 = scores[:, :rows] * exp_scale - stats[0:1]
            x2 = scores[:, rows:] * exp_scale - stats[1:2]
            if diagonal:
                seen = (lax.broadcasted_iota(jnp.int32, (rows, rows), 0)
                        <= lax.broadcasted_iota(jnp.int32, (rows, rows), 1))
                x1 = jnp.where(seen, x1, -jnp.inf)
                x2 = jnp.where(seen, x2, -jnp.inf)
            p1 = jnp.exp2(x1)
            p2 = jnp.exp2(x2)
            g1 = (p1 * (mixed - stats[2:3])).astype(BF16)
            g2 = (p2 * (stats[3:4] - mixed)).astype(BF16)
            part_dv = dot_nn((p1 - p2).astype(BF16), grads)
            part_dk = dot_nn(jnp.concatenate([g1, g2], axis=1), queries)
            if diagonal:
                dv_acc[:, at] = part_dv
                dk_acc[:, at] = part_dk
            else:
                dv_acc[:, at] += part_dv
                dk_acc[:, at] += part_dk
            return carry
        lax.fori_loop(0, heads, one, 0)

    def lat_copy(d):
        to = lax.rem(s + d, nsp)
        mine = pl.ds(pl.multiple_of(t * part, part), part)
        return copy(lat.at[mine, pl.ds(pl.multiple_of(to * slab, slab), slab)],
                    latb.at[s, mine, :], la_s.at[d], la_r.at[d], to)

    def own_lat():
        return pltpu.make_async_copy(
            lat.at[pl.ds(pl.multiple_of(t * part, part), part), pl.ds(pl.multiple_of(s * slab, slab), slab)],
            latb.at[s, pl.ds(pl.multiple_of(t * part, part), part), :], own_sem)

    def share_copy(d):
        mine = pl.ds(pl.multiple_of(t * part, part), part)
        return pltpu.make_async_remote_copy(
            src_ref=latb.at[:, mine, :], dst_ref=latb.at[:, mine, :],
            send_sem=lb_s.at[d], recv_sem=lb_r.at[d],
            device_id={"tp": lax.rem(t + d, ntp)}, device_id_type=MESH)

    own_lat().start()
    query_side(own_k, own_v, True)
    key_side(own_q, own_g, row, True)
    for d in range(1, nsp):
        lat_copy(d).start()

    def step(k, carry):
        below, above = z - k, z + k
        has_below, has_above = below >= 0, above < nz
        kb = jnp.maximum(below, 0) * 2 + y
        qb = jnp.minimum(above, nz - 1) * 2 + y

        for p in range(2):
            @pl.when(has_below)
            def _():
                kv_copy(kb, 0, 0, p).wait_recv()
                kv_copy(kb, 1, k, p).start()

            @pl.when(has_below & (z < nz - 1))
            def _():
                kv_copy(kb, 0, k, p).start()

            @pl.when(has_above)
            def _():
                qg_copy(qb, 0, 0, p).wait_recv()
                qg_copy(qb, 1, k, p).start()
                if p == 0:
                    st_copy(qb, 0, 0).wait_recv()
                    st_copy(qb, 1, k).start()

            @pl.when(has_above & (z > 0))
            def _():
                qg_copy(qb, 0, k, p).start()
                if p == 0:
                    st_copy(qb, 0, k).start()

        def turn(c, carry):
            dist = k - c
            other = jnp.where(c == 0, y, 1 - y)
            bz, qz = z - dist, z + dist
            use_kv = (bz >= 0) & (dist < nz) & ((dist > 0) | (y == 1))
            use_qg = (qz < nz) & (dist < nz) & ((dist > 0) | (y == 0))
            kblk = jnp.maximum(bz, 0) * 2 + other
            qblk = jnp.minimum(qz, nz - 1) * 2 + other

            @pl.when(use_kv)
            def _():
                @pl.when(c == 1)
                def _():
                    for p in range(2):
                        kv_copy(kblk, 1, 0, p).wait_recv()
                query_side(kvb.at[kblk, 0], kvb.at[kblk, 1], False)

            @pl.when(use_qg)
            def _():
                @pl.when(c == 1)
                def _():
                    for p in range(2):
                        qg_copy(qblk, 1, 0, p).wait_recv()
                    st_copy(qblk, 1, 0).wait_recv()
                key_side(qgb.at[qblk, 0], qgb.at[qblk, 1], stb.at[qblk], False)
            return carry
        lax.fori_loop(0, 2, turn, 0)
        return carry

    lax.fori_loop(1, nz + 1, step, 0)

    own_dq[...] = (dq_acc[...] * score_scale).astype(BF16)
    half = rows // 2

    def dq_copy(block, lane, idx, p, own=False):
        to = (jnp.minimum(s + 2, nsp - 2 + y), jnp.maximum(s - 2, y), side)[lane]
        at = pl.ds(p * half, half)
        return copy(own_dq.at[at] if own else dqb.at[block, at], dqb.at[block, at],
                    dq_s.at[lane, p, idx], dq_r.at[p, block], to)

    for p in range(2):
        @pl.when(z < nz - 1)
        def _():
            dq_copy(s, 0, z, p, True).start()

        @pl.when(z > 0)
        def _():
            dq_copy(s, 1, z, p, True).start()

        dq_copy(s, 2, z, p, True).start()

    for h in range(heads):
        at = slice(h * width, (h + 1) * width)
        dq_out[:, h, :] = own_dq[:, at]
        dk_out[:, h, :] = (dk_acc[:, at] * score_scale).astype(BF16)
        dv_out[:, h, :] = dv_acc[:, at].astype(BF16)

    own_lat().wait()
    for d in range(1, nsp):
        lat_copy(d).wait_recv()
    for d in range(1, ntp):
        share_copy(d).start()
    for d in range(1, ntp):
        share_copy(d).wait_recv()

    wg_out[...] = dot_tn(latb[s], own_dq[...])

    def add_block(block):
        wg_out[...] += dot_tn(latb[block], dqb[block])

    def gather(k, carry):
        for p in range(2):
            for lane, there, ok, more in (
                (0, z - k, z - k >= 0, z < nz - 1),
                (1, z + k, z + k < nz, z > 0),
            ):
                bz = jnp.clip(there, 0, nz - 1)
                block = bz * 2 + y

                @pl.when(ok)
                def _():
                    dq_copy(block, lane, bz, p).wait_recv()
                    dq_copy(block, 2, bz, p).start()

                @pl.when(ok & more)
                def _():
                    dq_copy(block, lane, bz, p).start()

        def turn(c, carry):
            dist = jnp.where(c < 2, k, k - 1)
            up = lax.rem(c, 2)
            bz = jnp.where(up == 0, z - dist, z + dist)
            ok = (bz >= 0) & (bz < nz) & (dist < nz) & ((dist > 0) | (up == 0))
            other = jnp.where(c < 2, y, 1 - y)
            block = jnp.clip(bz, 0, nz - 1) * 2 + other

            @pl.when(ok)
            def _():
                @pl.when(c >= 2)
                def _():
                    for p in range(2):
                        dq_copy(block, 2, 0, p).wait_recv()
                add_block(block)
            return carry
        lax.fori_loop(0, 4, turn, 0)
        return carry

    lax.fori_loop(1, nz + 1, gather, 0)

    def drain(k, carry):
        below, above = z - k, z + k
        has_below, has_above = below >= 0, above < nz

        for p in range(2):
            @pl.when(has_below & (z < nz - 1))
            def _():
                kv_copy(s, 0, k, p).wait_send()

            @pl.when(has_below & ((k > 0) | (y == 0)))
            def _():
                kv_copy(s, 1, k, p).wait_send()

            @pl.when(has_above & (z > 0))
            def _():
                qg_copy(s, 0, k, p).wait_send()
                if p == 0:
                    st_copy(s, 0, k).wait_send()

            @pl.when(has_above & ((k > 0) | (y == 1)))
            def _():
                qg_copy(s, 1, k, p).wait_send()
                if p == 0:
                    st_copy(s, 1, k).wait_send()

            @pl.when((k <= z) & (z < nz - 1))
            def _():
                dq_copy(s, 0, k, p).wait_send()

            @pl.when((k >= z) & (z > 0))
            def _():
                dq_copy(s, 1, k, p).wait_send()

            dq_copy(s, 2, k, p).wait_send()
        return carry

    lax.fori_loop(0, nz, drain, 0)
    for d in range(1, nsp):
        lat_copy(d).wait_send()
    for d in range(1, ntp):
        share_copy(d).wait_send()


def vmem():
    return pl.BlockSpec(memory_space=pltpu.VMEM)


def body(nsp, ntp, latents, query_heads, key_heads, value_heads, map_outputs, log_sums, out_grad,
         mix_lambda, norm_gain):
    rows, heads, width = query_heads.shape
    flat = (rows, heads * width)
    slab = latents.shape[1] // nsp
    nz = nsp // 2
    dma = pltpu.SemaphoreType.DMA
    dq, dk, dv, wg = pl.pallas_call(
        functools.partial(main_kernel, nsp, ntp, heads, width),
        out_shape=(
            jax.ShapeDtypeStruct(query_heads.shape, BF16),
            jax.ShapeDtypeStruct(query_heads.shape, BF16),
            jax.ShapeDtypeStruct(query_heads.shape, BF16),
            jax.ShapeDtypeStruct((slab, heads * width), F32),
        ),
        in_specs=[pl.BlockSpec(memory_space=pltpu.SMEM)] + [vmem()] * 8,
        out_specs=(vmem(),) * 4,
        scratch_shapes=[
            pltpu.VMEM(flat, BF16),
            pltpu.VMEM((heads, rows, width), F32),
            pltpu.VMEM((heads, 4, rows), F32),
            pltpu.VMEM(flat, BF16),
            pltpu.VMEM((nsp, 2) + flat, BF16),
            pltpu.VMEM((nsp, 2) + flat, BF16),
            pltpu.VMEM((nsp, heads, 4, rows), F32),
            pltpu.VMEM((nsp,) + flat, BF16),
            pltpu.VMEM((nsp, rows, slab), BF16),
            pltpu.VMEM(flat, F32),
            pltpu.VMEM(flat, F32),
            pltpu.VMEM(flat, F32),
            dma((2, 2, nz)), dma((2, 2, nz)), dma((2, nz)), dma((3, 2, nz)),
            dma((2, nsp)), dma((2, nsp)), dma((nsp,)), dma((2, nsp)),
            dma((nsp,)), dma((nsp,)), dma((ntp,)), dma((ntp,)),
            dma,
        ],
        compiler_params=pltpu.CompilerParams(collective_id=0, has_side_effects=True),
        name="main",
    )(
        mix_lambda,
        norm_gain[None, :],
        latents,
        key_heads.reshape(flat),
        value_heads.reshape(flat),
        query_heads.reshape(flat),
        map_outputs,
        out_grad,
        jnp.transpose(log_sums, (1, 0, 2)),
    )
    return dq, dk, dv, wg


def row_norm_backward(heads, width, small, maps, grad_ref, row_ref):
    count = maps.shape[0]
    for h in range(heads):
        first = maps[:, 0, h, :].astype(F32)
        second = maps[:, 1, h, :].astype(F32)
        lam = small[heads, 1:2, h : h + 1]
        combined = first - lam * second
        inverse = lax.rsqrt(jnp.mean(combined * combined, axis=-1, keepdims=True) + EPSILON)
        weighted = small[heads, 0:1, :width] * maps[:, 2, h, :].astype(F32)
        grad = (
            inverse * weighted
            - inverse**3 * combined * jnp.mean(combined * weighted, axis=-1, keepdims=True)
        ).astype(BF16)
        grad_ref[:, h * width : (h + 1) * width] = grad
        wide = grad.astype(F32)
        row_ref[h, 0:1] = small[h, 0:1, :count] * LOG2E
        row_ref[h, 1:2] = small[h, 1:2, :count] * LOG2E - jnp.log(lam) * LOG2E
        lane = lax.broadcasted_iota(jnp.int32, wide.shape, 1)
        terms = jnp.where(lane == 0, jnp.sum(wide * first, axis=-1, keepdims=True),
                          jnp.sum(wide * second, axis=-1, keepdims=True))
        row_ref[h, 2:4] = jnp.transpose(terms)[0:2]


def hub_kernel(nsp, ntp, heads, width, small, lat, own_k, own_v, own_q, maps,
               dq_out, dk_out, dv_out, wg_out,
               own_g, row, blk, stb, dq_acc, dk_acc, dv_acc, db, out_b, in_b, in_a, kt, kin, kst, kret, latb,
               f_s, z_s, r_s, b_r, st_r, d_s, d_r, ob_s, ib_r, ia_r, kt_s, kin_r, tot_s, kst_s, kret_r,
               la_s, la_r, lb_s, lb_r, own_sem):
    nz = nsp // 2
    low, high, top = nz // 2 - 1, nz // 2, nz - 1
    s = lax.axis_index("sp")
    t = lax.axis_index("tp")
    z, y = s // 2, lax.rem(s, 2)
    rows = own_k.shape[0]
    span = 2 * rows
    pair = heads // 2
    lanes = pair * width
    part = rows // ntp
    slab = lat.shape[1] // nsp
    score_scale = (width // 2) ** (-0.5)
    exp_scale = score_scale * LOG2E
    partner = 2 * z + 1 - y
    Q, K, V, G, ST = range(5)

    barrier = pltpu.get_barrier_semaphore()
    for d in range(1, nsp):
        pl.semaphore_signal(barrier, inc=1, device_id={"sp": lax.rem(s + d, nsp)}, device_id_type=MESH)
    for d in range(1, ntp):
        pl.semaphore_signal(barrier, inc=1, device_id={"tp": lax.rem(t + d, ntp)}, device_id_type=MESH)
    pl.semaphore_wait(barrier, nsp - 1 + ntp - 1)

    def copy(src, dst, send, recv, to):
        return pltpu.make_async_remote_copy(
            src_ref=src, dst_ref=dst, send_sem=send, recv_sem=recv,
            device_id={"sp": to}, device_id_type=MESH)

    def at_level(level):
        return 2 * level + y

    def lane_of(p):
        return pl.ds(pl.multiple_of(p * lanes, lanes), lanes)

    def half_of(p):
        return pl.ds(pl.multiple_of(p * rows, rows), rows)

    owned = (own_q, own_k, own_v, own_g)

    def source(a, p):
        if a == ST:
            return row.at[pl.ds(p * pair, pair)]
        return owned[a].at[:, lane_of(p)]

    def landing(a, level, half):
        return stb.at[level, half] if a == ST else blk.at[a, level, half_of(half), :]

    def landed(a, level, half):
        return st_r.at[level, half] if a == ST else b_r.at[a, level, half]

    def swap(a):
        return copy(source(a, 1 - y), landing(a, z, y), f_s.at[a], landed(a, z, y), partner)

    def arrive(a, level, half):
        copy(landing(a, level, half), landing(a, level, half), f_s.at[a], landed(a, level, half), partner).wait_recv()

    def pass_on(a, own):
        half = y if own else 1 - y
        return copy(source(a, y) if own else landing(a, z, half), landing(a, z, half),
                    z_s.at[a, 0 if own else 1], landed(a, z, half), at_level(jnp.where(z > high, high, low)))

    def passes(action, arrays, own):
        for a in arrays:
            if a in (K, V):
                @pl.when(z < low)
                def _():
                    action(pass_on(a, own))
            else:
                @pl.when(z >= high)
                def _():
                    action(pass_on(a, own))

    def relay(a, half):
        return copy(landing(a, top, half), landing(a, top, half), r_s.at[a, half], landed(a, top, half), at_level(low))

    def relays(arrays, half):
        @pl.when(z == high)
        def _():
            for a in arrays:
                arrive(a, top, half)
                relay(a, half).start()

    def start(c):
        c.start()

    def lat_copy(d):
        to = lax.rem(s + d, nsp)
        mine = pl.ds(pl.multiple_of(t * part, part), part)
        return copy(lat.at[mine, pl.ds(pl.multiple_of(to * slab, slab), slab)],
                    latb.at[s, mine, :], la_s.at[d], la_r.at[s], to)

    def own_lat():
        return pltpu.make_async_copy(
            lat.at[:, pl.ds(pl.multiple_of(s * slab, slab), slab)], latb.at[s], own_sem)

    sides = ntp // 2
    side, core = t // 2, lax.rem(t, 2)

    def share_copy(b, k):
        away = lax.rem(side + (k if k < sides else k - sides), sides)
        quarter = t if k < sides else 2 * away + core
        to = 2 * away + core if 0 < k < sides else 2 * side + 1 - core
        at = pl.ds(pl.multiple_of(quarter * part, part), part)
        return pltpu.make_async_remote_copy(
            src_ref=latb.at[b, at, :], dst_ref=latb.at[b, at, :],
            send_sem=lb_s.at[b, k], recv_sem=lb_r.at[b, quarter],
            device_id={"tp": to}, device_id_type=MESH)

    def share_arrive(b, quarter):
        at = pl.ds(pl.multiple_of(quarter * part, part), part)
        pltpu.make_async_remote_copy(
            src_ref=latb.at[b, at, :], dst_ref=latb.at[b, at, :],
            send_sem=lb_s.at[b, 0], recv_sem=lb_r.at[b, quarter],
            device_id={"tp": 2 * side + 1 - core}, device_id_type=MESH).wait_recv()

    def group_of(src, dst, group):
        sz, dz = src // 2, dst // 2
        late = (sz >= high) & (dz < high)
        upper = (sz >= high) & (dz >= high) & (dz < sz)
        first = (lax.rem(src, 2) == lax.rem(dst, 2)) & ((dz > sz) | (sz < high))
        if group in (3, 4):
            return late & ((dz < low) if group == 3 else (dz >= low))
        if group == 2:
            return upper
        rest = jnp.logical_not(late | upper)
        if group == 0:
            return rest & first
        return rest & jnp.logical_not(first) & ((sz >= low) if group == 1 else (sz < low))

    def lat_send(group):
        for d in range(1, nsp):
            @pl.when(group_of(s, lax.rem(s + d, nsp), group))
            def _():
                lat_copy(d).start()

    def share_send(group):
        def step(d, carry):
            b = lax.rem(s + d, nsp)

            @pl.when(group_of(b, s, group))
            def _():
                mine = pl.ds(pl.multiple_of(t * part, part), part)
                copy(latb.at[b, mine, :], latb.at[b, mine, :], la_s.at[1], la_r.at[b], partner).wait_recv()
                for k in reversed(range(sides)):
                    share_copy(b, k).start()
            return carry
        lax.fori_loop(1, nsp, step, 0)

    def share_hand(group):
        def hand(d, carry):
            b = lax.rem(s + d, nsp)

            @pl.when(group_of(b, s, group))
            def _():
                for k in range(sides + 1, 2 * sides):
                    share_arrive(b, 2 * lax.rem(side + k - sides, sides) + core)
                    share_copy(b, k).start()
            return carry
        lax.fori_loop(1, nsp, hand, 0)

    def lat_share(group):
        share_send(group)
        share_hand(group)

    swap(Q).start()
    passes(start, (Q, K, V), True)
    swap(K).start()
    swap(V).start()
    @pl.when(z >= low)
    def _():
        lat_send(0)
    own_lat().start()

    row_norm_backward(heads, width, small, maps, own_g, row)

    swap(G).start()
    swap(ST).start()
    passes(start, (ST, G), True)

    for a in (Q, K, V, G):
        blk[a, z, half_of(y), :] = owned[a][:, lane_of(y)]
    stb[z, y] = row[pl.ds(y * pair, pair)]
    dq_acc[...] = jnp.zeros_like(dq_acc)
    dk_acc[...] = jnp.zeros_like(dk_acc)
    dv_acc[...] = jnp.zeros_like(dv_acc)

    for a in (Q, K, V, ST, G):
        arrive(a, z, 1 - y)
        passes(start, (a,), False)
        if a == Q:
            relays((Q,), y)
        if a == K:
            relays((ST, G), y)
        if a == V:
            relays((Q,), 1 - y)

            @pl.when(z < low)
            def _():
                lat_send(0)


    lane_id = lax.broadcasted_iota(jnp.int32, (1, width), 1)
    first_map = jnp.where(lane_id < width // 2, 1.0, 0.0).astype(BF16)
    second_map = jnp.where(lane_id < width // 2, 0.0, 1.0).astype(BF16)

    def split(x):
        return jnp.concatenate([x * first_map, x * second_map], axis=0)

    def visit(qz, kz, slot, diagonal):
        def one(h, carry):
            at = pl.ds(pl.multiple_of(h * width, width), width)
            for a in range(2):
                start_row = a * rows if diagonal else 0
                kr = pl.ds(a * rows, rows)
                qr = pl.ds(start_row, span - start_row)
                count = span - start_row
                keys = split(blk[K, kz, kr, at])
                queries = split(blk[Q, qz, qr, at])
                grads = blk[G, qz, qr, at]
                scores = dot_nt(blk[K, kz, kr, at], queries)
                mixed = dot_nt(blk[V, kz, kr, at], grads)
                stats = jnp.concatenate([stb[qz, p, h] for p in range(start_row // rows, 2)], axis=1)
                x1 = scores[:, :count] * exp_scale - stats[0:1]
                x2 = scores[:, count:] * exp_scale - stats[1:2]
                if diagonal:
                    seen = (lax.broadcasted_iota(jnp.int32, (rows, count), 0)
                            <= lax.broadcasted_iota(jnp.int32, (rows, count), 1))
                    x1 = jnp.where(seen, x1, -jnp.inf)
                    x2 = jnp.where(seen, x2, -jnp.inf)
                p1 = jnp.exp2(x1)
                p2 = jnp.exp2(x2)
                g1 = (p1 * (mixed - stats[2:3])).astype(BF16)
                g2 = (p2 * (stats[3:4] - mixed)).astype(BF16)
                dv_acc[slot, kr, at] += dot_nn((p1 - p2).astype(BF16), grads)
                dk_acc[slot, kr, at] += dot_nn(jnp.concatenate([g1, g2], axis=1), queries)
                dq_acc[qz, h, :, qr] += dot_tn(keys, jnp.concatenate([g1, g2], axis=0))
            return carry
        lax.fori_loop(0, pair, one, 0)

    def dq_value(level, c):
        at = pl.ds(c * rows, rows)
        return jnp.concatenate([jnp.transpose(dq_acc[level, h, :, at]) for h in range(pair)], axis=1) * score_scale

    def grad_copy(level, lane, c):
        if lane == 0:
            to = partner
        elif lane == 1:
            down = high if level == 0 else 0
            to = at_level(jnp.where(z == low, down, jnp.where(z == high, top, low)))
        else:
            to = at_level(high)
        piece = db.at[level, y, half_of(c), :]
        return copy(piece, piece, d_s.at[level, lane, c], d_r.at[level, y, c], to)

    def grad_lanes(level):
        chained = (z <= high) if level == 0 else (z == high) | (z == low)
        if level != low:
            return ((0, None), (1, chained))
        return ((0, None), (1, chained), (2, z == low))

    def grad_each(level, action, chunks=(0, 1), only=(0, 1, 2)):
        for c in chunks:
            for lane, ok in reversed(grad_lanes(level)):
                if lane not in only:
                    continue
                if ok is None:
                    action(grad_copy(level, lane, c))
                else:
                    @pl.when(ok)
                    def _():
                        action(grad_copy(level, lane, c))

    def grad_arrive(level, p, c):
        piece = db.at[level, p, half_of(c), :]
        copy(piece, piece, d_s.at[level, 0, c], d_r.at[level, p, c], partner).wait_recv()

    def part_copy(i, c):
        return copy(out_b.at[i, half_of(c), :], in_b.at[i, half_of(c), :], ob_s.at[i, c], ib_r.at[i, c],
                    at_level(jnp.where(z == low, high, low)))

    def top_copy(c):
        return copy(out_b.at[0, half_of(c), :], in_a.at[half_of(c), :], ob_s.at[0, c], ia_r.at[c], at_level(high))

    def rows_of(c):
        return slice(c * rows, (c + 1) * rows)

    def key_copy(i):
        return copy(kt.at[i], kin.at[i], kt_s.at[i], kin_r.at[i], at_level(low))

    def total_copy(i, half):
        return copy(kt.at[i, half_of(half), :], kret.at[i, y], tot_s.at[i, half], kret_r.at[i, y], half)

    def return_copy(i):
        return copy(kst.at[i], kret.at[i, y], kst_s.at[i], kret_r.at[i, y], partner)

    @pl.when(z >= low)
    def _():
        lat_send(1)

    visit(z, z, 0, True)
    relays((ST, G), 1 - y)

    @pl.when(z >= high)
    def _():
        for c in range(2):
            out_b[0, rows_of(c)] = dq_value(z, c).astype(BF16)

    @pl.when(z == high)
    def _():
        lat_send(3)
        for c in range(2):
            part_copy(0, c).start()

    @pl.when(z > high)
    def _():
        for c in range(2):
            top_copy(c).start()
        lat_send(3)
        lat_send(2)

    @pl.when(z < low)
    def _():
        for c in range(2):
            db[0, y, rows_of(c)] = dq_value(0, c).astype(BF16)
        grad_each(0, start)
        for i in range(2):
            kt[i] = (dv_acc[0] if i else dk_acc[0] * score_scale).astype(BF16)
            key_copy(i).start()
        lat_send(5)

    def return_keys():
        for i, acc, scale in ((0, dk_acc, score_scale), (1, dv_acc, 1.0)):
            kst[i] = (acc[0, half_of(1 - y), :] * scale).astype(BF16)
            return_copy(i).start()
            kret[i, y] = (acc[0, half_of(y), :] * scale).astype(BF16)

    def hand_on(level):
        for c in range(2):
            grad_arrive(level, y, c)
            grad_each(level, start, (c,))

    def total(level):
        i = level - high
        for c in range(2):
            part_copy(i, c).wait_recv()
            whole = dq_value(level, c) + in_b[i, rows_of(c)].astype(F32)
            if level == top:
                above = in_a[rows_of(c)].astype(F32)
                whole = whole + jnp.where(z == high, above, jnp.zeros_like(above))
            db[level, y, rows_of(c)] = whole.astype(BF16)
            grad_each(level, start, (c,))

    def key_results(which=(0, 1)):
        for i in which:
            copy(kst.at[i], kret.at[i, 1 - y], kst_s.at[i], kret_r.at[i, 1 - y], partner).wait_recv()

            @pl.when(z < low)
            def _():
                copy(kst.at[i], kret.at[i, y], kst_s.at[i], kret_r.at[i, y], partner).wait_recv()
            out = dv_out if i else dk_out
            for p in range(2):
                for h in range(pair):
                    out[:, p * pair + h, :] = kret[i, p, :, h * width : (h + 1) * width]

    def query_results(own):
        for p in range(2):
            @pl.when((y == p) if own else (y != p))
            def _():
                for h in range(pair):
                    dq_out[:, p * pair + h, :] = db[z, p, half_of(y), h * width : (h + 1) * width]

    def weights(level):
        for c in range(2):
            grad_arrive(level, 1 - y, c)
        for half in range(2):
            b = 2 * level + half

            @pl.when(s != b)
            def _():
                for k in range(sides):
                    share_arrive(b, 2 * lax.rem(side + k, sides) + 1 - core)
        feed = latb[2 * level : 2 * level + 2].reshape(span, slab)
        for p in range(2):
            at = slice(p * lanes, (p + 1) * lanes)
            term = dot_tn(feed, db[level, p])
            if level == 0:
                wg_out[:, at] = term
            else:
                wg_out[:, at] += term

    @pl.when(z == low)
    def _():
        def step(i, carry):
            qz = jnp.where(i == 0, low, high + (i - 1) // 2)
            kz = jnp.where(i == 0, 0, lax.rem(i - 1, 2))

            @pl.when(i == 0)
            def _():
                for half in range(2):
                    arrive(K, 0, half)
                    arrive(V, 0, half)

            @pl.when((i > 0) & (kz == 0))
            def _():
                for a in (Q, ST, G):
                    for half in range(2):
                        arrive(a, qz, half)

            visit(qz, kz, 1 - kz, False)

            @pl.when(i == 0)
            def _():
                for c in range(2):
                    db[low, y, rows_of(c)] = dq_value(low, c).astype(BF16)
                grad_each(low, start)
                share_send(0)

            @pl.when((i > 0) & (kz == 1))
            def _():
                for c in range(2):
                    out_b[qz - high, rows_of(c)] = dq_value(qz, c).astype(BF16)
                    part_copy(qz - high, c).start()

            @pl.when((qz == high) & (kz == 1))
            def _():
                share_hand(0)

            @pl.when((qz == top) & (kz == 0))
            def _():
                for c in range(2):
                    grad_arrive(0, y, c)
                grad_each(0, start, only=(0,))
            return carry
        lax.fori_loop(0, 5, step, 0)
        grad_each(0, start, only=(1,))
        return_keys()

        def key_total(j):
            key_copy(j).wait_recv()
            acc = dv_acc[1] if j else dk_acc[1] * score_scale
            kt[j] = (acc + kin[j].astype(F32)).astype(BF16)
            for half in range(2):
                total_copy(j, half).start()

        key_total(0)
        share_send(1)
        total(high)
        share_hand(1)
        total(top)
        key_total(1)
        lat_share(5)

    @pl.when(z == high)
    def _():
        visit(top, high, 0, False)
        for c in range(2):
            top_copy(c).wait_recv()
            out_b[1, rows_of(c)] = (dq_value(top, c) + in_a[rows_of(c)].astype(F32)).astype(BF16)
            part_copy(1, c).start()
        return_keys()
        share_send(0)
        hand_on(low)
        share_hand(0)
        total(high)
        lat_send(4)
        share_send(2)
        share_send(1)
        key_results()
        share_hand(2)
        share_hand(1)
        total(top)
        hand_on(0)
        lat_share(5)

    @pl.when(z < low)
    def _():
        share_send(0)
        hand_on(low)
        share_hand(0)
        share_send(1)
        share_send(5)
        share_hand(1)
        share_hand(5)
        share_send(3)
        share_hand(3)

    @pl.when(z > high)
    def _():
        return_keys()
        share_send(0)
        hand_on(low)
        share_hand(0)
        key_results()
        share_send(1)
        hand_on(high)
        lat_send(4)
        share_hand(1)
        hand_on(top)
        share_send(5)
        hand_on(0)
        share_hand(5)

    def sent(c):
        c.wait_send()


    for a in range(5):
        sent(swap(a))
    for own in (True, False):
        passes(sent, (Q, K, V, ST, G), own)
    for a in (Q, ST, G):
        @pl.when(z == high)
        def _():
            for half in range(2):
                sent(relay(a, half))
    for i in range(2):
        @pl.when(z >= low)
        def _():
            sent(return_copy(i))

        @pl.when((z == low) | (z == high))
        def _():
            for c in range(2):
                sent(part_copy(i, c))

        @pl.when(z < low)
        def _():
            sent(key_copy(i))

    @pl.when(z > high)
    def _():
        for c in range(2):
            sent(top_copy(c))
    for d in range(1, nsp):
        sent(lat_copy(d))

    own_lat().wait()

    @pl.when(z > high)
    def _():
        query_results(True)

    for level in range(high):
        weights(level)

        @pl.when(z < low)
        def _():
            hand_on(high + level)

    @pl.when(z < high)
    def _():
        query_results(True)
        query_results(False)
        share_send(4)

        @pl.when(z == low)
        def _():
            key_results()

        @pl.when(z < low)
        def _():
            key_results((0,))
        share_hand(4)

    for level in range(high, nz):
        weights(level)

        @pl.when(z == level)
        def _():
            if level < top:
                query_results(True)
            query_results(False)

        if level == high:
            @pl.when(z < low)
            def _():
                key_results((1,))

    for level in range(nz):
        grad_each(level, sent)

    @pl.when(z == low)
    def _():
        for i in range(2):
            for half in range(2):
                sent(total_copy(i, half))

    def drain(d, carry):
        for k in range(2 * sides):
            if k != sides:
                sent(share_copy(lax.rem(s + d, nsp), k))
        return carry
    lax.fori_loop(1, nsp, drain, 0)


def finish_kernel(a, b, c, d, a_out, b_out, c_out, d_out, sems):
    stores = [
        pltpu.make_async_copy(src, dst, sems.at[i])
        for i, (src, dst) in enumerate(((a, a_out), (b, b_out), (c, c_out), (d, d_out)))
    ]
    for store in stores:
        store.start()
    for store in stores:
        store.wait()


def far():
    return pl.BlockSpec(memory_space=pltpu.HBM)


def hub_body(nsp, ntp, latents, query_heads, key_heads, value_heads, map_outputs, log_sums, out_grad,
             mix_lambda, norm_gain):
    rows, heads, width = query_heads.shape
    flat = (rows, heads * width)
    slab = latents.shape[1] // nsp
    nz = nsp // 2
    pair = heads // 2
    block = (2 * rows, pair * width)
    half = (rows, pair * width)
    dma = pltpu.SemaphoreType.DMA
    room = max(rows, width, heads)

    sums = jnp.transpose(log_sums, (1, 2, 0))
    small = (
        jnp.pad(sums, ((0, 1), (0, 0), (0, room - rows)))
        + jnp.pad(norm_gain[None, None, :], ((heads, 0), (0, 1), (0, room - width)))
        + jnp.pad(mix_lambda[None, None, :], ((heads, 0), (1, 0), (0, room - heads)))
    )
    results = pl.pallas_call(
        functools.partial(hub_kernel, nsp, ntp, heads, width),
        out_shape=(
            jax.ShapeDtypeStruct(query_heads.shape, BF16),
            jax.ShapeDtypeStruct(query_heads.shape, BF16),
            jax.ShapeDtypeStruct(query_heads.shape, BF16),
            jax.ShapeDtypeStruct((slab, heads * width), F32),
        ),
        in_specs=[vmem(), far()] + [vmem()] * 4,
        out_specs=(vmem(),) * 4,
        scratch_shapes=[
            pltpu.VMEM(flat, BF16),
            pltpu.VMEM((heads, 4, rows), F32),
            pltpu.VMEM((4, nz) + block, BF16),
            pltpu.VMEM((nz, 2, pair, 4, rows), F32),
            pltpu.VMEM((nz, pair, width, 2 * rows), F32),
            pltpu.VMEM((2,) + block, F32),
            pltpu.VMEM((2,) + block, F32),
            pltpu.VMEM((nz, 2) + block, BF16),
            pltpu.VMEM((2,) + block, BF16),
            pltpu.VMEM((2,) + block, BF16),
            pltpu.VMEM(block, BF16),
            pltpu.VMEM((2,) + block, BF16),
            pltpu.VMEM((2,) + block, BF16),
            pltpu.VMEM((2,) + half, BF16),
            pltpu.VMEM((2, 2) + half, BF16),
            pltpu.VMEM((nsp, rows, slab), BF16),
            dma((5,)), dma((5, 2)), dma((5, 2)), dma((4, nz, 2)), dma((nz, 2)), dma((nz, 3, 2)), dma((nz, 2, 2)),
            dma((2, 2)), dma((2, 2)), dma((2,)), dma((2,)), dma((2,)), dma((2, 2)), dma((2,)), dma((2, 2)),
            dma((nsp,)), dma((nsp,)), dma((nsp, ntp)), dma((nsp, ntp)),
            dma,
        ],
        compiler_params=pltpu.CompilerParams(
            collective_id=0, has_side_effects=True, vmem_limit_bytes=52500000),
        name="hub",
    )(
        small,
        latents,
        key_heads.reshape(flat),
        value_heads.reshape(flat),
        query_heads.reshape(flat),
        jnp.concatenate([map_outputs, out_grad[:, None]], axis=1),
    )
    return pl.pallas_call(
        finish_kernel,
        out_shape=tuple(jax.ShapeDtypeStruct(a.shape, a.dtype) for a in results),
        in_specs=[vmem()] * 4,
        out_specs=(far(),) * 4,
        scratch_shapes=[pltpu.SemaphoreType.DMA((4,))],
        compiler_params=pltpu.CompilerParams(vmem_limit_bytes=52500000),
        name="finish",
    )(*results)


def solution(mesh):
    placed = (
        P("sp", None),
        P("sp", "tp", None),
        P("sp", "tp", None),
        P("sp", "tp", None),
        P("sp", None, "tp", None),
        P("sp", "tp", None),
        P("sp", "tp", None),
        P("tp"),
        P(),
    )
    nsp, ntp = mesh.shape["sp"], mesh.shape["tp"]

    def chosen(*args):
        heads = args[1].shape[1]
        return (hub_body if nsp == 8 and heads % 2 == 0 else body)(nsp, ntp, *args)

    return jax.shard_map(
        chosen,
        mesh=mesh,
        in_specs=placed,
        out_specs=(P("sp", "tp", None), P("sp", "tp", None), P("sp", "tp", None), P("sp", "tp")),
        check_vma=False,
    )
```

```python
import functools
import math

import jax
import jax.numpy as jnp
from jax import lax
from jax.experimental import pallas as pl
from jax.experimental.pallas import tpu as pltpu
from jax.sharding import PartitionSpec as P

EPSILON = 1e-05
LOG2E = math.log2(math.e)
F32 = jnp.float32
BF16 = jnp.bfloat16
MESH = pl.DeviceIdType.MESH


def dot_nn(a, b):
    return lax.dot_general(a, b, (((1,), (0,)), ((), ())), preferred_element_type=F32)


def dot_nt(a, b):
    return lax.dot_general(a, b, (((1,), (1,)), ((), ())), preferred_element_type=F32)


def dot_tn(a, b):
    return lax.dot_general(a, b, (((0,), (0,)), ((), ())), preferred_element_type=F32)


def norm_backward(heads, width, lam_ref, gain_ref, mo_ref, og_ref, lse_ref, grad_ref, col_ref, row_ref):
    for h in range(heads):
        first = mo_ref[:, 0, h, :].astype(F32)
        second = mo_ref[:, 1, h, :].astype(F32)
        lam = lam_ref[h]
        combined = first - lam * second
        inverse = lax.rsqrt(jnp.mean(combined * combined, axis=-1, keepdims=True) + EPSILON)
        weighted = gain_ref[...] * og_ref[:, h, :].astype(F32)
        grad = (
            inverse * weighted
            - inverse**3 * combined * jnp.mean(combined * weighted, axis=-1, keepdims=True)
        ).astype(BF16)
        grad_ref[:, h * width : (h + 1) * width] = grad
        wide = grad.astype(F32)
        lse = lse_ref[h] * LOG2E
        log_lam = jnp.log(jnp.full((1, 1), lam, F32)) * LOG2E
        lane = lax.broadcasted_iota(jnp.int32, wide.shape, 1)
        stats = jnp.where(lane == 0, lse[:, 0:1], lse[:, 1:2] - log_lam)
        stats = jnp.where(lane == 2, jnp.sum(wide * first, axis=-1, keepdims=True), stats)
        stats = jnp.where(lane == 3, jnp.sum(wide * second, axis=-1, keepdims=True), stats)
        col_ref[h] = stats
        row_ref[h] = jnp.transpose(stats)[0:4]


def main_kernel(nsp, ntp, heads, width, lam, gain, lat, own_k, own_v, own_q, mo, og, lse,
                dq_out, dk_out, dv_out, wg_out,
                own_g, col, row, own_dq, kvb, qgb, stb, dqb, latb, dq_acc, dk_acc, dv_acc,
                kv_s, qg_s, st_s, dq_s, kv_r, qg_r, st_r, dq_r,
                la_s, la_r, lb_s, lb_r, own_sem):
    nz = nsp // 2
    s = lax.axis_index("sp")
    t = lax.axis_index("tp")
    z, y = s // 2, lax.rem(s, 2)
    rows = own_k.shape[0]
    part = rows // ntp
    slab = lat.shape[1] // nsp
    score_scale = (width // 2) ** (-0.5)
    exp_scale = score_scale * LOG2E

    barrier = pltpu.get_barrier_semaphore()
    for d in range(1, nsp):
        pl.semaphore_signal(barrier, inc=1, device_id={"sp": lax.rem(s + d, nsp)}, device_id_type=MESH)
    for d in range(1, ntp):
        pl.semaphore_signal(barrier, inc=1, device_id={"tp": lax.rem(t + d, ntp)}, device_id_type=MESH)
    pl.semaphore_wait(barrier, nsp - 1 + ntp - 1)

    def copy(src, dst, send, recv, to):
        return pltpu.make_async_remote_copy(
            src_ref=src, dst_ref=dst, send_sem=send, recv_sem=recv,
            device_id={"sp": to}, device_id_type=MESH)

    side = 2 * z + (1 - y)

    def kv_copy(block, lane, k, p, src=None):
        to = jnp.minimum(s + 2, nsp - 1) if lane == 0 else side
        return copy(kvb.at[block, p] if src is None else src, kvb.at[block, p],
                    kv_s.at[lane, p, k], kv_r.at[p, block], to)

    def qg_copy(block, lane, k, p, src=None):
        to = jnp.maximum(s - 2, 0) if lane == 0 else side
        return copy(qgb.at[block, p] if src is None else src, qgb.at[block, p],
                    qg_s.at[lane, p, k], qg_r.at[p, block], to)

    def st_copy(block, lane, k, src=None):
        to = jnp.maximum(s - 2, 0) if lane == 0 else side
        return copy(stb.at[block] if src is None else src, stb.at[block],
                    st_s.at[lane, k], st_r.at[block], to)

    for p, src in ((0, own_k), (1, own_v)):
        @pl.when(z < nz - 1)
        def _():
            kv_copy(s, 0, 0, p, src).start()

        @pl.when(y == 0)
        def _():
            kv_copy(s, 1, 0, p, src).start()

    @pl.when(z > 0)
    def _():
        qg_copy(s, 0, 0, 0, own_q).start()

    @pl.when(y == 1)
    def _():
        qg_copy(s, 1, 0, 0, own_q).start()

    norm_backward(heads, width, lam, gain, mo, og, lse, own_g, col, row)

    @pl.when(z > 0)
    def _():
        st_copy(s, 0, 0, row).start()
        qg_copy(s, 0, 0, 1, own_g).start()

    @pl.when(y == 1)
    def _():
        st_copy(s, 1, 0, row).start()
        qg_copy(s, 1, 0, 1, own_g).start()

    lane_id = lax.broadcasted_iota(jnp.int32, (1, width), 1)
    low = jnp.where(lane_id < width // 2, 1.0, 0.0).astype(BF16)
    high = jnp.where(lane_id < width // 2, 0.0, 1.0).astype(BF16)

    def split(x):
        return jnp.concatenate([x * low, x * high], axis=0)

    def query_side(k_at, v_at, diagonal):
        def one(h, carry):
            at = pl.ds(pl.multiple_of(h * width, width), width)
            keys = split(k_at[:, at])
            scores = dot_nt(own_q[:, at], keys)
            mixed = dot_nt(own_g[:, at], v_at[:, at])
            stats = col[h]
            x1 = scores[:, :rows] * exp_scale - stats[:, 0:1]
            x2 = scores[:, rows:] * exp_scale - stats[:, 1:2]
            if diagonal:
                seen = (lax.broadcasted_iota(jnp.int32, (rows, rows), 1)
                        <= lax.broadcasted_iota(jnp.int32, (rows, rows), 0))
                x1 = jnp.where(seen, x1, -jnp.inf)
                x2 = jnp.where(seen, x2, -jnp.inf)
            g1 = (jnp.exp2(x1) * (mixed - stats[:, 2:3])).astype(BF16)
            g2 = (jnp.exp2(x2) * (stats[:, 3:4] - mixed)).astype(BF16)
            part_dq = dot_nn(jnp.concatenate([g1, g2], axis=1), keys)
            if diagonal:
                dq_acc[:, at] = part_dq
            else:
                dq_acc[:, at] += part_dq
            return carry
        lax.fori_loop(0, heads, one, 0)

    def key_side(q_at, g_at, row_at, diagonal):
        def one(h, carry):
            at = pl.ds(pl.multiple_of(h * width, width), width)
            queries = split(q_at[:, at])
            grads = g_at[:, at]
            scores = dot_nt(own_k[:, at], queries)
            mixed = dot_nt(own_v[:, at], grads)
            stats = row_at[h]
            x1 = scores[:, :rows] * exp_scale - stats[0:1]
            x2 = scores[:, rows:] * exp_scale - stats[1:2]
            if diagonal:
                seen = (lax.broadcasted_iota(jnp.int32, (rows, rows), 0)
                        <= lax.broadcasted_iota(jnp.int32, (rows, rows), 1))
                x1 = jnp.where(seen, x1, -jnp.inf)
                x2 = jnp.where(seen, x2, -jnp.inf)
            p1 = jnp.exp2(x1)
            p2 = jnp.exp2(x2)
            g1 = (p1 * (mixed - stats[2:3])).astype(BF16)
            g2 = (p2 * (stats[3:4] - mixed)).astype(BF16)
            part_dv = dot_nn((p1 - p2).astype(BF16), grads)
            part_dk = dot_nn(jnp.concatenate([g1, g2], axis=1), queries)
            if diagonal:
                dv_acc[:, at] = part_dv
                dk_acc[:, at] = part_dk
            else:
                dv_acc[:, at] += part_dv
                dk_acc[:, at] += part_dk
            return carry
        lax.fori_loop(0, heads, one, 0)

    def lat_copy(d):
        to = lax.rem(s + d, nsp)
        mine = pl.ds(pl.multiple_of(t * part, part), part)
        return copy(lat.at[mine, pl.ds(pl.multiple_of(to * slab, slab), slab)],
                    latb.at[s, mine, :], la_s.at[d], la_r.at[d], to)

    def own_lat():
        return pltpu.make_async_copy(
            lat.at[pl.ds(pl.multiple_of(t * part, part), part), pl.ds(pl.multiple_of(s * slab, slab), slab)],
            latb.at[s, pl.ds(pl.multiple_of(t * part, part), part), :], own_sem)

    def share_copy(d):
        mine = pl.ds(pl.multiple_of(t * part, part), part)
        return pltpu.make_async_remote_copy(
            src_ref=latb.at[:, mine, :], dst_ref=latb.at[:, mine, :],
            send_sem=lb_s.at[d], recv_sem=lb_r.at[d],
            device_id={"tp": lax.rem(t + d, ntp)}, device_id_type=MESH)

    own_lat().start()
    query_side(own_k, own_v, True)
    key_side(own_q, own_g, row, True)
    for d in range(1, nsp):
        lat_copy(d).start()

    def step(k, carry):
        below, above = z - k, z + k
        has_below, has_above = below >= 0, above < nz
        kb = jnp.maximum(below, 0) * 2 + y
        qb = jnp.minimum(above, nz - 1) * 2 + y

        for p in range(2):
            @pl.when(has_below)
            def _():
                kv_copy(kb, 0, 0, p).wait_recv()
                kv_copy(kb, 1, k, p).start()

            @pl.when(has_below & (z < nz - 1))
            def _():
                kv_copy(kb, 0, k, p).start()

            @pl.when(has_above)
            def _():
                qg_copy(qb, 0, 0, p).wait_recv()
                qg_copy(qb, 1, k, p).start()
                if p == 0:
                    st_copy(qb, 0, 0).wait_recv()
                    st_copy(qb, 1, k).start()

            @pl.when(has_above & (z > 0))
            def _():
                qg_copy(qb, 0, k, p).start()
                if p == 0:
                    st_copy(qb, 0, k).start()

        def turn(c, carry):
            dist = k - c
            other = jnp.where(c == 0, y, 1 - y)
            bz, qz = z - dist, z + dist
            use_kv = (bz >= 0) & (dist < nz) & ((dist > 0) | (y == 1))
            use_qg = (qz < nz) & (dist < nz) & ((dist > 0) | (y == 0))
            kblk = jnp.maximum(bz, 0) * 2 + other
            qblk = jnp.minimum(qz, nz - 1) * 2 + other

            @pl.when(use_kv)
            def _():
                @pl.when(c == 1)
                def _():
                    for p in range(2):
                        kv_copy(kblk, 1, 0, p).wait_recv()
                query_side(kvb.at[kblk, 0], kvb.at[kblk, 1], False)

            @pl.when(use_qg)
            def _():
                @pl.when(c == 1)
                def _():
                    for p in range(2):
                        qg_copy(qblk, 1, 0, p).wait_recv()
                    st_copy(qblk, 1, 0).wait_recv()
                key_side(qgb.at[qblk, 0], qgb.at[qblk, 1], stb.at[qblk], False)
            return carry
        lax.fori_loop(0, 2, turn, 0)
        return carry

    lax.fori_loop(1, nz + 1, step, 0)

    own_dq[...] = (dq_acc[...] * score_scale).astype(BF16)
    half = rows // 2

    def dq_copy(block, lane, idx, p, own=False):
        to = (jnp.minimum(s + 2, nsp - 2 + y), jnp.maximum(s - 2, y), side)[lane]
        at = pl.ds(p * half, half)
        return copy(own_dq.at[at] if own else dqb.at[block, at], dqb.at[block, at],
                    dq_s.at[lane, p, idx], dq_r.at[p, block], to)

    for p in range(2):
        @pl.when(z < nz - 1)
        def _():
            dq_copy(s, 0, z, p, True).start()

        @pl.when(z > 0)
        def _():
            dq_copy(s, 1, z, p, True).start()

        dq_copy(s, 2, z, p, True).start()

    for h in range(heads):
        at = slice(h * width, (h + 1) * width)
        dq_out[:, h, :] = own_dq[:, at]
        dk_out[:, h, :] = (dk_acc[:, at] * score_scale).astype(BF16)
        dv_out[:, h, :] = dv_acc[:, at].astype(BF16)

    own_lat().wait()
    for d in range(1, nsp):
        lat_copy(d).wait_recv()
    for d in range(1, ntp):
        share_copy(d).start()
    for d in range(1, ntp):
        share_copy(d).wait_recv()

    wg_out[...] = dot_tn(latb[s], own_dq[...])

    def add_block(block):
        wg_out[...] += dot_tn(latb[block], dqb[block])

    def gather(k, carry):
        for p in range(2):
            for lane, there, ok, more in (
                (0, z - k, z - k >= 0, z < nz - 1),
                (1, z + k, z + k < nz, z > 0),
            ):
                bz = jnp.clip(there, 0, nz - 1)
                block = bz * 2 + y

                @pl.when(ok)
                def _():
                    dq_copy(block, lane, bz, p).wait_recv()
                    dq_copy(block, 2, bz, p).start()

                @pl.when(ok & more)
                def _():
                    dq_copy(block, lane, bz, p).start()

        def turn(c, carry):
            dist = jnp.where(c < 2, k, k - 1)
            up = lax.rem(c, 2)
            bz = jnp.where(up == 0, z - dist, z + dist)
            ok = (bz >= 0) & (bz < nz) & (dist < nz) & ((dist > 0) | (up == 0))
            other = jnp.where(c < 2, y, 1 - y)
            block = jnp.clip(bz, 0, nz - 1) * 2 + other

            @pl.when(ok)
            def _():
                @pl.when(c >= 2)
                def _():
                    for p in range(2):
                        dq_copy(block, 2, 0, p).wait_recv()
                add_block(block)
            return carry
        lax.fori_loop(0, 4, turn, 0)
        return carry

    lax.fori_loop(1, nz + 1, gather, 0)

    def drain(k, carry):
        below, above = z - k, z + k
        has_below, has_above = below >= 0, above < nz

        for p in range(2):
            @pl.when(has_below & (z < nz - 1))
            def _():
                kv_copy(s, 0, k, p).wait_send()

            @pl.when(has_below & ((k > 0) | (y == 0)))
            def _():
                kv_copy(s, 1, k, p).wait_send()

            @pl.when(has_above & (z > 0))
            def _():
                qg_copy(s, 0, k, p).wait_send()
                if p == 0:
                    st_copy(s, 0, k).wait_send()

            @pl.when(has_above & ((k > 0) | (y == 1)))
            def _():
                qg_copy(s, 1, k, p).wait_send()
                if p == 0:
                    st_copy(s, 1, k).wait_send()

            @pl.when((k <= z) & (z < nz - 1))
            def _():
                dq_copy(s, 0, k, p).wait_send()

            @pl.when((k >= z) & (z > 0))
            def _():
                dq_copy(s, 1, k, p).wait_send()

            dq_copy(s, 2, k, p).wait_send()
        return carry

    lax.fori_loop(0, nz, drain, 0)
    for d in range(1, nsp):
        lat_copy(d).wait_send()
    for d in range(1, ntp):
        share_copy(d).wait_send()


def vmem():
    return pl.BlockSpec(memory_space=pltpu.VMEM)


def body(nsp, ntp, latents, query_heads, key_heads, value_heads, map_outputs, log_sums, out_grad,
         mix_lambda, norm_gain):
    rows, heads, width = query_heads.shape
    flat = (rows, heads * width)
    slab = latents.shape[1] // nsp
    nz = nsp // 2
    dma = pltpu.SemaphoreType.DMA
    dq, dk, dv, wg = pl.pallas_call(
        functools.partial(main_kernel, nsp, ntp, heads, width),
        out_shape=(
            jax.ShapeDtypeStruct(query_heads.shape, BF16),
            jax.ShapeDtypeStruct(query_heads.shape, BF16),
            jax.ShapeDtypeStruct(query_heads.shape, BF16),
            jax.ShapeDtypeStruct((slab, heads * width), F32),
        ),
        in_specs=[pl.BlockSpec(memory_space=pltpu.SMEM)] + [vmem()] * 8,
        out_specs=(vmem(),) * 4,
        scratch_shapes=[
            pltpu.VMEM(flat, BF16),
            pltpu.VMEM((heads, rows, width), F32),
            pltpu.VMEM((heads, 4, rows), F32),
            pltpu.VMEM(flat, BF16),
            pltpu.VMEM((nsp, 2) + flat, BF16),
            pltpu.VMEM((nsp, 2) + flat, BF16),
            pltpu.VMEM((nsp, heads, 4, rows), F32),
            pltpu.VMEM((nsp,) + flat, BF16),
            pltpu.VMEM((nsp, rows, slab), BF16),
            pltpu.VMEM(flat, F32),
            pltpu.VMEM(flat, F32),
            pltpu.VMEM(flat, F32),
            dma((2, 2, nz)), dma((2, 2, nz)), dma((2, nz)), dma((3, 2, nz)),
            dma((2, nsp)), dma((2, nsp)), dma((nsp,)), dma((2, nsp)),
            dma((nsp,)), dma((nsp,)), dma((ntp,)), dma((ntp,)),
            dma,
        ],
        compiler_params=pltpu.CompilerParams(collective_id=0, has_side_effects=True),
        name="main",
    )(
        mix_lambda,
        norm_gain[None, :],
        latents,
        key_heads.reshape(flat),
        value_heads.reshape(flat),
        query_heads.reshape(flat),
        map_outputs,
        out_grad,
        jnp.transpose(log_sums, (1, 0, 2)),
    )
    return dq, dk, dv, wg


def row_norm_backward(heads, width, small, maps, grad_ref, row_ref):
    count = maps.shape[0]
    for h in range(heads):
        first = maps[:, 0, h, :].astype(F32)
        second = maps[:, 1, h, :].astype(F32)
        lam = small[heads, 1:2, h : h + 1]
        combined = first - lam * second
        inverse = lax.rsqrt(jnp.mean(combined * combined, axis=-1, keepdims=True) + EPSILON)
        weighted = small[heads, 0:1, :width] * maps[:, 2, h, :].astype(F32)
        grad = (
            inverse * weighted
            - inverse**3 * combined * jnp.mean(combined * weighted, axis=-1, keepdims=True)
        ).astype(BF16)
        grad_ref[:, h * width : (h + 1) * width] = grad
        wide = grad.astype(F32)
        row_ref[h, 0:1] = small[h, 0:1, :count] * LOG2E
        row_ref[h, 1:2] = small[h, 1:2, :count] * LOG2E - jnp.log(lam) * LOG2E
        lane = lax.broadcasted_iota(jnp.int32, wide.shape, 1)
        terms = jnp.where(lane == 0, jnp.sum(wide * first, axis=-1, keepdims=True),
                          jnp.sum(wide * second, axis=-1, keepdims=True))
        row_ref[h, 2:4] = jnp.transpose(terms)[0:2]


def hub_kernel(nsp, ntp, heads, width, small, lat, own_k, own_v, own_q, maps,
               dq_out, dk_out, dv_out, wg_out,
               own_g, row, blk, stb, dq_acc, dk_acc, dv_acc, db, out_b, in_b, in_a, kt, kin, kst, kret, latb,
               f_s, z_s, r_s, b_r, st_r, d_s, d_r, ob_s, ib_r, ia_r, kt_s, kin_r, tot_s, kst_s, kret_r,
               la_s, la_r, lb_s, lb_r, own_sem):
    nz = nsp // 2
    low, high, top = nz // 2 - 1, nz // 2, nz - 1
    s = lax.axis_index("sp")
    t = lax.axis_index("tp")
    z, y = s // 2, lax.rem(s, 2)
    rows = own_k.shape[0]
    span = 2 * rows
    pair = heads // 2
    lanes = pair * width
    part = rows // ntp
    slab = lat.shape[1] // nsp
    score_scale = (width // 2) ** (-0.5)
    exp_scale = score_scale * LOG2E
    partner = 2 * z + 1 - y
    Q, K, V, G, ST = range(5)

    barrier = pltpu.get_barrier_semaphore()
    for d in range(1, nsp):
        pl.semaphore_signal(barrier, inc=1, device_id={"sp": lax.rem(s + d, nsp)}, device_id_type=MESH)
    for d in range(1, ntp):
        pl.semaphore_signal(barrier, inc=1, device_id={"tp": lax.rem(t + d, ntp)}, device_id_type=MESH)
    pl.semaphore_wait(barrier, nsp - 1 + ntp - 1)

    def copy(src, dst, send, recv, to):
        return pltpu.make_async_remote_copy(
            src_ref=src, dst_ref=dst, send_sem=send, recv_sem=recv,
            device_id={"sp": to}, device_id_type=MESH)

    def at_level(level):
        return 2 * level + y

    def lane_of(p):
        return pl.ds(pl.multiple_of(p * lanes, lanes), lanes)

    def half_of(p):
        return pl.ds(pl.multiple_of(p * rows, rows), rows)

    owned = (own_q, own_k, own_v, own_g)

    def source(a, p):
        if a == ST:
            return row.at[pl.ds(p * pair, pair)]
        return owned[a].at[:, lane_of(p)]

    def landing(a, level, half):
        return stb.at[level, half] if a == ST else blk.at[a, level, half_of(half), :]

    def landed(a, level, half):
        return st_r.at[level, half] if a == ST else b_r.at[a, level, half]

    def swap(a):
        return copy(source(a, 1 - y), landing(a, z, y), f_s.at[a], landed(a, z, y), partner)

    def arrive(a, level, half):
        copy(landing(a, level, half), landing(a, level, half), f_s.at[a], landed(a, level, half), partner).wait_recv()

    def pass_on(a, own):
        half = y if own else 1 - y
        return copy(source(a, y) if own else landing(a, z, half), landing(a, z, half),
                    z_s.at[a, 0 if own else 1], landed(a, z, half), at_level(jnp.where(z > high, high, low)))

    def passes(action, arrays, own):
        for a in arrays:
            if a in (K, V):
                @pl.when(z < low)
                def _():
                    action(pass_on(a, own))
            else:
                @pl.when(z >= high)
                def _():
                    action(pass_on(a, own))

    def relay(a, half):
        return copy(landing(a, top, half), landing(a, top, half), r_s.at[a, half], landed(a, top, half), at_level(low))

    def relays(arrays, half):
        @pl.when(z == high)
        def _():
            for a in arrays:
                arrive(a, top, half)
                relay(a, half).start()

    def start(c):
        c.start()

    def lat_copy(d):
        to = lax.rem(s + d, nsp)
        mine = pl.ds(pl.multiple_of(t * part, part), part)
        return copy(lat.at[mine, pl.ds(pl.multiple_of(to * slab, slab), slab)],
                    latb.at[s, mine, :], la_s.at[d], la_r.at[s], to)

    def own_lat():
        return pltpu.make_async_copy(
            lat.at[:, pl.ds(pl.multiple_of(s * slab, slab), slab)], latb.at[s], own_sem)

    sides = ntp // 2
    side, core = t // 2, lax.rem(t, 2)

    def share_copy(b, k):
        away = lax.rem(side + (k if k < sides else k - sides), sides)
        quarter = t if k < sides else 2 * away + core
        to = 2 * away + core if 0 < k < sides else 2 * side + 1 - core
        at = pl.ds(pl.multiple_of(quarter * part, part), part)
        return pltpu.make_async_remote_copy(
            src_ref=latb.at[b, at, :], dst_ref=latb.at[b, at, :],
            send_sem=lb_s.at[b, k], recv_sem=lb_r.at[b, quarter],
            device_id={"tp": to}, device_id_type=MESH)

    def share_arrive(b, quarter):
        at = pl.ds(pl.multiple_of(quarter * part, part), part)
        pltpu.make_async_remote_copy(
            src_ref=latb.at[b, at, :], dst_ref=latb.at[b, at, :],
            send_sem=lb_s.at[b, 0], recv_sem=lb_r.at[b, quarter],
            device_id={"tp": 2 * side + 1 - core}, device_id_type=MESH).wait_recv()

    def group_of(src, dst, group):
        sz, dz = src // 2, dst // 2
        late = (sz >= high) & (dz < high)
        upper = (sz >= high) & (dz >= high) & (dz < sz)
        first = (lax.rem(src, 2) == lax.rem(dst, 2)) & ((dz > sz) | (sz < high))
        if group in (3, 4):
            return late & ((dz < low) if group == 3 else (dz >= low))
        if group == 2:
            return upper
        rest = jnp.logical_not(late | upper)
        if group == 0:
            return rest & first
        return rest & jnp.logical_not(first) & ((sz >= low) if group == 1 else (sz < low))

    def lat_send(group):
        for d in range(1, nsp):
            @pl.when(group_of(s, lax.rem(s + d, nsp), group))
            def _():
                lat_copy(d).start()

    def share_send(group):
        def step(d, carry):
            b = lax.rem(s + d, nsp)

            @pl.when(group_of(b, s, group))
            def _():
                mine = pl.ds(pl.multiple_of(t * part, part), part)
                copy(latb.at[b, mine, :], latb.at[b, mine, :], la_s.at[1], la_r.at[b], partner).wait_recv()
                for k in reversed(range(sides)):
                    share_copy(b, k).start()
            return carry
        lax.fori_loop(1, nsp, step, 0)

    def share_hand(group):
        def hand(d, carry):
            b = lax.rem(s + d, nsp)

            @pl.when(group_of(b, s, group))
            def _():
                for k in range(sides + 1, 2 * sides):
                    share_arrive(b, 2 * lax.rem(side + k - sides, sides) + core)
                    share_copy(b, k).start()
            return carry
        lax.fori_loop(1, nsp, hand, 0)

    def lat_share(group):
        share_send(group)
        share_hand(group)

    swap(Q).start()
    passes(start, (Q, K, V), True)
    swap(K).start()
    swap(V).start()
    @pl.when(z >= low)
    def _():
        lat_send(0)
    own_lat().start()

    row_norm_backward(heads, width, small, maps, own_g, row)

    swap(G).start()
    swap(ST).start()
    passes(start, (ST, G), True)

    for a in (Q, K, V, G):
        blk[a, z, half_of(y), :] = owned[a][:, lane_of(y)]
    stb[z, y] = row[pl.ds(y * pair, pair)]
    dq_acc[...] = jnp.zeros_like(dq_acc)
    dk_acc[...] = jnp.zeros_like(dk_acc)
    dv_acc[...] = jnp.zeros_like(dv_acc)

    for a in (Q, K, V, ST, G):
        arrive(a, z, 1 - y)
        passes(start, (a,), False)
        if a == Q:
            relays((Q,), y)
        if a == K:
            relays((ST, G), y)
        if a == V:
            relays((Q,), 1 - y)

            @pl.when(z < low)
            def _():
                lat_send(0)


    lane_id = lax.broadcasted_iota(jnp.int32, (1, width), 1)
    first_map = jnp.where(lane_id < width // 2, 1.0, 0.0).astype(BF16)
    second_map = jnp.where(lane_id < width // 2, 0.0, 1.0).astype(BF16)

    def split(x):
        return jnp.concatenate([x * first_map, x * second_map], axis=0)

    def visit(qz, kz, slot, diagonal):
        def one(h, carry):
            at = pl.ds(pl.multiple_of(h * width, width), width)
            for a in range(2):
                start_row = a * rows if diagonal else 0
                kr = pl.ds(a * rows, rows)
                qr = pl.ds(start_row, span - start_row)
                count = span - start_row
                keys = split(blk[K, kz, kr, at])
                queries = split(blk[Q, qz, qr, at])
                grads = blk[G, qz, qr, at]
                scores = dot_nt(blk[K, kz, kr, at], queries)
                mixed = dot_nt(blk[V, kz, kr, at], grads)
                stats = jnp.concatenate([stb[qz, p, h] for p in range(start_row // rows, 2)], axis=1)
                x1 = scores[:, :count] * exp_scale - stats[0:1]
                x2 = scores[:, count:] * exp_scale - stats[1:2]
                if diagonal:
                    seen = (lax.broadcasted_iota(jnp.int32, (rows, count), 0)
                            <= lax.broadcasted_iota(jnp.int32, (rows, count), 1))
                    x1 = jnp.where(seen, x1, -jnp.inf)
                    x2 = jnp.where(seen, x2, -jnp.inf)
                p1 = jnp.exp2(x1)
                p2 = jnp.exp2(x2)
                g1 = (p1 * (mixed - stats[2:3])).astype(BF16)
                g2 = (p2 * (stats[3:4] - mixed)).astype(BF16)
                dv_acc[slot, kr, at] += dot_nn((p1 - p2).astype(BF16), grads)
                dk_acc[slot, kr, at] += dot_nn(jnp.concatenate([g1, g2], axis=1), queries)
                dq_acc[qz, h, :, qr] += dot_tn(keys, jnp.concatenate([g1, g2], axis=0))
            return carry
        lax.fori_loop(0, pair, one, 0)

    def dq_value(level, c):
        at = pl.ds(c * rows, rows)
        return jnp.concatenate([jnp.transpose(dq_acc[level, h, :, at]) for h in range(pair)], axis=1) * score_scale

    def grad_copy(level, lane, c):
        if lane == 0:
            to = partner
        elif lane == 1:
            down = high if level == 0 else 0
            to = at_level(jnp.where(z == low, down, jnp.where(z == high, top, low)))
        else:
            to = at_level(high)
        piece = db.at[level, y, half_of(c), :]
        return copy(piece, piece, d_s.at[level, lane, c], d_r.at[level, y, c], to)

    def grad_lanes(level):
        chained = (z <= high) if level == 0 else (z == high) | (z == low)
        if level != low:
            return ((0, None), (1, chained))
        return ((0, None), (1, chained), (2, z == low))

    def grad_each(level, action, chunks=(0, 1), only=(0, 1, 2)):
        for c in chunks:
            for lane, ok in reversed(grad_lanes(level)):
                if lane not in only:
                    continue
                if ok is None:
                    action(grad_copy(level, lane, c))
                else:
                    @pl.when(ok)
                    def _():
                        action(grad_copy(level, lane, c))

    def grad_arrive(level, p, c):
        piece = db.at[level, p, half_of(c), :]
        copy(piece, piece, d_s.at[level, 0, c], d_r.at[level, p, c], partner).wait_recv()

    def part_copy(i, c):
        return copy(out_b.at[i, half_of(c), :], in_b.at[i, half_of(c), :], ob_s.at[i, c], ib_r.at[i, c],
                    at_level(jnp.where(z == low, high, low)))

    def top_copy(c):
        return copy(out_b.at[0, half_of(c), :], in_a.at[half_of(c), :], ob_s.at[0, c], ia_r.at[c], at_level(high))

    def rows_of(c):
        return slice(c * rows, (c + 1) * rows)

    def key_copy(i):
        return copy(kt.at[i], kin.at[i], kt_s.at[i], kin_r.at[i], at_level(low))

    def total_copy(i, half):
        return copy(kt.at[i, half_of(half), :], kret.at[i, y], tot_s.at[i, half], kret_r.at[i, y], half)

    def return_copy(i):
        return copy(kst.at[i], kret.at[i, y], kst_s.at[i], kret_r.at[i, y], partner)

    @pl.when(z >= low)
    def _():
        lat_send(1)

    visit(z, z, 0, True)
    relays((ST, G), 1 - y)

    @pl.when(z >= high)
    def _():
        for c in range(2):
            out_b[0, rows_of(c)] = dq_value(z, c).astype(BF16)

    @pl.when(z == high)
    def _():
        lat_send(3)
        for c in range(2):
            part_copy(0, c).start()

    @pl.when(z > high)
    def _():
        for c in range(2):
            top_copy(c).start()
        lat_send(3)
        lat_send(2)

    @pl.when(z < low)
    def _():
        for c in range(2):
            db[0, y, rows_of(c)] = dq_value(0, c).astype(BF16)
        grad_each(0, start)
        for i in range(2):
            kt[i] = (dv_acc[0] if i else dk_acc[0] * score_scale).astype(BF16)
            key_copy(i).start()
        lat_send(5)

    def return_keys():
        for i, acc, scale in ((0, dk_acc, score_scale), (1, dv_acc, 1.0)):
            kst[i] = (acc[0, half_of(1 - y), :] * scale).astype(BF16)
            return_copy(i).start()
            kret[i, y] = (acc[0, half_of(y), :] * scale).astype(BF16)

    def hand_on(level):
        for c in range(2):
            grad_arrive(level, y, c)
            grad_each(level, start, (c,))

    def total(level):
        i = level - high
        for c in range(2):
            part_copy(i, c).wait_recv()
            whole = dq_value(level, c) + in_b[i, rows_of(c)].astype(F32)
            if level == top:
                above = in_a[rows_of(c)].astype(F32)
                whole = whole + jnp.where(z == high, above, jnp.zeros_like(above))
            db[level, y, rows_of(c)] = whole.astype(BF16)
            grad_each(level, start, (c,))

    def key_results(which=(0, 1)):
        for i in which:
            copy(kst.at[i], kret.at[i, 1 - y], kst_s.at[i], kret_r.at[i, 1 - y], partner).wait_recv()

            @pl.when(z < low)
            def _():
                copy(kst.at[i], kret.at[i, y], kst_s.at[i], kret_r.at[i, y], partner).wait_recv()
            out = dv_out if i else dk_out
            for p in range(2):
                for h in range(pair):
                    out[:, p * pair + h, :] = kret[i, p, :, h * width : (h + 1) * width]

    def query_results(own):
        for p in range(2):
            @pl.when((y == p) if own else (y != p))
            def _():
                for h in range(pair):
                    dq_out[:, p * pair + h, :] = db[z, p, half_of(y), h * width : (h + 1) * width]

    def weights(level):
        for c in range(2):
            grad_arrive(level, 1 - y, c)
        for half in range(2):
            b = 2 * level + half

            @pl.when(s != b)
            def _():
                for k in range(sides):
                    share_arrive(b, 2 * lax.rem(side + k, sides) + 1 - core)
        feed = latb[2 * level : 2 * level + 2].reshape(span, slab)
        for p in range(2):
            at = slice(p * lanes, (p + 1) * lanes)
            term = dot_tn(feed, db[level, p])
            if level == 0:
                wg_out[:, at] = term
            else:
                wg_out[:, at] += term

    @pl.when(z == low)
    def _():
        def step(i, carry):
            qz = jnp.where(i == 0, low, high + (i - 1) // 2)
            kz = jnp.where(i == 0, 0, lax.rem(i - 1, 2))

            @pl.when(i == 0)
            def _():
                for half in range(2):
                    arrive(K, 0, half)
                    arrive(V, 0, half)

            @pl.when((i > 0) & (kz == 0))
            def _():
                for a in (Q, ST, G):
                    for half in range(2):
                        arrive(a, qz, half)

            visit(qz, kz, 1 - kz, False)

            @pl.when(i == 0)
            def _():
                for c in range(2):
                    db[low, y, rows_of(c)] = dq_value(low, c).astype(BF16)
                grad_each(low, start)
                share_send(0)

            @pl.when((i > 0) & (kz == 1))
            def _():
                for c in range(2):
                    out_b[qz - high, rows_of(c)] = dq_value(qz, c).astype(BF16)
                    part_copy(qz - high, c).start()

            @pl.when((qz == high) & (kz == 1))
            def _():
                share_hand(0)

            @pl.when((qz == top) & (kz == 0))
            def _():
                for c in range(2):
                    grad_arrive(0, y, c)
                grad_each(0, start, only=(0,))
            return carry
        lax.fori_loop(0, 5, step, 0)
        grad_each(0, start, only=(1,))
        return_keys()

        def key_total(j):
            key_copy(j).wait_recv()
            acc = dv_acc[1] if j else dk_acc[1] * score_scale
            kt[j] = (acc + kin[j].astype(F32)).astype(BF16)
            for half in range(2):
                total_copy(j, half).start()

        key_total(0)
        share_send(1)
        total(high)
        share_hand(1)
        total(top)
        key_total(1)
        share_send(5)
        share_send(4)
        share_hand(5)

    @pl.when(z == high)
    def _():
        visit(top, high, 0, False)
        for c in range(2):
            top_copy(c).wait_recv()
            out_b[1, rows_of(c)] = (dq_value(top, c) + in_a[rows_of(c)].astype(F32)).astype(BF16)
            part_copy(1, c).start()
        return_keys()
        share_send(0)
        hand_on(low)
        share_hand(0)
        total(high)
        lat_send(4)
        share_send(2)
        share_send(1)
        key_results()
        share_hand(2)
        share_hand(1)
        total(top)
        hand_on(0)
        lat_share(5)

    @pl.when(z < low)
    def _():
        share_send(0)
        hand_on(low)
        share_hand(0)
        share_send(1)
        share_send(5)
        share_hand(1)
        share_hand(5)
        share_send(3)
        share_hand(3)

    @pl.when(z > high)
    def _():
        return_keys()
        share_send(0)
        hand_on(low)
        share_hand(0)
        key_results()
        share_send(1)
        hand_on(high)
        lat_send(4)
        share_hand(1)
        hand_on(top)
        share_send(5)
        hand_on(0)
        share_hand(5)

    def sent(c):
        c.wait_send()


    for a in range(5):
        sent(swap(a))
    for own in (True, False):
        passes(sent, (Q, K, V, ST, G), own)
    for a in (Q, ST, G):
        @pl.when(z == high)
        def _():
            for half in range(2):
                sent(relay(a, half))
    for i in range(2):
        @pl.when(z >= low)
        def _():
            sent(return_copy(i))

        @pl.when((z == low) | (z == high))
        def _():
            for c in range(2):
                sent(part_copy(i, c))

        @pl.when(z < low)
        def _():
            sent(key_copy(i))

    @pl.when(z > high)
    def _():
        for c in range(2):
            sent(top_copy(c))
    for d in range(1, nsp):
        sent(lat_copy(d))

    own_lat().wait()

    @pl.when(z > high)
    def _():
        query_results(True)

    for level in range(high):
        weights(level)

        @pl.when(z < low)
        def _():
            hand_on(high + level)

    @pl.when(z < high)
    def _():
        query_results(True)
        query_results(False)

        @pl.when(z < low)
        def _():
            share_send(4)

        @pl.when(z == low)
        def _():
            key_results()

        @pl.when(z < low)
        def _():
            key_results((0,))
        share_hand(4)

    for level in range(high, nz):
        weights(level)

        @pl.when(z == level)
        def _():
            if level < top:
                query_results(True)
            query_results(False)

        if level == high:
            @pl.when(z < low)
            def _():
                key_results((1,))

    for level in range(nz):
        grad_each(level, sent)

    @pl.when(z == low)
    def _():
        for i in range(2):
            for half in range(2):
                sent(total_copy(i, half))

    def drain(d, carry):
        for k in range(2 * sides):
            if k != sides:
                sent(share_copy(lax.rem(s + d, nsp), k))
        return carry
    lax.fori_loop(1, nsp, drain, 0)


def finish_kernel(a, b, c, d, a_out, b_out, c_out, d_out, sems):
    stores = [
        pltpu.make_async_copy(src, dst, sems.at[i])
        for i, (src, dst) in enumerate(((a, a_out), (b, b_out), (c, c_out), (d, d_out)))
    ]
    for store in stores:
        store.start()
    for store in stores:
        store.wait()


def far():
    return pl.BlockSpec(memory_space=pltpu.HBM)


def hub_body(nsp, ntp, latents, query_heads, key_heads, value_heads, map_outputs, log_sums, out_grad,
             mix_lambda, norm_gain):
    rows, heads, width = query_heads.shape
    flat = (rows, heads * width)
    slab = latents.shape[1] // nsp
    nz = nsp // 2
    pair = heads // 2
    block = (2 * rows, pair * width)
    half = (rows, pair * width)
    dma = pltpu.SemaphoreType.DMA
    room = max(rows, width, heads)

    sums = jnp.transpose(log_sums, (1, 2, 0))
    small = (
        jnp.pad(sums, ((0, 1), (0, 0), (0, room - rows)))
        + jnp.pad(norm_gain[None, None, :], ((heads, 0), (0, 1), (0, room - width)))
        + jnp.pad(mix_lambda[None, None, :], ((heads, 0), (1, 0), (0, room - heads)))
    )
    results = pl.pallas_call(
        functools.partial(hub_kernel, nsp, ntp, heads, width),
        out_shape=(
            jax.ShapeDtypeStruct(query_heads.shape, BF16),
            jax.ShapeDtypeStruct(query_heads.shape, BF16),
            jax.ShapeDtypeStruct(query_heads.shape, BF16),
            jax.ShapeDtypeStruct((slab, heads * width), F32),
        ),
        in_specs=[vmem(), far()] + [vmem()] * 4,
        out_specs=(vmem(),) * 4,
        scratch_shapes=[
            pltpu.VMEM(flat, BF16),
            pltpu.VMEM((heads, 4, rows), F32),
            pltpu.VMEM((4, nz) + block, BF16),
            pltpu.VMEM((nz, 2, pair, 4, rows), F32),
            pltpu.VMEM((nz, pair, width, 2 * rows), F32),
            pltpu.VMEM((2,) + block, F32),
            pltpu.VMEM((2,) + block, F32),
            pltpu.VMEM((nz, 2) + block, BF16),
            pltpu.VMEM((2,) + block, BF16),
            pltpu.VMEM((2,) + block, BF16),
            pltpu.VMEM(block, BF16),
            pltpu.VMEM((2,) + block, BF16),
            pltpu.VMEM((2,) + block, BF16),
            pltpu.VMEM((2,) + half, BF16),
            pltpu.VMEM((2, 2) + half, BF16),
            pltpu.VMEM((nsp, rows, slab), BF16),
            dma((5,)), dma((5, 2)), dma((5, 2)), dma((4, nz, 2)), dma((nz, 2)), dma((nz, 3, 2)), dma((nz, 2, 2)),
            dma((2, 2)), dma((2, 2)), dma((2,)), dma((2,)), dma((2,)), dma((2, 2)), dma((2,)), dma((2, 2)),
            dma((nsp,)), dma((nsp,)), dma((nsp, ntp)), dma((nsp, ntp)),
            dma,
        ],
        compiler_params=pltpu.CompilerParams(
            collective_id=0, has_side_effects=True, vmem_limit_bytes=52500000),
        name="hub",
    )(
        small,
        latents,
        key_heads.reshape(flat),
        value_heads.reshape(flat),
        query_heads.reshape(flat),
        jnp.concatenate([map_outputs, out_grad[:, None]], axis=1),
    )
    return pl.pallas_call(
        finish_kernel,
        out_shape=tuple(jax.ShapeDtypeStruct(a.shape, a.dtype) for a in results),
        in_specs=[vmem()] * 4,
        out_specs=(far(),) * 4,
        scratch_shapes=[pltpu.SemaphoreType.DMA((4,))],
        compiler_params=pltpu.CompilerParams(vmem_limit_bytes=52500000),
        name="finish",
    )(*results)


def solution(mesh):
    placed = (
        P("sp", None),
        P("sp", "tp", None),
        P("sp", "tp", None),
        P("sp", "tp", None),
        P("sp", None, "tp", None),
        P("sp", "tp", None),
        P("sp", "tp", None),
        P("tp"),
        P(),
    )
    nsp, ntp = mesh.shape["sp"], mesh.shape["tp"]

    def chosen(*args):
        heads = args[1].shape[1]
        return (hub_body if nsp == 8 and heads % 2 == 0 else body)(nsp, ntp, *args)

    return jax.shard_map(
        chosen,
        mesh=mesh,
        in_specs=placed,
        out_specs=(P("sp", "tp", None), P("sp", "tp", None), P("sp", "tp", None), P("sp", "tp")),
        check_vma=False,
    )
```
